128 devices in a mesh: sp: 32 (over z, y, core), tp: 4 (over x).
Axes of the slice: x: 4, y: 4, z: 4, core: 2. Of those that a mesh axis runs over, the one named last changes fastest.
Arguments:
- mixer_output_stream: bfloat16 [4096, 2048], P('sp', 'tp'), may hold values from -6 to 6
- layer_output_gradient: bfloat16 [4096, 2048], P('sp', 'tp'), may hold values from -3.5 to 3.5
- routes: int32 [4096, 2], P('sp'), may hold values from 0 to 31, all different within a row; in each aligned block of 128 rows (0 to 127, 128 to 255, ...) at most 12 rows name the same one
- expert_combine_weight: float32 [4096, 2], P('sp'), may hold values from 0.2 to 1
- expert_gate_weight: bfloat16 [32, 2048, 3584], P('sp', None, 'tp'), may hold values from -0.125 to 0.125
- expert_up_weight: bfloat16 [32, 2048, 3584], P('sp', None, 'tp'), may hold values from -0.125 to 0.125
- expert_down_weight: bfloat16 [32, 3584, 2048], P('sp', 'tp'), may hold values from -0.09375 to 0.09375
- head_mixer_input: bfloat16 [4096, 4096], P('sp', 'tp'), may hold values from -6 to 6
- head_step_size: float32 [4096, 64], P('sp', 'tp'), may hold values from 0.25 to 4
- head_decay_rate: float32 [64], P('tp'), may hold values from 0 to 1
- extra_log_decay: float32 [4096, 64], P('sp', 'tp'), may hold values from -3 to 0
- state_entering_span: float32 [64, 64, 128], P('tp'), may hold values from -48 to 48
- state_input_vectors: bfloat16 [4096, 1024], P('sp', 'tp'), may hold values from -1.75 to 1.75
- state_readout_vectors: bfloat16 [4096, 1024], P('sp', 'tp'), may hold values from -1.75 to 1.75
- gate_preactivation: bfloat16 [4096, 4096], P('sp', 'tp'), may hold values from -6 to 6
- group_norm_scale: float32 [4096], P('tp'), may hold values from 0.1 to 1.9
- mixer_output_weight: bfloat16 [4096, 2048], P('tp', 'sp'), may hold values from -0.09375 to 0.09375
Outputs:
- grad_gate: bfloat16 [32, 2048, 3584], P('sp', None, 'tp')
- grad_up: bfloat16 [32, 2048, 3584], P('sp', None, 'tp')
- grad_down: bfloat16 [32, 3584, 2048], P('sp', 'tp')
- grad_out_proj: float32 [4096, 2048], P('tp', 'sp')
- grad_input: bfloat16 [4096, 4096], P('sp', 'tp')
- grad_step: float32 [4096, 64], P('sp', 'tp')
- grad_state_in: bfloat16 [4096, 1024], P('sp', 'tp')
- grad_read_out: bfloat16 [4096, 1024], P('sp', 'tp')
- grad_gate_in: bfloat16 [4096, 4096], P('sp', 'tp')
The draws below stay inside these ranges and needn't reach their ends.
Inputs may be any that keep to these rules, and one draw needn't show every extreme that they name: `routes`: the two experts of a token differ. In each aligned block of 128 rows no expert is named more than 12 times, and in every draw some expert is named exactly 12 times in some block.
All inputs are finite; a program needn't handle non-finite values.
Results may differ from the reference program's by a relative error of at most 0.02.
Values may be sent and summed in bfloat16 or wider, within the bound.
A program may use at most 128 MiB of HBM per device.

```python
import math
from functools import partial
import jax
import jax.numpy as jnp
import numpy as np
from jax import lax

D = 2048
FF = 3584
HEADS = 64
HDIM = 64
GROUPS = 8
STATE = 128
BLK = 128
TOP = 2
TOK_DEV = 128
DI = 4096
EXPERTS = 32
CAP = 12
TOKENS = 4096
N_TP = 4


def draw_head_step_size(key, part):
    first, second = jax.random.split(key)
    rough = jnp.exp(jax.random.uniform(first, (TOKENS, HEADS), jnp.float32, math.log(0.5), math.log(2.0)))
    spans = TOKENS // TOK_DEV
    factor = jnp.exp(jax.random.uniform(second, (spans, 1, 1), jnp.float32, math.log(0.5), math.log(2.0)))
    return (rough.reshape(spans, TOK_DEV, HEADS) * factor).reshape(TOKENS, HEADS)


def draw_head_decay_rate(key, part):
    first, second = jax.random.split(key)
    picks = jax.random.randint(first, (HEADS,), 0, 8)
    limit = 4
    spread = jnp.exp(jax.random.uniform(second, (HEADS,), jnp.float32, math.log(0.5), math.log(2.0)))
    fast_rate = 3.0 / BLK * spread
    slow_rate = 0.25 / TOKENS * spread
    return jnp.where(picks < limit, fast_rate, slow_rate)


def draw_extra_log_decay(key, part):
    first, second = jax.random.split(key)
    places = jax.random.randint(first, (3,), 0, TOKENS)
    amounts = jnp.log(jax.random.uniform(second, (3, HEADS), jnp.float32, 0.5, 0.8))
    hits = (jnp.arange(TOKENS, dtype=jnp.int32)[:, None] == places[None, :]).astype(jnp.float32)
    return jnp.dot(hits, amounts, precision=lax.Precision.HIGHEST)


def strengthened(result, rng, source, target, parts, factor):
    owner, partner = [(jnp.arange(result.shape[dim]) // (result.shape[dim] // parts)).reshape([-1 if axis == dim else 1 for axis in range(result.ndim)]) for dim in (source, target)]
    chosen = jax.random.permutation(rng, parts)[partner]
    strong = (owner == chosen) | (owner == (partner + parts // 2) % parts)
    return jnp.where(strong, factor * result, result)


def level_of(own_key, shape, cuts, smallest, high):
    factor_of, own = 1.0, jax.random.fold_in(own_key, 6)
    for dim, parts in cuts:
        steps = jnp.exp(jax.random.uniform(jax.random.fold_in(own, dim), (parts,), jnp.float32, smallest / len(cuts), high / len(cuts)))
        factor_of = factor_of * jnp.repeat(steps, shape[dim] // parts).reshape([-1 if axis == dim else 1 for axis in range(len(shape))])
    return factor_of


def deal_out(stream_key, own, number, rows, number_of, top, most, slope):
    ranking = jax.random.permutation(stream_key, number_of)
    heavy_load, common = portions_of(number_of, rows * top, most, slope, True), portions_of(number_of, rows * top, most, slope, False)
    places = jnp.arange(number_of)

    def named(sizes, turn):
        used = int((sizes > 0).sum())
        fixed = max(1, used // 4)
        moved = fixed + (places - fixed + turn * (used - fixed)) % max(1, number_of - fixed)
        return jnp.zeros((number_of,), jnp.int32).at[ranking[jnp.where(places < fixed, places, moved)]].set(jnp.asarray(sizes, jnp.int32))

    sizes = jnp.where(number % 4 == 0, named(heavy_load, number // 4), named(common, number - number // 4 - 1))
    mixed = jax.random.permutation(jax.random.fold_in(own, 3), number_of)
    source_of, receiver = mixed[0:number_of // 2 * 2:2], mixed[1:number_of // 2 * 2:2]
    room = jnp.minimum(sizes[source_of] - 1, most - sizes[receiver]) // 2
    room = jnp.where((source_of == ranking[0]) | (receiver == ranking[0]) | (sizes[receiver] == 0), 0, jnp.maximum(room, 0))
    moved = jax.random.randint(jax.random.fold_in(own, 4), (number_of // 2,), 0, 1 << 20) % (room + 1)
    sizes = sizes.at[source_of].add(-moved).at[receiver].add(moved)
    members = jnp.searchsorted(jnp.cumsum(sizes), jnp.arange(rows * top), side="right").astype(jnp.int32)
    table = members.reshape(top, rows).T
    table = table[jax.random.permutation(jax.random.fold_in(own, 1), rows)]
    turn = jax.random.randint(jax.random.fold_in(own, 2), (rows, 1), 0, top)
    return jnp.take_along_axis(table, (jnp.arange(top)[None, :] + turn) % top, axis=1)


def portions_of(number_of, total, bound, slope, full):
    portions = [(1 << 20) // math.isqrt(rank ** slope) + 1 for rank in range(1, number_of + 1)]
    largest = bound if full else min(bound, max(-(-total // number_of), total * portions[0] // sum(portions)))
    least = 1 if total - largest >= number_of - 1 else 0
    counts, spare = [largest] + [least] * (number_of - 1), total - largest - least * (number_of - 1)
    while spare > 0:
        free = [i for i in range(1, number_of) if counts[i] < largest] or [i for i in range(1, number_of) if counts[i] < bound]
        mass, remaining = sum([portions[i] for i in free]), spare
        for i in free:
            addition = min(bound - counts[i], max(1, remaining * portions[i] // mass), spare)
            counts[i] = counts[i] + addition
            spare = spare - addition
    return np.array(counts)


def scatter_about(stream_key, extent, deviation, most, pieces=(), held_as=jnp.bfloat16):
    values = deviation * jax.random.normal(stream_key, extent, jnp.float32)
    if pieces:
        values = values * level_of(stream_key, extent, pieces, -0.22, 0.18)
    return jnp.clip(values, -most, most).astype(held_as)


def gaussian_with(key, shape, width, bound, shards, heavy, held_as=jnp.bfloat16):
    entries = width * jax.random.normal(key, shape, jnp.float32)
    if shards:
        entries = entries * level_of(key, shape, shards, -0.22, 0.18)
    return jnp.clip(strengthened(entries, jax.random.fold_in(key, 3), *heavy), -bound, bound).astype(held_as)


def setup_inputs(seed: int = 0) -> dict:
    seeds = jax.random.split(jax.random.key(seed), 18)
    mixer_output_stream = scatter_about(seeds[0], (TOKENS, D), 1.0, 6.0, ((0, 32), (1, 4)))
    layer_output_gradient = gaussian_with(seeds[1], (TOKENS, D), 0.3, 3.5, ((0, 32), (1, 4)), (0, 1, 32, 2.75))
    routes_keys = jax.random.split(jax.random.fold_in(seeds[2], 1), TOKENS // TOK_DEV)
    routes_turns = jax.random.permutation(jax.random.fold_in(seeds[2], 3), TOKENS // TOK_DEV)
    routes = jax.vmap(lambda own, number: deal_out(jax.random.fold_in(seeds[2], 2), own, number, TOK_DEV, EXPERTS, TOP, CAP, 1))(routes_keys, routes_turns).reshape((TOKENS, TOP))
    expert_combine_weight = jnp.clip(0.2 + 0.8 * jax.random.uniform(seeds[3], (TOKENS, TOP), jnp.float32) ** level_of(seeds[3], (TOKENS, TOP), ((0, 32),), -0.2, 0.2), 0.2, 1.0)
    expert_gate_weight = scatter_about(seeds[4], (EXPERTS, D, FF), D ** -0.5, 0.125, ((0, 32), (2, 4)))
    expert_up_weight = scatter_about(seeds[5], (EXPERTS, D, FF), D ** -0.5, 0.125, ((0, 32), (2, 4)))
    expert_down_weight = scatter_about(seeds[6], (EXPERTS, FF, D), FF ** -0.5, 0.09375, ((0, 32), (1, 4)))
    head_mixer_input = scatter_about(seeds[7], (TOKENS, DI), 1.0, 6.0, ((0, 32), (1, 4)))
    head_step_size = draw_head_step_size(jax.random.fold_in(seeds[17], 71), 0)
    head_decay_rate = draw_head_decay_rate(jax.random.fold_in(seeds[17], 71), 0)
    extra_log_decay = draw_extra_log_decay(jax.random.fold_in(seeds[17], 71), 0)
    state_entering_span = scatter_about(seeds[11], (HEADS, HDIM, STATE), 8.0, 48.0, ((0, 4),), jnp.float32)
    state_input_vectors = scatter_about(seeds[12], (TOKENS, GROUPS * STATE), (STATE ** -0.25), 1.75, ((0, 32), (1, 4)))
    state_readout_vectors = scatter_about(seeds[13], (TOKENS, GROUPS * STATE), (STATE ** -0.25), 1.75, ((0, 32), (1, 4)))
    gate_preactivation = scatter_about(seeds[14], (TOKENS, DI), 1.0, 6.0, ((0, 32), (1, 4)))
    group_norm_scale = jnp.clip(1.0 + 0.18 * jax.random.normal(seeds[15], (DI,), jnp.float32), 0.1, 1.9)
    mixer_output_weight = scatter_about(seeds[16], (DI, D), DI ** -0.5, 0.09375, ((0, 4), (1, 32)))
    return dict(mixer_output_stream=mixer_output_stream, layer_output_gradient=layer_output_gradient, routes=routes, expert_combine_weight=expert_combine_weight, expert_gate_weight=expert_gate_weight, expert_up_weight=expert_up_weight, expert_down_weight=expert_down_weight, head_mixer_input=head_mixer_input, head_step_size=head_step_size, head_decay_rate=head_decay_rate, extra_log_decay=extra_log_decay, state_entering_span=state_entering_span, state_input_vectors=state_input_vectors, state_readout_vectors=state_readout_vectors, gate_preactivation=gate_preactivation, group_norm_scale=group_norm_scale, mixer_output_weight=mixer_output_weight)


norm_eps = 1e-05
exact_mode = lax.Precision.HIGHEST

def span_local_scan(input_heads, time_step, decay_speed, sudden_decay, input_vector_groups, readout_groups, starting_state):
    length, head_count, head_size = input_heads.shape
    groups, state_size = (input_vector_groups.shape[1], input_vector_groups.shape[2])
    per_group = head_count // groups
    block_count = length // BLK
    log_decay_total = sudden_decay - time_step * decay_speed[None, :]
    scaled = (input_heads * time_step[:, :, None]).reshape(block_count, BLK, groups, per_group, head_size)
    log_decay_total = log_decay_total.reshape(block_count, BLK, groups, per_group)
    b_rows = input_vector_groups.reshape(block_count, BLK, groups, state_size)
    c_rows = readout_groups.reshape(block_count, BLK, groups, state_size)
    cumulative = jnp.cumsum(log_decay_total, axis=1)
    causal_mask = jnp.tril(jnp.ones((BLK, BLK), dtype=bool))
    cum_t = jnp.moveaxis(cumulative, 1, -1)
    gaps = cum_t[..., :, None] - cum_t[..., None, :]
    decays = jnp.where(causal_mask, jnp.exp(jnp.where(causal_mask, gaps, 0.0)), 0.0)
    affinity = jnp.einsum('blgn,bsgn->bgls', c_rows, b_rows, precision=exact_mode)
    y_diag = jnp.einsum('bghls,bsghp->blghp', affinity[:, :, None] * decays, scaled, precision=exact_mode)
    to_end = jnp.exp(cumulative[:, -1:] - cumulative)
    states = jnp.einsum('blgn,blghp->bghpn', b_rows, scaled * to_end[..., None], precision=exact_mode)
    block_decay = jnp.exp(cumulative[:, -1])

    def advance(running, inputs):
        block_state, decay_now = inputs
        return (decay_now[..., None, None] * running + block_state, running)
    first_state = starting_state.reshape(groups, per_group, head_size, state_size)
    closing_state, incoming_state = lax.scan(advance, first_state, (states, block_decay))
    y_off = jnp.einsum('blgn,bghpn->blghp', c_rows, incoming_state, precision=exact_mode) * jnp.exp(cumulative)[..., None]
    result_rows = (y_diag + y_off).reshape(length, head_count, head_size)
    return (result_rows, closing_state.reshape(head_count, head_size, state_size))

def gate_norm(scan_out, gate_vals, group_norm_scale, groups):
    length = scan_out.shape[0]
    gated = scan_out.reshape(length, -1) * jax.nn.silu(gate_vals)
    grouped = gated.reshape(length, groups, -1)
    factor = lax.rsqrt(lax.optimization_barrier(jnp.mean(grouped * grouped, axis=-1, keepdims=True)) + norm_eps)
    return (grouped * factor).reshape(length, -1) * group_norm_scale[None, :]

def slot_index(route_rows, expert_count, capacity):
    flat_routes = route_rows.reshape(-1)
    onehot = (flat_routes[:, None] == jnp.arange(expert_count, dtype=jnp.int32)[None, :]).astype(jnp.int32)
    before = jnp.cumsum(onehot, axis=0) - onehot
    return flat_routes * capacity + lax.optimization_barrier(jnp.sum(before * onehot, axis=1))

def build_table(destination, slot_count):
    pair_count = destination.shape[0]
    return jnp.full((slot_count,), pair_count, jnp.int32).at[destination].set(jnp.arange(pair_count, dtype=jnp.int32))

def pack_rows(stream, grad_rows, slot_table, weights):
    token_of = slot_table // 2
    routed = jnp.take(stream, token_of, axis=0, mode='fill', fill_value=0)
    weight_of = jnp.take(weights.reshape(-1), slot_table, mode='fill', fill_value=0.0)
    picked = jnp.take(grad_rows, token_of, axis=0, mode='fill', fill_value=0).astype(jnp.float32)
    return (routed, (picked * weight_of[:, None]).astype(jnp.bfloat16))

def expert_hidden(routed_rows, routed_grads, w_gate, w_up, w_down):
    pre_gate = jnp.dot(routed_rows, w_gate, preferred_element_type=jnp.float32)
    pre_up = jnp.dot(routed_rows, w_up, preferred_element_type=jnp.float32)
    activated = jax.nn.silu(pre_gate)
    hidden = (activated * pre_up).astype(jnp.bfloat16)
    hidden_grad = lax.dot_general(routed_grads, w_down, (((1,), (1,)), ((), ())), preferred_element_type=jnp.float32)
    sigmoid_gate = jax.nn.sigmoid(pre_gate)
    gate_grad = (hidden_grad * pre_up * sigmoid_gate * (1.0 + pre_gate * (1.0 - sigmoid_gate))).astype(jnp.bfloat16)
    up_grad = (hidden_grad * activated).astype(jnp.bfloat16)
    return (hidden, gate_grad, up_grad)

def expert_weight_grads(routed_rows, routed_grads, hidden, gate_grad, up_grad):
    contract = (((0,), (0,)), ((), ()))
    grad_g = lax.dot_general(routed_rows, gate_grad, contract, preferred_element_type=jnp.float32)
    grad_u = lax.dot_general(routed_rows, up_grad, contract, preferred_element_type=jnp.float32)
    grad_d = lax.dot_general(hidden, routed_grads, contract, preferred_element_type=jnp.float32)
    return (grad_g.astype(jnp.bfloat16), grad_u.astype(jnp.bfloat16), grad_d.astype(jnp.bfloat16))

def row_partial(gate_grad, up_grad, w_gate, w_up):
    contract = (((1,), (1,)), ((), ()))
    partial_sum = lax.dot_general(gate_grad, w_gate, contract, preferred_element_type=jnp.float32)
    partial_sum = partial_sum + lax.dot_general(up_grad, w_up, contract, preferred_element_type=jnp.float32)
    return lax.optimization_barrier(partial_sum.astype(jnp.bfloat16)).astype(jnp.float32)

def add_returns(grad_rows, returned, destination):
    token_count = grad_rows.shape[0]
    gathered = jnp.take(returned, destination, axis=0).reshape(token_count, -1, returned.shape[-1]).astype(jnp.float32)
    return (grad_rows.astype(jnp.float32) + lax.optimization_barrier(jnp.sum(gathered, axis=1))).astype(jnp.bfloat16)

def reference(mixer_output_stream, layer_output_gradient, routes, expert_combine_weight, expert_gate_weight, expert_up_weight, expert_down_weight, head_mixer_input, head_step_size, head_decay_rate, extra_log_decay, state_entering_span, state_input_vectors, state_readout_vectors, gate_preactivation, group_norm_scale, mixer_output_weight):
    blocks = TOKENS // TOK_DEV
    destination = jax.vmap(partial(slot_index, expert_count=EXPERTS, capacity=CAP))(routes.reshape(blocks, TOK_DEV, TOP))
    tables = jax.vmap(partial(build_table, slot_count=EXPERTS * CAP))(destination)
    sent_rows, sent_grads = jax.vmap(pack_rows)(mixer_output_stream.reshape(blocks, TOK_DEV, D), layer_output_gradient.reshape(blocks, TOK_DEV, D), tables, expert_combine_weight.reshape(blocks, TOK_DEV, TOP))

    def by_expert(values):
        return values.reshape(blocks, EXPERTS, CAP, D).transpose(1, 0, 2, 3).reshape(EXPERTS, blocks * CAP, D)

    def per_expert(packed):
        routed_rows, routed_grads, w_gate, w_up, w_down = packed
        hidden, gate_grad, up_grad = expert_hidden(routed_rows, routed_grads, w_gate, w_up, w_down)
        grad_g, grad_u, grad_d = expert_weight_grads(routed_rows, routed_grads, hidden, gate_grad, up_grad)
        block_width = w_gate.shape[1] // N_TP
        running = jnp.zeros((routed_rows.shape[0], w_gate.shape[0]), jnp.float32)
        for block_number in range(N_TP):
            first_col = block_number * block_width
            running = running + row_partial(gate_grad[:, first_col:first_col + block_width], up_grad[:, first_col:first_col + block_width], w_gate[:, first_col:first_col + block_width], w_up[:, first_col:first_col + block_width])
        return (grad_g, grad_u, grad_d, running.astype(jnp.bfloat16))
    grad_gate, grad_up, grad_down, returned = lax.map(per_expert, (by_expert(sent_rows), by_expert(sent_grads), expert_gate_weight, expert_up_weight, expert_down_weight))
    returned = returned.reshape(EXPERTS, blocks, CAP, D).transpose(1, 0, 2, 3).reshape(blocks, EXPERTS * CAP, D)
    mix_grad = jax.vmap(add_returns)(layer_output_gradient.reshape(blocks, TOK_DEV, D), returned, destination).reshape(TOKENS, D)
    input_heads = head_mixer_input.astype(jnp.float32).reshape(TOKENS, HEADS, HDIM)
    input_vector_groups = state_input_vectors.astype(jnp.float32).reshape(TOKENS, GROUPS, STATE)
    readout_groups = state_readout_vectors.astype(jnp.float32).reshape(TOKENS, GROUPS, STATE)

    def forward(input_values, time_step_values, input_vector_entries, readout_entries):
        result_rows, closing_state = span_local_scan(input_values, time_step_values, head_decay_rate, extra_log_decay, input_vector_entries, readout_entries, state_entering_span)
        return result_rows
    scan_out, pull_back = jax.vjp(forward, input_heads, head_step_size, input_vector_groups, readout_groups)

    def apply_norm(scan_vals, gate_vals):
        return gate_norm(scan_vals, gate_vals, group_norm_scale, GROUPS)
    normed, pull_norm = jax.vjp(apply_norm, scan_out, gate_preactivation.astype(jnp.float32))
    normed_low = normed.astype(jnp.bfloat16)
    grad_out_proj = lax.dot_general(normed_low, mix_grad, (((0,), (0,)), ((), ())), preferred_element_type=jnp.float32)
    normed_grad = lax.dot_general(mix_grad, mixer_output_weight, (((1,), (1,)), ((), ())), preferred_element_type=jnp.float32)
    scanned_gradient, gate_grad_in = pull_norm(normed_grad)
    input_grad, step_grad, b_grad, c_grad = pull_back(scanned_gradient)
    return (grad_gate, grad_up, grad_down, grad_out_proj, input_grad.reshape(TOKENS, DI).astype(jnp.bfloat16), step_grad, b_grad.reshape(TOKENS, GROUPS * STATE).astype(jnp.bfloat16), c_grad.reshape(TOKENS, GROUPS * STATE).astype(jnp.bfloat16), gate_grad_in.astype(jnp.bfloat16))
```

```python
import functools

import jax
import jax.numpy as jnp
from jax import lax
from jax.experimental import pallas as pl
from jax.experimental.pallas import tpu as pltpu
from jax.sharding import PartitionSpec as P

HDIM = 64
STATE = 128
BLK = 128
SP = "sp"
CAP = 12
MESH = pl.DeviceIdType.MESH
F32 = jnp.float32
BF16 = jnp.bfloat16

norm_eps = 1e-05
exact_mode = lax.Precision.HIGHEST
VMEM_BYTES = 60 * 1024 * 1024


def vmem_spec():
    return pl.BlockSpec(memory_space=pltpu.VMEM)


def any_spec():
    return pl.BlockSpec(memory_space=pl.ANY)


def dot(a, b, contract=((1,), (0,))):
    return lax.dot_general(a, b, (contract, ((), ())), preferred_element_type=F32)


def iota(shape, dim):
    return lax.broadcasted_iota(jnp.int32, shape, dim)


def divide(x, by):
    return ((x.astype(F32) + 0.5) * (1.0 / by)).astype(jnp.int32)


def slots_in_rows(routes, experts):
    top, tokens = routes.shape
    ids = iota((experts, tokens), 0)
    earlier = (iota((tokens, tokens), 0) < iota((tokens, tokens), 1)).astype(BF16)
    before = jnp.zeros((experts, 1), F32)
    rows = []
    for k in range(top):
        hits = (ids == routes[k : k + 1, :]).astype(F32)
        rank = dot(hits.astype(BF16), earlier) + before
        rows.append(jnp.sum(hits * rank, axis=0, keepdims=True))
        before = before + jnp.sum(hits, axis=1, keepdims=True)
    return [routes[k : k + 1, :] * CAP + rows[k].astype(jnp.int32) for k in range(top)]


def slots_in_columns(routes, experts):
    tokens, top = routes.shape
    ids = iota((tokens, experts), 1)
    earlier = (iota((tokens, tokens), 1) < iota((tokens, tokens), 0)).astype(BF16)
    before = jnp.zeros((1, experts), F32)
    columns = []
    for k in range(top):
        hits = (ids == routes[:, k : k + 1]).astype(F32)
        rank = dot(earlier, hits.astype(BF16)) + before
        columns.append(jnp.sum(hits * rank, axis=1, keepdims=True))
        before = before + jnp.sum(hits, axis=0, keepdims=True)
    return [routes[:, k : k + 1] * CAP + columns[k].astype(jnp.int32) for k in range(top)]


def pack_kernel(experts, routes_ref, weights_ref, stream_ref, grads_ref, out_ref):
    tokens = stream_ref.shape[0]
    half = stream_ref.shape[1] // 2
    slots = slots_in_rows(routes_ref[...], experts)
    row = iota((experts * 4 * CAP, 1), 0)
    expert = divide(row, 4 * CAP)
    inner = row - expert * (4 * CAP)
    part = divide(inner, CAP)
    slot = expert * CAP + inner - part * CAP
    first = (slot == slots[0]).astype(F32)
    second = (slot == slots[1]).astype(F32)
    match = (first + second).astype(BF16)
    weight = jnp.sum(
        first * weights_ref[0:1, :] + second * weights_ref[1:2, :], axis=1, keepdims=True
    )
    x0 = dot(match, stream_ref[:, :half])
    x1 = dot(match, stream_ref[:, half:])
    g0 = dot(match, grads_ref[:, :half])
    g1 = dot(match, grads_ref[:, half:])
    low = jnp.where(part == 0, x0, g0 * weight)
    high = jnp.where(part == 2, x1, g1 * weight)
    out_ref[...] = jnp.where(part < 2, low, high).astype(BF16)


def pack(routes, weights, stream, grads, experts):
    half = stream.shape[1] // 2
    packed = pl.pallas_call(
        functools.partial(pack_kernel, experts),
        out_shape=jax.ShapeDtypeStruct((experts * 4 * CAP, half), BF16),
        in_specs=[vmem_spec()] * 4,
        out_specs=vmem_spec(),
        compiler_params=pltpu.CompilerParams(vmem_limit_bytes=VMEM_BYTES),
        name="pack",
    )(routes.T, weights.T, stream, grads)
    return packed.reshape(experts, 4 * CAP, half)


def greet(me, tp, n_sp, n_tp, step=1, ring=False, partner=None):
    barrier = pltpu.get_barrier_semaphore()

    def hello(d, carry):
        pl.semaphore_signal(
            barrier, inc=1, device_id=(lax.rem(me + d * step, n_sp), tp), device_id_type=MESH
        )
        return carry

    lax.fori_loop(1, n_sp // step, hello, 0)
    count = n_sp // step - 1
    if partner is not None:
        pl.semaphore_signal(barrier, inc=1, device_id=(partner, tp), device_id_type=MESH)
        count += 1
    if ring:
        for other in (lax.rem(tp + 1, n_tp), lax.rem(tp + n_tp - 1, n_tp)):
            pl.semaphore_signal(barrier, inc=1, device_id=(me, other), device_id_type=MESH)
        count += 2
    pl.semaphore_wait(barrier, count)


def dispatch_kernel(
    n_sp, n_tp, in_ref, out_ref, own, a_send, a_recv, s_right, s_left, r_left, r_right, f_send, f_recv
):
    me, tp = lax.axis_index("sp"), lax.axis_index("tp")
    right, left = lax.rem(tp + 1, n_tp), lax.rem(tp + n_tp - 1, n_tp)
    far = lax.rem(tp + 2, n_tp)
    greet(me, tp, n_sp, n_tp, ring=True)

    def origin(d):
        return lax.rem(me + n_sp - d, n_sp)

    def exchange(d):
        to = lax.rem(me + d, n_sp)
        return pltpu.make_async_remote_copy(
            in_ref.at[to], out_ref.at[tp, me], a_send.at[d], a_recv.at[d], (to, tp), MESH
        )

    def arrived(d):
        return pltpu.make_async_remote_copy(
            in_ref.at[me], out_ref.at[tp, origin(d)], a_send.at[d], a_recv.at[d], (me, tp), MESH
        )

    def to_right(d, block):
        piece = out_ref.at[block, origin(d)]
        return pltpu.make_async_remote_copy(
            piece, piece, s_right.at[d], r_left.at[d], (me, right), MESH
        )

    def to_left(d, block):
        piece = out_ref.at[block, origin(d)]
        return pltpu.make_async_remote_copy(
            piece, piece, s_left.at[d], r_right.at[d], (me, left), MESH
        )

    def onward(d, block, to):
        piece = out_ref.at[block, origin(d)]
        return pltpu.make_async_remote_copy(
            piece, piece, f_send.at[d], f_recv.at[d], (me, to), MESH
        )

    def start_exchange(d, carry):
        exchange(d).start()
        return carry

    lax.fori_loop(1, n_sp, start_exchange, 0)
    mine = pltpu.make_async_copy(in_ref.at[me], out_ref.at[tp, me], own)
    mine.start()
    mine.wait()
    to_right(0, tp).start()
    to_left(0, tp).start()

    def spread(d, carry):
        arrived(d).wait_recv()
        to_right(d, tp).start()
        to_left(d, tp).start()
        return carry

    lax.fori_loop(1, n_sp, spread, 0)

    def relay(q, carry):
        d = 2 * q
        to_right(d, left).wait_recv()
        onward(d, left, right).start()
        to_left(d + 1, right).wait_recv()
        onward(d + 1, right, left).start()
        return carry

    lax.fori_loop(0, n_sp // 2, relay, 0)

    def finish(q, carry):
        d = 2 * q
        to_left(d, right).wait_recv()
        to_right(d + 1, left).wait_recv()
        onward(d, far, right).wait()
        onward(d + 1, far, left).wait()
        to_right(d, tp).wait_send()
        to_left(d, tp).wait_send()
        to_right(d + 1, tp).wait_send()
        to_left(d + 1, tp).wait_send()
        return carry

    lax.fori_loop(0, n_sp // 2, finish, 0)

    def drain(d, carry):
        exchange(d).wait_send()
        return carry

    lax.fori_loop(1, n_sp, drain, 0)


def dispatch(packed, n_sp, n_tp):
    dma = pltpu.SemaphoreType.DMA
    return pl.pallas_call(
        functools.partial(dispatch_kernel, n_sp, n_tp),
        out_shape=jax.ShapeDtypeStruct((n_tp,) + packed.shape, BF16),
        in_specs=[vmem_spec()],
        out_specs=vmem_spec(),
        scratch_shapes=[dma] + [dma((n_sp,))] * 8,
        compiler_params=pltpu.CompilerParams(
            collective_id=0, has_side_effects=True, vmem_limit_bytes=VMEM_BYTES
        ),
        name="dispatch",
    )(packed)


def return_kernel(
    n_sp,
    n_tp,
    part_ref,
    routes_ref,
    grads_ref,
    mix_ref,
    from_left,
    from_right,
    sum_right,
    sum_left,
    out_blocks,
    back,
    own_cols,
    s_r,
    s_l,
    r_l,
    r_r,
    a_send,
    a_recv,
    g_send,
    g_recv,
    local,
):
    me, tp = lax.axis_index("sp"), lax.axis_index("tp")
    right, left = lax.rem(tp + 1, n_tp), lax.rem(tp + n_tp - 1, n_tp)
    far = lax.rem(tp + 2, n_tp)
    tokens, width = grads_ref.shape
    half, quarter = width // 2, width // 4
    greet(me, tp, n_sp, n_tp, ring=True)

    def block(b, which):
        return part_ref.at[:, pl.ds(pl.multiple_of(b * width + which * half, half), half)]

    def right_copy(k, src):
        return pltpu.make_async_remote_copy(
            src, from_left.at[k], s_r.at[k], r_l.at[k], (me, right), MESH
        )

    def left_copy(k, src):
        return pltpu.make_async_remote_copy(
            src, from_right.at[k], s_l.at[k], r_r.at[k], (me, left), MESH
        )

    right_copy(0, block(far, 0)).start()
    left_copy(0, block(far, 1)).start()
    right_copy(1, block(right, 1)).start()
    left_copy(1, block(left, 0)).start()

    slots = slots_in_columns(routes_ref[...], n_sp)
    column = iota((1, n_sp * 4 * CAP), 1)
    expert = divide(column, 4 * CAP)
    inner = column - expert * (4 * CAP)
    piece = divide(inner, CAP)
    slot = expert * CAP + inner - piece * CAP
    match = (slots[0] == slot) | (slots[1] == slot)

    right_copy(0, block(far, 0)).wait()
    sum_right[...] = (
        block(right, 0)[...].astype(F32) + from_left[0].astype(F32)
    ).astype(BF16)
    right_copy(2, sum_right).start()
    left_copy(0, block(far, 1)).wait()
    sum_left[...] = (
        block(left, 1)[...].astype(F32) + from_right[0].astype(F32)
    ).astype(BF16)
    left_copy(2, sum_left).start()
    right_copy(1, block(right, 1)).wait()
    left_copy(1, block(left, 0)).wait()
    right_copy(2, sum_right).wait()
    left_copy(2, sum_left).wait()

    rows = part_ref.shape[0]
    group_of = 8
    span = group_of * CAP
    wide = iota((group_of * 4 * CAP, 1), 0)
    wide_src = divide(wide, 4 * CAP)
    wide_in = wide - wide_src * (4 * CAP)
    wide_piece = divide(wide_in, CAP)
    wide_row = wide_src * CAP + wide_in - wide_piece * CAP
    spots = iota((1, span), 1)
    place = [((wide_row == spots) & (wide_piece == c)).astype(BF16) for c in range(4)]
    for g in range(rows // span):
        at = slice(g * span, (g + 1) * span)
        low = (
            block(tp, 0)[at, :].astype(F32)
            + from_left[2, at, :].astype(F32)
            + from_right[1, at, :].astype(F32)
        ).astype(BF16)
        high = (
            block(tp, 1)[at, :].astype(F32)
            + from_right[2, at, :].astype(F32)
            + from_left[1, at, :].astype(F32)
        ).astype(BF16)
        laid = (
            dot(place[0], low[:, :quarter])
            + dot(place[1], low[:, quarter:])
            + dot(place[2], high[:, :quarter])
            + dot(place[3], high[:, quarter:])
        )
        out_blocks[g * group_of : (g + 1) * group_of] = laid.astype(BF16).reshape(
            group_of, 4 * CAP, quarter
        )

    def exchange(d):
        to = lax.rem(me + d, n_sp)
        return pltpu.make_async_remote_copy(
            out_blocks.at[to], back.at[me], a_send.at[d], a_recv.at[d], (to, tp), MESH
        )

    def start_exchange(d, carry):
        exchange(d).start()
        return carry

    lax.fori_loop(1, n_sp, start_exchange, 0)
    mine = pltpu.make_async_copy(out_blocks.at[me], back.at[me], local)
    mine.start()
    mine.wait()

    def finish_exchange(d, carry):
        exchange(d).wait()
        return carry

    lax.fori_loop(1, n_sp, finish_exchange, 0)
    returned = back[...].reshape(n_sp * 4 * CAP, quarter)
    for c in range(4):
        chosen = jnp.where(match & (piece == c), 1.0, 0.0).astype(BF16)
        cols = slice(c * quarter, (c + 1) * quarter)
        own_cols[:, cols] = (grads_ref[:, cols].astype(F32) + dot(chosen, returned)).astype(BF16)

    def spot(b):
        return mix_ref.at[:, pl.ds(pl.multiple_of(b * width, width), width)]

    def spot_half(b, which):
        return mix_ref.at[:, pl.ds(pl.multiple_of(b * width + which * half, half), half)]

    def gather(k, src, dst, to):
        return pltpu.make_async_remote_copy(
            src, dst, g_send.at[k], g_recv.at[k], (me, to), MESH
        )

    gather(0, own_cols, spot(tp), right).start()
    gather(1, own_cols, spot(tp), left).start()
    spot(tp)[...] = own_cols[...]
    gather(0, own_cols, spot(left), right).wait_recv()
    gather(2, spot_half(left, 0), spot_half(left, 0), right).start()
    gather(1, own_cols, spot(right), left).wait_recv()
    gather(3, spot_half(right, 1), spot_half(right, 1), left).start()
    gather(2, spot_half(far, 0), spot_half(far, 0), right).wait()
    gather(3, spot_half(far, 1), spot_half(far, 1), left).wait()
    gather(0, own_cols, spot(tp), right).wait_send()
    gather(1, own_cols, spot(tp), left).wait_send()


def give_back(partial_rows, routes, grads, n_sp, n_tp):
    rows = partial_rows.shape[0]
    tokens, width = grads.shape
    half, quarter = width // 2, width // 4
    dma = pltpu.SemaphoreType.DMA
    return pl.pallas_call(
        functools.partial(return_kernel, n_sp, n_tp),
        out_shape=jax.ShapeDtypeStruct((tokens, width * n_tp), BF16),
        in_specs=[vmem_spec()] * 3,
        out_specs=vmem_spec(),
        scratch_shapes=[
            pltpu.VMEM((3, rows, half), BF16),
            pltpu.VMEM((3, rows, half), BF16),
            pltpu.VMEM((rows, half), BF16),
            pltpu.VMEM((rows, half), BF16),
            pltpu.VMEM((n_sp, 4 * CAP, quarter), BF16),
            pltpu.VMEM((n_sp, 4 * CAP, quarter), BF16),
            pltpu.VMEM((tokens, width), BF16),
            dma((3,)),
            dma((3,)),
            dma((3,)),
            dma((3,)),
            dma((n_sp,)),
            dma((n_sp,)),
            dma((4,)),
            dma((4,)),
            dma,
        ],
        compiler_params=pltpu.CompilerParams(
            collective_id=1, has_side_effects=True, vmem_limit_bytes=VMEM_BYTES
        ),
        name="give_back",
    )(partial_rows, routes, grads)


def carry_kernel(
    n_sp, n_tp, reverse, state_ref, decay_ref, first_ref, out_ref, states, decays, carries, one, two, sends, recvs, d_sends, d_recvs, b_sends, b_recvs
):
    me, tp = lax.axis_index("sp"), lax.axis_index("tp")
    greet(me, tp, n_sp, n_tp)

    def state_copy(d):
        to = lax.rem(me + d, n_sp)
        return pltpu.make_async_remote_copy(
            state_ref.at[to], states.at[me], sends.at[d], recvs.at[d], (to, tp), MESH
        )

    def decay_copy(d):
        to = lax.rem(me + d, n_sp)
        return pltpu.make_async_remote_copy(
            decay_ref.at[to], decays.at[me], d_sends.at[d], d_recvs.at[d], (to, tp), MESH
        )

    def back_copy(d):
        to = lax.rem(me + d, n_sp)
        return pltpu.make_async_remote_copy(
            carries.at[to], out_ref.at[me], b_sends.at[d], b_recvs.at[d], (to, tp), MESH
        )

    def start(d, carry):
        decay_copy(d).start()
        state_copy(d).start()
        return carry

    def finish(d, carry):
        decay_copy(d).wait()
        state_copy(d).wait()
        return carry

    lax.fori_loop(1, n_sp, start, 0)
    mine = pltpu.make_async_copy(state_ref.at[me], states.at[me], one)
    mine_too = pltpu.make_async_copy(decay_ref.at[me], decays.at[me], two)
    mine.start()
    mine_too.start()
    mine.wait()
    mine_too.wait()
    lax.fori_loop(1, n_sp, finish, 0)
    running = first_ref[...]
    for step in range(n_sp):
        i = n_sp - 1 - step if reverse else step
        carries[i] = running.astype(BF16)
        running = decays[i] * running + states[i].astype(F32)

    def start_back(d, carry):
        back_copy(d).start()
        return carry

    def finish_back(d, carry):
        back_copy(d).wait()
        return carry

    lax.fori_loop(1, n_sp, start_back, 0)
    mine = pltpu.make_async_copy(carries.at[me], out_ref.at[me], one)
    mine.start()
    mine.wait()
    lax.fori_loop(1, n_sp, finish_back, 0)


def carried(state, decay, first, n_sp, n_tp, reverse, identity):
    heads, channels, entries = state.shape
    rows = heads * channels // n_sp
    state = state.reshape(n_sp, rows, entries).astype(BF16)
    decay = jnp.broadcast_to(
        jnp.repeat(decay, channels // rows)[:, None, None], (n_sp, 1, entries)
    ) + jnp.zeros((n_sp, 1, entries), F32)
    dma = pltpu.SemaphoreType.DMA
    out = pl.pallas_call(
        functools.partial(carry_kernel, n_sp, n_tp, reverse),
        out_shape=jax.ShapeDtypeStruct((n_sp, rows, entries), BF16),
        in_specs=[vmem_spec()] * 3,
        out_specs=vmem_spec(),
        scratch_shapes=[
            pltpu.VMEM((n_sp, rows, entries), BF16),
            pltpu.VMEM((n_sp, 1, entries), F32),
            pltpu.VMEM((n_sp, rows, entries), BF16),
            dma,
            dma,
        ]
        + [dma((n_sp,))] * 6,
        compiler_params=pltpu.CompilerParams(
            collective_id=identity, has_side_effects=True, vmem_limit_bytes=VMEM_BYTES
        ),
        name="carry_back" if reverse else "carry",
    )(state, decay, first)
    return out.reshape(heads, channels, entries).astype(F32)


def proj_kernel(
    n_sp, n_tp, normed_ref, mix_ref, out_ref, normed2, mix2, parts, landed, total, other, p_send, p_recv, a_send, a_recv
):
    me, tp = lax.axis_index("sp"), lax.axis_index("tp")
    core = lax.rem(me, 2)
    partner = me + 1 - 2 * core
    chip = lax.div(me, 2)
    chips = n_sp // 2
    half = normed_ref.shape[1] // 2
    cols = out_ref.shape[1]
    greet(me, tp, n_sp, n_tp, step=2, partner=partner)

    def pair(k, src, dst):
        return pltpu.make_async_remote_copy(
            src, dst, p_send.at[k], p_recv.at[k], (partner, tp), MESH
        )

    def mine(c):
        return pl.ds(pl.multiple_of(c * half, half), half)

    pair(0, normed_ref.at[:, mine(1 - core)], normed2).start()
    pair(1, mix_ref, mix2).start()
    pair(0, normed_ref.at[:, mine(1 - core)], normed2).wait()
    pair(1, mix_ref, mix2).wait()
    for c in range(chips):
        at = slice(c * 2 * cols, (c + 1) * 2 * cols)
        parts[c] = (
            dot(normed_ref[:, mine(core)], mix_ref[:, at], ((0,), (0,)))
            + dot(normed2[...], mix2[:, at], ((0,), (0,)))
        ).astype(BF16)

    def exchange(d):
        to = lax.rem(chip + d, chips)
        return pltpu.make_async_remote_copy(
            parts.at[to], landed.at[chip], a_send.at[d], a_recv.at[d], (2 * to + core, tp), MESH
        )

    def start(d, carry):
        exchange(d).start()
        return carry

    lax.fori_loop(1, chips, start, 0)
    total[...] = parts[chip].astype(F32)

    def finish(d, carry):
        exchange(d).wait()
        total[...] += landed[lax.rem(chip + chips - d, chips)].astype(F32)
        return carry

    lax.fori_loop(1, chips, finish, 0)
    pair(2, total, other).start()
    out_ref[mine(core), :] = jnp.where(core == 0, total[:, :cols], total[:, cols:])
    pair(2, total, other).wait()
    out_ref[mine(1 - core), :] = jnp.where(core == 0, other[:, :cols], other[:, cols:])


def project(normed_low, mix, n_sp, n_tp):
    tokens, channels = normed_low.shape
    width = mix.shape[1]
    half = channels // 2
    chips = n_sp // 2
    cols = width // n_sp
    dma = pltpu.SemaphoreType.DMA
    return pl.pallas_call(
        functools.partial(proj_kernel, n_sp, n_tp),
        out_shape=jax.ShapeDtypeStruct((channels, cols), F32),
        in_specs=[vmem_spec()] * 2,
        out_specs=vmem_spec(),
        scratch_shapes=[
            pltpu.VMEM((tokens, half), BF16),
            pltpu.VMEM((tokens, width), BF16),
            pltpu.VMEM((chips, half, 2 * cols), BF16),
            pltpu.VMEM((chips, half, 2 * cols), BF16),
            pltpu.VMEM((half, 2 * cols), F32),
            pltpu.VMEM((half, 2 * cols), F32),
            dma((3,)),
            dma((3,)),
            dma((chips,)),
            dma((chips,)),
        ],
        compiler_params=pltpu.CompilerParams(
            collective_id=4, has_side_effects=True, vmem_limit_bytes=VMEM_BYTES
        ),
        name="project",
    )(normed_low, mix)


def expert_kernel(steps, in_ref, gate_ref, up_ref, down_ref, dgate_ref, dup_ref, ddown_ref, rows_ref, x, g, acc):
    step = pl.program_id(0)
    n_tp, n_sp, tall, half = in_ref.shape
    rows = n_sp * CAP

    @pl.when(step == 0)
    def _():
        group_of = 8
        span = group_of * CAP
        spots = iota((1, group_of * tall), 1)
        src = divide(spots, tall)
        inner = spots - src * tall
        part = divide(inner, CAP)
        row = src * CAP + inner - part * CAP
        mine = iota((span, 1), 0)
        pick = [((row == mine) & (part == p)).astype(BF16) for p in range(4)]
        for t in range(n_tp):
            for k in range(n_sp // group_of):
                block = in_ref[t, k * group_of : (k + 1) * group_of].reshape(
                    group_of * tall, half
                )
                at = slice(k * span, (k + 1) * span)
                for c in range(2):
                    cols = slice((2 * t + c) * half, (2 * t + c + 1) * half)
                    x[at, cols] = dot(pick[2 * c], block).astype(BF16)
                    g[at, cols] = dot(pick[2 * c + 1], block).astype(BF16)
        acc[...] = jnp.zeros_like(acc)

    w_gate, w_up, w_down = gate_ref[0], up_ref[0], down_ref[0]
    pre_gate = dot(x[...], w_gate)
    pre_up = dot(x[...], w_up)
    hidden_grad = dot(g[...], w_down, ((1,), (1,)))
    sigmoid_gate = jax.nn.sigmoid(pre_gate)
    activated = pre_gate * sigmoid_gate
    hidden = (activated * pre_up).astype(BF16)
    gate_grad = (
        hidden_grad * pre_up * sigmoid_gate * (1.0 + pre_gate * (1.0 - sigmoid_gate))
    ).astype(BF16)
    up_grad = (hidden_grad * activated).astype(BF16)
    over_rows = ((0,), (0,))
    dgate_ref[0] = dot(x[...], gate_grad, over_rows).astype(BF16)
    dup_ref[0] = dot(x[...], up_grad, over_rows).astype(BF16)
    ddown_ref[0] = dot(hidden, g[...], over_rows).astype(BF16)
    acc[...] += dot(gate_grad, w_gate, ((1,), (1,))) + dot(up_grad, w_up, ((1,), (1,)))

    @pl.when(step == steps - 1)
    def _():
        rows_ref[...] = acc[...].astype(BF16)


def experts_backward(arrived, w_gate, w_up, w_down):
    n_tp, n_sp, tall, half = arrived.shape
    _, width, hidden = w_gate.shape
    rows = n_sp * CAP
    tile = 128
    steps = hidden // tile
    by_col = pl.BlockSpec((1, width, tile), lambda j: (0, 0, j))
    by_row = pl.BlockSpec((1, tile, width), lambda j: (0, j, 0))
    return pl.pallas_call(
        functools.partial(expert_kernel, steps),
        grid=(steps,),
        out_shape=(
            jax.ShapeDtypeStruct(w_gate.shape, BF16),
            jax.ShapeDtypeStruct(w_up.shape, BF16),
            jax.ShapeDtypeStruct(w_down.shape, BF16),
            jax.ShapeDtypeStruct((rows, width), BF16),
        ),
        in_specs=[
            pl.BlockSpec(arrived.shape, lambda j: (0, 0, 0, 0)),
            by_col,
            by_col,
            by_row,
        ],
        out_specs=(by_col, by_col, by_row, pl.BlockSpec((rows, width), lambda j: (0, 0))),
        scratch_shapes=[
            pltpu.VMEM((rows, width), BF16),
            pltpu.VMEM((rows, width), BF16),
            pltpu.VMEM((rows, width), F32),
        ],
        compiler_params=pltpu.CompilerParams(vmem_limit_bytes=VMEM_BYTES),
        name="experts",
    )(arrived, w_gate, w_up, w_down)


def span_local_scan(
    input_heads,
    time_step,
    decay_speed,
    sudden_decay,
    input_vector_groups,
    readout_groups,
    starting_state,
):
    length, head_count, head_size = input_heads.shape
    groups, state_size = (input_vector_groups.shape[1], input_vector_groups.shape[2])
    per_group = head_count // groups
    block_count = length // BLK
    log_decay_total = sudden_decay - time_step * decay_speed[None, :]
    scaled = (input_heads * time_step[:, :, None]).reshape(
        block_count, BLK, groups, per_group, head_size
    )
    log_decay_total = log_decay_total.reshape(block_count, BLK, groups, per_group)
    b_rows = input_vector_groups.reshape(block_count, BLK, groups, state_size)
    c_rows = readout_groups.reshape(block_count, BLK, groups, state_size)
    cumulative = jnp.cumsum(log_decay_total, axis=1)
    causal_mask = jnp.tril(jnp.ones((BLK, BLK), dtype=bool))
    cum_t = jnp.moveaxis(cumulative, 1, -1)
    gaps = cum_t[..., :, None] - cum_t[..., None, :]
    decays = jnp.where(causal_mask, jnp.exp(jnp.where(causal_mask, gaps, 0.0)), 0.0)
    affinity = jnp.einsum("blgn,bsgn->bgls", c_rows, b_rows, precision=exact_mode)
    y_diag = jnp.einsum(
        "bghls,bsghp->blghp", affinity[:, :, None] * decays, scaled, precision=exact_mode
    )
    to_end = jnp.exp(cumulative[:, -1:] - cumulative)
    states = jnp.einsum(
        "blgn,blghp->bghpn", b_rows, scaled * to_end[..., None], precision=exact_mode
    )
    block_decay = jnp.exp(cumulative[:, -1])

    def advance(running, inputs):
        block_state, decay_now = inputs
        return (decay_now[..., None, None] * running + block_state, running)

    first_state = starting_state.reshape(groups, per_group, head_size, state_size)
    closing_state, incoming_state = lax.scan(advance, first_state, (states, block_decay))
    y_off = (
        jnp.einsum("blgn,bghpn->blghp", c_rows, incoming_state, precision=exact_mode)
        * jnp.exp(cumulative)[..., None]
    )
    result_rows = (y_diag + y_off).reshape(length, head_count, head_size)
    return (result_rows, closing_state.reshape(head_count, head_size, state_size))


def span_final_state(input_heads, time_step, decay_speed, sudden_decay, input_vector_groups):
    length, head_count, head_size = input_heads.shape
    groups = input_vector_groups.shape[1]
    log_decay_total = sudden_decay - time_step * decay_speed[None, :]
    sum_total = jnp.sum(log_decay_total, axis=0)
    after = sum_total[None, :] - jnp.cumsum(log_decay_total, axis=0)
    weighted = (input_heads * (time_step * jnp.exp(after))[:, :, None]).reshape(
        length, groups, head_count // groups, head_size
    )
    result = jnp.einsum("tgn,tghp->ghpn", input_vector_groups, weighted, precision=exact_mode)
    return (result.reshape(head_count, head_size, -1), jnp.exp(sum_total))


def carried_weight(scanned_gradient, readout_groups, time_step, decay_speed, sudden_decay):
    length, head_count, head_size = scanned_gradient.shape
    groups = readout_groups.shape[1]
    log_decay_total = sudden_decay - time_step * decay_speed[None, :]
    weighted = (
        scanned_gradient * jnp.exp(jnp.cumsum(log_decay_total, axis=0))[:, :, None]
    ).reshape(length, groups, head_count // groups, head_size)
    result = jnp.einsum("tgn,tghp->ghpn", readout_groups, weighted, precision=exact_mode)
    return result.reshape(head_count, head_size, -1)


def gate_norm(scan_out, gate_vals, group_norm_scale, groups):
    length = scan_out.shape[0]
    gated = scan_out.reshape(length, -1) * jax.nn.silu(gate_vals)
    grouped = gated.reshape(length, groups, -1)
    factor = lax.rsqrt(jnp.mean(grouped * grouped, axis=-1, keepdims=True) + norm_eps)
    return (grouped * factor).reshape(length, -1) * group_norm_scale[None, :]


def body(
    n_sp,
    n_tp,
    mixer_output_stream,
    layer_output_gradient,
    routes,
    expert_combine_weight,
    expert_gate_weight,
    expert_up_weight,
    expert_down_weight,
    head_mixer_input,
    head_step_size,
    head_decay_rate,
    extra_log_decay,
    state_entering_span,
    state_input_vectors,
    state_readout_vectors,
    gate_preactivation,
    group_norm_scale,
    mixer_output_weight,
):
    local_tokens = routes.shape[0]
    packed = pack(routes, expert_combine_weight, mixer_output_stream, layer_output_gradient, n_sp)
    arrived = dispatch(packed, n_sp, n_tp)
    grad_g, grad_u, grad_d, partial_rows = experts_backward(
        arrived, expert_gate_weight, expert_up_weight, expert_down_weight
    )
    mix_grad = give_back(partial_rows, routes, layer_output_gradient, n_sp, n_tp)

    head_local = head_step_size.shape[1]
    group_local = state_input_vectors.shape[1] // STATE
    input_heads = head_mixer_input.astype(F32).reshape(local_tokens, head_local, HDIM)
    input_vector_groups = state_input_vectors.astype(F32).reshape(local_tokens, group_local, STATE)
    readout_groups = state_readout_vectors.astype(F32).reshape(local_tokens, group_local, STATE)
    within_span_state, within_span_decay = span_final_state(
        input_heads, head_step_size, head_decay_rate, extra_log_decay, input_vector_groups
    )
    part_rows = head_local * HDIM // n_sp
    entering = lax.dynamic_index_in_dim(
        state_entering_span.reshape(n_sp, part_rows, STATE), lax.axis_index(SP), 0, keepdims=False
    )
    incoming_state = carried(
        within_span_state, within_span_decay, entering, n_sp, n_tp, False, 2
    )

    def forward(input_values, time_step_values, input_vector_entries, readout_entries):
        return span_local_scan(
            input_values,
            time_step_values,
            head_decay_rate,
            extra_log_decay,
            input_vector_entries,
            readout_entries,
            incoming_state,
        )

    (scan_out, closing_state), pull_back = jax.vjp(
        forward, input_heads, head_step_size, input_vector_groups, readout_groups
    )

    def apply_norm(scan_vals, gate_vals):
        return gate_norm(scan_vals, gate_vals, group_norm_scale, group_local)

    normed, pull_norm = jax.vjp(apply_norm, scan_out, gate_preactivation.astype(F32))
    normed_low = normed.astype(BF16)
    normed_grad = lax.dot_general(
        mix_grad,
        lax.all_gather(mixer_output_weight, SP, axis=1, tiled=True),
        (((1,), (1,)), ((), ())),
        preferred_element_type=F32,
    )
    scanned_gradient, gate_grad_in = pull_norm(normed_grad)
    reached_gradient = carried_weight(
        scanned_gradient, readout_groups, head_step_size, head_decay_rate, extra_log_decay
    )
    later_grad = carried(
        reached_gradient, within_span_decay, jnp.zeros_like(entering), n_sp, n_tp, True, 3
    )
    input_grad, step_grad, b_grad, c_grad = pull_back((scanned_gradient, later_grad))
    proj_grad = project(normed_low, mix_grad, n_sp, n_tp)
    return (
        grad_g,
        grad_u,
        grad_d,
        proj_grad,
        input_grad.reshape(local_tokens, -1).astype(BF16),
        step_grad,
        b_grad.reshape(local_tokens, -1).astype(BF16),
        c_grad.reshape(local_tokens, -1).astype(BF16),
        gate_grad_in.astype(BF16),
    )


def solution(mesh):
    placed = (
        P(SP, "tp"),
        P(SP, "tp"),
        P(SP, None),
        P(SP, None),
        P(SP, None, "tp"),
        P(SP, None, "tp"),
        P(SP, "tp", None),
        P(SP, "tp"),
        P(SP, "tp"),
        P("tp"),
        P(SP, "tp"),
        P("tp", None, None),
        P(SP, "tp"),
        P(SP, "tp"),
        P(SP, "tp"),
        P("tp"),
        P("tp", SP),
    )
    return jax.shard_map(
        functools.partial(body, mesh.shape["sp"], mesh.shape["tp"]),
        mesh=mesh,
        in_specs=placed,
        out_specs=(
            P(SP, None, "tp"),
            P(SP, None, "tp"),
            P(SP, "tp", None),
            P("tp", SP),
            P(SP, "tp"),
            P(SP, "tp"),
            P(SP, "tp"),
            P(SP, "tp"),
            P(SP, "tp"),
        ),
        check_vma=False,
    )
```

```python
import functools

import jax
import jax.numpy as jnp
from jax import lax
from jax.experimental import pallas as pl
from jax.experimental.pallas import tpu as pltpu
from jax.sharding import PartitionSpec as P

HDIM = 64
STATE = 128
SP = "sp"
CAP = 12
MESH = pl.DeviceIdType.MESH
F32 = jnp.float32
BF16 = jnp.bfloat16

norm_eps = 1e-05
VMEM_BYTES = 60 * 1024 * 1024


def vmem_spec():
    return pl.BlockSpec(memory_space=pltpu.VMEM)


def any_spec():
    return pl.BlockSpec(memory_space=pl.ANY)


def dot(a, b, contract=((1,), (0,))):
    return lax.dot_general(a, b, (contract, ((), ())), preferred_element_type=F32)


def iota(shape, dim):
    return lax.broadcasted_iota(jnp.int32, shape, dim)


def divide(x, by):
    return ((x.astype(F32) + 0.5) * (1.0 / by)).astype(jnp.int32)


def slots_in_rows(routes, experts):
    top, tokens = routes.shape
    ids = iota((experts, tokens), 0)
    earlier = (iota((tokens, tokens), 0) < iota((tokens, tokens), 1)).astype(BF16)
    before = jnp.zeros((experts, 1), F32)
    rows = []
    for k in range(top):
        hits = (ids == routes[k : k + 1, :]).astype(F32)
        rank = dot(hits.astype(BF16), earlier) + before
        rows.append(jnp.sum(hits * rank, axis=0, keepdims=True))
        before = before + jnp.sum(hits, axis=1, keepdims=True)
    return [routes[k : k + 1, :] * CAP + rows[k].astype(jnp.int32) for k in range(top)]


def slots_in_columns(routes, experts):
    tokens, top = routes.shape
    ids = iota((tokens, experts), 1)
    earlier = (iota((tokens, tokens), 1) < iota((tokens, tokens), 0)).astype(BF16)
    before = jnp.zeros((1, experts), F32)
    columns = []
    for k in range(top):
        hits = (ids == routes[:, k : k + 1]).astype(F32)
        rank = dot(earlier, hits.astype(BF16)) + before
        columns.append(jnp.sum(hits * rank, axis=1, keepdims=True))
        before = before + jnp.sum(hits, axis=0, keepdims=True)
    return [routes[:, k : k + 1] * CAP + columns[k].astype(jnp.int32) for k in range(top)]


def pack_kernel(experts, routes_ref, weights_ref, stream_ref, grads_ref, out_ref):
    tokens = stream_ref.shape[0]
    half = stream_ref.shape[1] // 2
    slots = slots_in_rows(routes_ref[...], experts)
    row = iota((experts * 4 * CAP, 1), 0)
    expert = divide(row, 4 * CAP)
    inner = row - expert * (4 * CAP)
    part = divide(inner, CAP)
    slot = expert * CAP + inner - part * CAP
    first = (slot == slots[0]).astype(F32)
    second = (slot == slots[1]).astype(F32)
    match = (first + second).astype(BF16)
    weight = jnp.sum(
        first * weights_ref[0:1, :] + second * weights_ref[1:2, :], axis=1, keepdims=True
    )
    x0 = dot(match, stream_ref[:, :half])
    x1 = dot(match, stream_ref[:, half:])
    g0 = dot(match, grads_ref[:, :half])
    g1 = dot(match, grads_ref[:, half:])
    low = jnp.where(part == 0, x0, g0 * weight)
    high = jnp.where(part == 2, x1, g1 * weight)
    out_ref[...] = jnp.where(part < 2, low, high).astype(BF16)


def pack(routes, weights, stream, grads, experts):
    half = stream.shape[1] // 2
    packed = pl.pallas_call(
        functools.partial(pack_kernel, experts),
        out_shape=jax.ShapeDtypeStruct((experts * 4 * CAP, half), BF16),
        in_specs=[vmem_spec()] * 4,
        out_specs=vmem_spec(),
        compiler_params=pltpu.CompilerParams(vmem_limit_bytes=VMEM_BYTES),
        name="pack",
    )(routes.T, weights.T, stream, grads)
    return packed.reshape(experts, 4 * CAP, half)


def greet(me, tp, n_sp, n_tp, step=1, ring=False, partner=None):
    barrier = pltpu.get_barrier_semaphore()

    def hello(d, carry):
        pl.semaphore_signal(
            barrier, inc=1, device_id=(lax.rem(me + d * step, n_sp), tp), device_id_type=MESH
        )
        return carry

    lax.fori_loop(1, n_sp // step, hello, 0)
    count = n_sp // step - 1
    if partner is not None:
        pl.semaphore_signal(barrier, inc=1, device_id=(partner, tp), device_id_type=MESH)
        count += 1
    if ring:
        for other in (lax.rem(tp + 1, n_tp), lax.rem(tp + n_tp - 1, n_tp)):
            pl.semaphore_signal(barrier, inc=1, device_id=(me, other), device_id_type=MESH)
        count += 2
    pl.semaphore_wait(barrier, count)


def split(x, pieces):
    terms = []
    for _ in range(pieces):
        term = x.astype(BF16)
        terms.append(term)
        x = x - term.astype(F32)
    return terms


def dot_split(x, exact, pieces, contract, left=True):
    total = None
    for term in split(x, pieces):
        part = dot(term, exact, contract) if left else dot(exact, term, contract)
        total = part if total is None else total + part
    return total


def triangle(n, keep):
    return keep(iota((n, n), 0), iota((n, n), 1)).astype(BF16)


def head_spread(heads, size):
    channel, head = iota((heads, heads * size), 1), iota((heads, heads * size), 0)
    return ((channel >= head * size) & (channel < (head + 1) * size)).astype(BF16)


def spread(x, owner):
    return dot_split(x, owner, 2, ((1,), (0,)))


def by_head(x, owner):
    return dot_split(x, owner, 2, ((1,), (1,)))


def cumulative_decay(time_step, rate, extra):
    log_decay = extra - time_step * rate
    upto = triangle(log_decay.shape[0], lambda t, s: s <= t)
    return dot_split(log_decay, upto, 3, ((1,), (0,)), left=False)


def in_rows(x):
    n = x.shape[1]
    return dot_split(x, triangle(n, lambda a, b: a == b), 3, ((1,), (1,)), left=False)


def decay_between(cum, cum_rows, h):
    gap = cum[:, h : h + 1] - cum_rows[h : h + 1, :]
    n = gap.shape[0]
    return jnp.exp(jnp.where(iota((n, n), 1) <= iota((n, n), 0), gap, -1e30))


def halves(pair):
    lane = iota(pair.shape, 1)
    zero = jnp.zeros_like(pair)
    size = pair.shape[1] // 2
    return jnp.concatenate([jnp.where(lane < size, pair, zero), jnp.where(lane < size, zero, pair)], axis=0)


def front_kernel(
    n_sp,
    n_tp,
    in_ref,
    x_ref,
    dt_ref,
    rate_ref,
    extra_ref,
    first_ref,
    b_ref,
    c_ref,
    gate_ref,
    scale_ref,
    out_ref,
    y_ref,
    normed_ref,
    coming,
    state_mine,
    decay_mine,
    states,
    decays,
    carries,
    diag,
    own,
    one,
    two,
    a_send,
    a_recv,
    s_right,
    s_left,
    r_left,
    r_right,
    f_send,
    f_recv,
    sends,
    recvs,
    d_sends,
    d_recvs,
    b_sends,
    b_recvs,
):
    me, tp = lax.axis_index("sp"), lax.axis_index("tp")
    right, left = lax.rem(tp + 1, n_tp), lax.rem(tp + n_tp - 1, n_tp)
    far = lax.rem(tp + 2, n_tp)
    greet(me, tp, n_sp, n_tp, ring=True)

    def origin(d):
        return lax.rem(me + n_sp - d, n_sp)

    def exchange(d):
        to = lax.rem(me + d, n_sp)
        return pltpu.make_async_remote_copy(
            in_ref.at[to], out_ref.at[tp, me], a_send.at[d], a_recv.at[d], (to, tp), MESH
        )

    def arrived(d):
        return pltpu.make_async_remote_copy(
            in_ref.at[me], out_ref.at[tp, origin(d)], a_send.at[d], a_recv.at[d], (me, tp), MESH
        )

    def to_right(d, block):
        piece = out_ref.at[block, origin(d)]
        return pltpu.make_async_remote_copy(
            piece, piece, s_right.at[d], r_left.at[d], (me, right), MESH
        )

    def to_left(d, block):
        piece = out_ref.at[block, origin(d)]
        return pltpu.make_async_remote_copy(
            piece, piece, s_left.at[d], r_right.at[d], (me, left), MESH
        )

    def onward(d, block, to):
        piece = out_ref.at[block, origin(d)]
        return pltpu.make_async_remote_copy(
            piece, piece, f_send.at[d], f_recv.at[d], (me, to), MESH
        )

    def start_exchange(d, carry):
        exchange(d).start()
        return carry

    lax.fori_loop(1, n_sp, start_exchange, 0)
    mine = pltpu.make_async_copy(in_ref.at[me], out_ref.at[tp, me], own)
    mine.start()

    tokens, heads = dt_ref.shape
    channels = x_ref.shape[1]
    groups = b_ref.shape[1] // STATE
    wide = channels // groups
    owner = head_spread(heads, HDIM)
    dt = dt_ref[...]
    cum = cumulative_decay(dt, rate_ref[...], extra_ref[...])
    cum_rows = in_rows(cum)
    last = cum[tokens - 1 : tokens, :]
    values = x_ref[...].astype(F32)
    ending = (values * spread(dt * jnp.exp(last - cum), owner)).astype(BF16)
    parts, rows, entries = state_mine.shape
    per_group = parts // groups
    for g in range(groups):
        state = dot(
            ending[:, g * wide : (g + 1) * wide],
            b_ref[:, g * STATE : (g + 1) * STATE],
            ((0,), (0,)),
        )
        state_mine[g * per_group : (g + 1) * per_group] = state.astype(BF16).reshape(
            per_group, rows, entries
        )
    total = jnp.exp(last)
    for p in range(parts):
        h = p * rows // HDIM
        decay_mine[p] = jnp.broadcast_to(total[:, h : h + 1], (1, entries))

    mine.wait()
    to_right(0, tp).start()
    to_left(0, tp).start()

    def state_copy(d):
        to = lax.rem(me + d, n_sp)
        return pltpu.make_async_remote_copy(
            state_mine.at[to], states.at[me], sends.at[d], recvs.at[d], (to, tp), MESH
        )

    def decay_copy(d):
        to = lax.rem(me + d, n_sp)
        return pltpu.make_async_remote_copy(
            decay_mine.at[to], decays.at[me], d_sends.at[d], d_recvs.at[d], (to, tp), MESH
        )

    def back_copy(d):
        to = lax.rem(me + d, n_sp)
        return pltpu.make_async_remote_copy(
            carries.at[to], coming.at[me], b_sends.at[d], b_recvs.at[d], (to, tp), MESH
        )

    def start_states(d, carry):
        decay_copy(d).start()
        state_copy(d).start()
        return carry

    lax.fori_loop(1, n_sp, start_states, 0)
    kept = pltpu.make_async_copy(state_mine.at[me], states.at[me], one)
    kept_too = pltpu.make_async_copy(decay_mine.at[me], decays.at[me], two)
    kept.start()
    kept_too.start()

    def spread_out(d, carry):
        arrived(d).wait_recv()
        to_right(d, tp).start()
        to_left(d, tp).start()
        return carry

    lax.fori_loop(1, n_sp, spread_out, 0)

    scaled = (values * spread(dt, owner)).astype(BF16)
    affinity = [
        dot(
            c_ref[:, g * STATE : (g + 1) * STATE],
            b_ref[:, g * STATE : (g + 1) * STATE],
            ((1,), (1,)),
        )
        for g in range(groups)
    ]
    for q in range(heads // 2):
        g = q // (heads // 2 // groups)
        both = jnp.concatenate(
            [(affinity[g] * decay_between(cum, cum_rows, 2 * q + j)).astype(BF16) for j in range(2)],
            axis=1,
        )
        at = slice(q * 2 * HDIM, (q + 1) * 2 * HDIM)
        diag[:, at] = dot(both, halves(scaled[:, at]))

    kept.wait()
    kept_too.wait()

    def finish_states(d, carry):
        decay_copy(d).wait()
        state_copy(d).wait()
        return carry

    lax.fori_loop(1, n_sp, finish_states, 0)
    running = first_ref[...]
    for i in range(n_sp):
        carries[i] = running.astype(BF16)
        running = decays[i] * running + states[i].astype(F32)

    def start_back(d, carry):
        back_copy(d).start()
        return carry

    lax.fori_loop(1, n_sp, start_back, 0)
    kept_back = pltpu.make_async_copy(carries.at[me], coming.at[me], one)
    kept_back.start()

    def relay(q, carry):
        d = 2 * q
        to_right(d, left).wait_recv()
        onward(d, left, right).start()
        to_left(d + 1, right).wait_recv()
        onward(d + 1, right, left).start()
        return carry

    lax.fori_loop(0, n_sp // 2, relay, 0)
    kept_back.wait()

    def finish_back(d, carry):
        back_copy(d).wait()
        return carry

    lax.fori_loop(1, n_sp, finish_back, 0)
    since = spread(jnp.exp(cum), owner)
    for g in range(groups):
        at = slice(g * wide, (g + 1) * wide)
        incoming = coming[g * per_group : (g + 1) * per_group].reshape(wide, entries)
        y = diag[:, at] + since[:, at] * dot(
            c_ref[:, g * STATE : (g + 1) * STATE], incoming, ((1,), (1,))
        )
        y_ref[:, at] = y
        gate = gate_ref[:, at].astype(F32)
        gated = y * gate * jax.nn.sigmoid(gate)
        factor = lax.rsqrt(jnp.mean(gated * gated, axis=1, keepdims=True) + norm_eps)
        normed_ref[:, at] = (gated * factor * scale_ref[:, at]).astype(BF16)

    def finish(q, carry):
        d = 2 * q
        to_left(d, right).wait_recv()
        to_right(d + 1, left).wait_recv()
        onward(d, far, right).wait()
        onward(d + 1, far, left).wait()
        to_right(d, tp).wait_send()
        to_left(d, tp).wait_send()
        to_right(d + 1, tp).wait_send()
        to_left(d + 1, tp).wait_send()
        return carry

    lax.fori_loop(0, n_sp // 2, finish, 0)

    def drain(d, carry):
        exchange(d).wait_send()
        return carry

    lax.fori_loop(1, n_sp, drain, 0)


def front(packed, x, dt, rate, extra, first, b, c, gate, scale, n_sp, n_tp):
    dma = pltpu.SemaphoreType.DMA
    tokens, channels = x.shape
    rows, entries = first.shape
    return pl.pallas_call(
        functools.partial(front_kernel, n_sp, n_tp),
        out_shape=(
            jax.ShapeDtypeStruct((n_tp,) + packed.shape, BF16),
            jax.ShapeDtypeStruct((tokens, channels), F32),
            jax.ShapeDtypeStruct((tokens, channels), BF16),
            jax.ShapeDtypeStruct((n_sp, rows, entries), BF16),
        ),
        in_specs=[vmem_spec()] * 10,
        out_specs=(vmem_spec(),) * 4,
        scratch_shapes=[
            pltpu.VMEM((n_sp, rows, entries), BF16),
            pltpu.VMEM((n_sp, 1, entries), F32),
            pltpu.VMEM((n_sp, rows, entries), BF16),
            pltpu.VMEM((n_sp, 1, entries), F32),
            pltpu.VMEM((n_sp, rows, entries), BF16),
            pltpu.VMEM((tokens, channels), F32),
            dma,
            dma,
            dma,
        ]
        + [dma((n_sp,))] * 14,
        compiler_params=pltpu.CompilerParams(
            collective_id=0, has_side_effects=True, vmem_limit_bytes=VMEM_BYTES
        ),
        name="front",
    )(packed, x, dt, rate, extra, first, b, c, gate, scale)


def expert_kernel(
    n_sp,
    n_tp,
    in_ref,
    gate_hbm,
    up_hbm,
    down_hbm,
    routes_ref,
    grads_ref,
    mix_ref,
    dgate_hbm,
    dup_hbm,
    ddown_hbm,
    w_gate,
    w_up,
    w_down,
    d_gate,
    d_up,
    d_down,
    x,
    x_t,
    g,
    gate_grad,
    up_grad,
    hidden,
    part_ref,
    from_left,
    from_right,
    sum_right,
    sum_left,
    out_blocks,
    back,
    own_cols,
    loads,
    stores,
    s_r,
    s_l,
    r_l,
    r_r,
    a_send,
    a_recv,
    g_send,
    g_recv,
    local,
):
    me, tp = lax.axis_index("sp"), lax.axis_index("tp")
    right, left = lax.rem(tp + 1, n_tp), lax.rem(tp + n_tp - 1, n_tp)
    far = lax.rem(tp + 2, n_tp)
    tokens, width = grads_ref.shape
    half, quarter = width // 2, width // 4
    model, units = w_gate.shape
    rows = x.shape[0]
    cuts = [(i, min(256, units - i)) for i in range(0, units, 256)]
    fetches = []
    for k, (start, size) in enumerate(cuts):
        at = pl.ds(start, size)
        fetches.append(
            [
                pltpu.make_async_copy(gate_hbm.at[0, :, at], w_gate.at[:, at], loads.at[3 * k]),
                pltpu.make_async_copy(up_hbm.at[0, :, at], w_up.at[:, at], loads.at[3 * k + 1]),
                pltpu.make_async_copy(down_hbm.at[0, at, :], w_down.at[at, :], loads.at[3 * k + 2]),
            ]
        )
        for fetch in fetches[-1]:
            fetch.start()
    greet(me, tp, n_sp, n_tp, ring=True)

    tall = in_ref.shape[2]
    group_of = 8
    span = group_of * CAP
    spots = iota((1, group_of * tall), 1)
    src = divide(spots, tall)
    inner = spots - src * tall
    which = divide(inner, CAP)
    row = src * CAP + inner - which * CAP
    lines = iota((span, 1), 0)
    pick = [((row == lines) & (which == p)).astype(BF16) for p in range(4)]
    for t in range(n_tp):
        for k in range(n_sp // group_of):
            block = in_ref[t, k * group_of : (k + 1) * group_of].reshape(group_of * tall, half)
            at = slice(k * span, (k + 1) * span)
            for c in range(2):
                cols = slice((2 * t + c) * half, (2 * t + c + 1) * half)
                x[at, cols] = dot(pick[2 * c], block).astype(BF16)
                g[at, cols] = dot(pick[2 * c + 1], block).astype(BF16)

    for k, (start, size) in enumerate(cuts):
        for fetch in fetches[k]:
            fetch.wait()
        at = slice(start, start + size)
        pre_gate = dot(x[...], w_gate[:, at])
        pre_up = dot(x[...], w_up[:, at])
        hidden_grad = dot(g[...], w_down[at, :], ((1,), (1,)))
        sigmoid_gate = jax.nn.sigmoid(pre_gate)
        activated = pre_gate * sigmoid_gate
        hidden[:, at] = (activated * pre_up).astype(BF16)
        gate_grad[:, at] = (
            hidden_grad * pre_up * sigmoid_gate * (1.0 + pre_gate * (1.0 - sigmoid_gate))
        ).astype(BF16)
        up_grad[:, at] = (hidden_grad * activated).astype(BF16)

    def row_block(b):
        for c in range(2):
            cols = pl.ds(pl.multiple_of(b * width + c * half, half), half)
            part_ref[2 * b + c] = (
                dot(gate_grad[...], w_gate[cols, :], ((1,), (1,)))
                + dot(up_grad[...], w_up[cols, :], ((1,), (1,)))
            ).astype(BF16)

    def block(b, which):
        return part_ref.at[2 * b + which]

    def right_copy(k, src):
        return pltpu.make_async_remote_copy(
            src, from_left.at[k], s_r.at[k], r_l.at[k], (me, right), MESH
        )

    def left_copy(k, src):
        return pltpu.make_async_remote_copy(
            src, from_right.at[k], s_l.at[k], r_r.at[k], (me, left), MESH
        )

    row_block(far)
    row_block(right)
    right_copy(0, block(far, 0)).start()
    left_copy(0, block(far, 1)).start()
    row_block(left)
    right_copy(1, block(right, 1)).start()
    row_block(tp)
    left_copy(1, block(left, 0)).start()

    saves = []

    def save(k, src, dst):
        copy = pltpu.make_async_copy(src, dst, stores.at[k])
        copy.start()
        saves.append(copy)

    def passed_right():
        right_copy(0, block(far, 0)).wait()
        sum_right[...] = (block(right, 0)[...].astype(F32) + from_left[0].astype(F32)).astype(BF16)
        left_copy(0, block(far, 1)).wait()
        sum_left[...] = (block(left, 1)[...].astype(F32) + from_right[0].astype(F32)).astype(BF16)

    def gate_up_rows(i):
        at = slice(i * 256, (i + 1) * 256)
        x_t[at, :] = jnp.transpose(x[:, at])
        d_gate[at, :] = dot(x_t[at, :], gate_grad[...]).astype(BF16)
        save(2 * i, d_gate.at[at, :], dgate_hbm.at[0, at, :])
        d_up[at, :] = dot(x_t[at, :], up_grad[...]).astype(BF16)
        save(2 * i + 1, d_up.at[at, :], dup_hbm.at[0, at, :])

    for i in range(4):
        gate_up_rows(i)
    passed_right()
    right_copy(2, sum_right).start()
    left_copy(2, sum_left).start()
    for i in range(4, 8):
        gate_up_rows(i)

    for k, (start, size) in enumerate(cuts):
        at = slice(start, start + size)
        d_down[at, :] = dot(hidden[:, at], g[...], ((0,), (0,))).astype(BF16)
        save(16 + k, d_down.at[at, :], ddown_hbm.at[0, at, :])

    slots = slots_in_columns(routes_ref[...], n_sp)
    column = iota((1, n_sp * 4 * CAP), 1)
    expert = divide(column, 4 * CAP)
    place_in = column - expert * (4 * CAP)
    piece = divide(place_in, CAP)
    slot = expert * CAP + place_in - piece * CAP
    match = (slots[0] == slot) | (slots[1] == slot)

    right_copy(1, block(right, 1)).wait()
    left_copy(1, block(left, 0)).wait()
    right_copy(2, sum_right).wait()
    left_copy(2, sum_left).wait()

    tall_out = iota((group_of * 4 * CAP, 1), 0)
    out_src = divide(tall_out, 4 * CAP)
    out_in = tall_out - out_src * (4 * CAP)
    out_piece = divide(out_in, CAP)
    out_row = out_src * CAP + out_in - out_piece * CAP
    pair_at = iota((1, span), 1)
    place = [((out_row == pair_at) & (out_piece == c)).astype(BF16) for c in range(4)]
    for k in range(rows // span):
        at = slice(k * span, (k + 1) * span)
        low = (
            part_ref[2 * tp, at, :].astype(F32)
            + from_left[2, at, :].astype(F32)
            + from_right[1, at, :].astype(F32)
        ).astype(BF16)
        high = (
            part_ref[2 * tp + 1, at, :].astype(F32)
            + from_right[2, at, :].astype(F32)
            + from_left[1, at, :].astype(F32)
        ).astype(BF16)
        laid = (
            dot(place[0], low[:, :quarter])
            + dot(place[1], low[:, quarter:])
            + dot(place[2], high[:, :quarter])
            + dot(place[3], high[:, quarter:])
        )
        out_blocks[k * group_of : (k + 1) * group_of] = laid.astype(BF16).reshape(
            group_of, 4 * CAP, quarter
        )

    def exchange(d):
        to = lax.rem(me + d, n_sp)
        return pltpu.make_async_remote_copy(
            out_blocks.at[to], back.at[me], a_send.at[d], a_recv.at[d], (to, tp), MESH
        )

    def start_exchange(d, carry):
        exchange(d).start()
        return carry

    lax.fori_loop(1, n_sp, start_exchange, 0)
    mine = pltpu.make_async_copy(out_blocks.at[me], back.at[me], local)
    mine.start()
    mine.wait()

    def finish_exchange(d, carry):
        exchange(d).wait()
        return carry

    lax.fori_loop(1, n_sp, finish_exchange, 0)
    returned = back[...].reshape(n_sp * 4 * CAP, quarter)
    for c in range(4):
        chosen = jnp.where(match & (piece == c), 1.0, 0.0).astype(BF16)
        cols = slice(c * quarter, (c + 1) * quarter)
        own_cols[:, cols] = (grads_ref[:, cols].astype(F32) + dot(chosen, returned)).astype(BF16)

    def spot(b):
        return mix_ref.at[:, pl.ds(pl.multiple_of(b * width, width), width)]

    def spot_half(b, which):
        return mix_ref.at[:, pl.ds(pl.multiple_of(b * width + which * half, half), half)]

    def gather(k, src, dst, to):
        return pltpu.make_async_remote_copy(
            src, dst, g_send.at[k], g_recv.at[k], (me, to), MESH
        )

    gather(0, own_cols, spot(tp), right).start()
    gather(1, own_cols, spot(tp), left).start()
    spot(tp)[...] = own_cols[...]
    gather(0, own_cols, spot(left), right).wait_recv()
    gather(2, spot_half(left, 0), spot_half(left, 0), right).start()
    gather(1, own_cols, spot(right), left).wait_recv()
    gather(3, spot_half(right, 1), spot_half(right, 1), left).start()
    gather(2, spot_half(far, 0), spot_half(far, 0), right).wait()
    gather(3, spot_half(far, 1), spot_half(far, 1), left).wait()
    gather(0, own_cols, spot(tp), right).wait_send()
    gather(1, own_cols, spot(tp), left).wait_send()
    for copy in saves:
        copy.wait()


def experts_backward(arrived, w_gate, w_up, w_down, routes, grads, n_sp, n_tp):
    _, model, units = w_gate.shape
    rows = n_sp * CAP
    tokens, width = grads.shape
    half, quarter = width // 2, width // 4
    dma = pltpu.SemaphoreType.DMA
    return pl.pallas_call(
        functools.partial(expert_kernel, n_sp, n_tp),
        out_shape=(
            jax.ShapeDtypeStruct((tokens, width * n_tp), BF16),
            jax.ShapeDtypeStruct(w_gate.shape, BF16),
            jax.ShapeDtypeStruct(w_up.shape, BF16),
            jax.ShapeDtypeStruct(w_down.shape, BF16),
        ),
        in_specs=[vmem_spec()] + [any_spec()] * 3 + [vmem_spec()] * 2,
        out_specs=(vmem_spec(),) + (any_spec(),) * 3,
        scratch_shapes=[
            pltpu.VMEM((model, units), BF16),
            pltpu.VMEM((model, units), BF16),
            pltpu.VMEM((units, model), BF16),
            pltpu.VMEM((model, units), BF16),
            pltpu.VMEM((model, units), BF16),
            pltpu.VMEM((units, model), BF16),
            pltpu.VMEM((rows, model), BF16),
            pltpu.VMEM((model, rows), BF16),
            pltpu.VMEM((rows, model), BF16),
            pltpu.VMEM((rows, units), BF16),
            pltpu.VMEM((rows, units), BF16),
            pltpu.VMEM((rows, units), BF16),
            pltpu.VMEM((2 * n_tp, rows, half), BF16),
            pltpu.VMEM((3, rows, half), BF16),
            pltpu.VMEM((3, rows, half), BF16),
            pltpu.VMEM((rows, half), BF16),
            pltpu.VMEM((rows, half), BF16),
            pltpu.VMEM((n_sp, 4 * CAP, quarter), BF16),
            pltpu.VMEM((n_sp, 4 * CAP, quarter), BF16),
            pltpu.VMEM((tokens, width), BF16),
            dma((12,)),
            dma((20,)),
            dma((3,)),
            dma((3,)),
            dma((3,)),
            dma((3,)),
            dma((n_sp,)),
            dma((n_sp,)),
            dma((4,)),
            dma((4,)),
            dma,
        ],
        compiler_params=pltpu.CompilerParams(
            collective_id=1, has_side_effects=True, vmem_limit_bytes=VMEM_BYTES
        ),
        name="experts",
    )(arrived, w_gate, w_up, w_down, routes, grads)


def tail_kernel(
    n_sp,
    n_tp,
    mix_ref,
    weight_hbm,
    y_ref,
    normed_ref,
    x_ref,
    dt_ref,
    rate_ref,
    extra_ref,
    coming_ref,
    b_ref,
    c_ref,
    gate_ref,
    scale_ref,
    proj_ref,
    dx_ref,
    ddt_ref,
    db_ref,
    dc_ref,
    dgate_ref,
    weight,
    normed2,
    mix2,
    parts,
    landed,
    total,
    other,
    state_mine,
    decay_mine,
    states,
    decays,
    carries,
    later,
    d_scaled,
    one,
    two,
    load,
    p_send,
    p_recv,
    a_send,
    a_recv,
    sends,
    recvs,
    d_sends,
    d_recvs,
    b_sends,
    b_recvs,
):
    me, tp = lax.axis_index("sp"), lax.axis_index("tp")
    core = lax.rem(me, 2)
    partner = me + 1 - 2 * core
    chip = lax.div(me, 2)
    chips = n_sp // 2
    fetch = pltpu.make_async_copy(weight_hbm, weight, load)
    fetch.start()
    greet(me, tp, n_sp, n_tp)
    tokens, heads = dt_ref.shape
    channels = x_ref.shape[1]
    groups = b_ref.shape[1] // STATE
    wide = channels // groups
    half = channels // 2
    cols = proj_ref.shape[1]
    n_parts, rows, entries = state_mine.shape
    per_group = n_parts // groups

    def pair(k, src, dst):
        return pltpu.make_async_remote_copy(
            src, dst, p_send.at[k], p_recv.at[k], (partner, tp), MESH
        )

    def mine(c):
        return pl.ds(pl.multiple_of(c * half, half), half)

    pair(0, normed_ref.at[:, mine(1 - core)], normed2).start()
    pair(1, mix_ref, mix2).start()

    owner = head_spread(heads, HDIM)
    dt = dt_ref[...]
    cum = cumulative_decay(dt, rate_ref[...], extra_ref[...])
    cum_rows = in_rows(cum)
    last = cum[tokens - 1 : tokens, :]
    since = spread(jnp.exp(cum), owner)
    fetch.wait()
    d_y = []
    for g in range(groups):
        at = slice(g * wide, (g + 1) * wide)
        normed_grad = dot(mix_ref[...], weight[at, :], ((1,), (1,)))
        y = y_ref[:, at]
        gate = gate_ref[:, at].astype(F32)
        sigmoid_gate = jax.nn.sigmoid(gate)
        activated = gate * sigmoid_gate
        gated = y * activated
        factor = lax.rsqrt(jnp.mean(gated * gated, axis=1, keepdims=True) + norm_eps)
        scaled_grad = normed_grad * scale_ref[:, at]
        along = jnp.mean(scaled_grad * gated, axis=1, keepdims=True) * factor * factor
        gated_grad = factor * (scaled_grad - gated * along)
        d_y.append(gated_grad * activated)
        dgate_ref[:, at] = (
            gated_grad * y * (sigmoid_gate * (1.0 + gate * (1.0 - sigmoid_gate)))
        ).astype(BF16)
    d_out = jnp.concatenate(d_y, axis=1)
    since_grad = since * d_out
    since_low = since_grad.astype(BF16)
    for g in range(groups):
        state = dot(
            since_low[:, g * wide : (g + 1) * wide],
            c_ref[:, g * STATE : (g + 1) * STATE],
            ((0,), (0,)),
        )
        state_mine[g * per_group : (g + 1) * per_group] = state.astype(BF16).reshape(
            per_group, rows, entries
        )
    whole = jnp.exp(last)
    for p in range(n_parts):
        h = p * rows // HDIM
        decay_mine[p] = jnp.broadcast_to(whole[:, h : h + 1], (1, entries))

    def state_copy(d):
        to = lax.rem(me + d, n_sp)
        return pltpu.make_async_remote_copy(
            state_mine.at[to], states.at[me], sends.at[d], recvs.at[d], (to, tp), MESH
        )

    def decay_copy(d):
        to = lax.rem(me + d, n_sp)
        return pltpu.make_async_remote_copy(
            decay_mine.at[to], decays.at[me], d_sends.at[d], d_recvs.at[d], (to, tp), MESH
        )

    def back_copy(d):
        to = lax.rem(me + d, n_sp)
        return pltpu.make_async_remote_copy(
            carries.at[to], later.at[me], b_sends.at[d], b_recvs.at[d], (to, tp), MESH
        )

    def start_states(d, carry):
        decay_copy(d).start()
        state_copy(d).start()
        return carry

    lax.fori_loop(1, n_sp, start_states, 0)
    kept = pltpu.make_async_copy(state_mine.at[me], states.at[me], one)
    kept_too = pltpu.make_async_copy(decay_mine.at[me], decays.at[me], two)
    kept.start()
    kept_too.start()

    pair(0, normed_ref.at[:, mine(1 - core)], normed2).wait()
    pair(1, mix_ref, mix2).wait()
    own_t = jnp.transpose(normed_ref[:, mine(core)])
    other_t = jnp.transpose(normed2[...])
    for c in range(chips):
        at = slice(c * 2 * cols, (c + 1) * 2 * cols)
        parts[c] = (dot(own_t, mix_ref[:, at]) + dot(other_t, mix2[:, at])).astype(BF16)

    def exchange(d):
        to = lax.rem(chip + d, chips)
        return pltpu.make_async_remote_copy(
            parts.at[to], landed.at[chip], a_send.at[d], a_recv.at[d], (2 * to + core, tp), MESH
        )

    def start_parts(d, carry):
        exchange(d).start()
        return carry

    kept.wait()
    kept_too.wait()

    def finish_states(d, carry):
        decay_copy(d).wait()
        state_copy(d).wait()
        return carry

    lax.fori_loop(1, n_sp, finish_states, 0)
    running = jnp.zeros((rows, entries), F32)
    for step in range(n_sp):
        i = n_sp - 1 - step
        carries[i] = running.astype(BF16)
        running = decays[i] * running + states[i].astype(F32)

    def start_back(d, carry):
        back_copy(d).start()
        return carry

    lax.fori_loop(1, n_sp, start_back, 0)
    lax.fori_loop(1, chips, start_parts, 0)
    kept_back = pltpu.make_async_copy(carries.at[me], later.at[me], one)
    kept_back.start()

    values = x_ref[...].astype(F32)
    steps = spread(dt, owner)
    scaled = values * steps
    scaled_low = scaled.astype(BF16)
    d_low = d_out.astype(BF16)
    not_before = triangle(tokens, lambda t, s: s >= t)
    below = (iota((tokens, tokens), 1) < iota((tokens, tokens), 0)).astype(F32)
    head_lane = iota((1, heads), 1)
    crossing = jnp.zeros((tokens, heads), F32)
    d_affinity = []
    for g in range(groups):
        affinity = dot(
            c_ref[:, g * STATE : (g + 1) * STATE],
            b_ref[:, g * STATE : (g + 1) * STATE],
            ((1,), (1,)),
        )
        sum_affinity = jnp.zeros((tokens, tokens), F32)
        first = g * (heads // 2 // groups)
        for q in range(first, first + heads // 2 // groups):
            at = slice(q * 2 * HDIM, (q + 1) * 2 * HDIM)
            d_halves = halves(d_low[:, at])
            d_weights = dot(d_halves, scaled_low[:, at], ((1,), (1,)))
            weights, moved = [], []
            for j in range(2):
                between = decay_between(cum, cum_rows, 2 * q + j)
                weights.append((affinity * between).astype(BF16))
                d_between = d_weights[j * tokens : (j + 1) * tokens] * between
                sum_affinity = sum_affinity + d_between
                moved.append((d_between * affinity).astype(BF16))
            d_scaled[:, at] = dot(jnp.concatenate(weights, axis=0), d_halves, ((0,), (0,)))
            reach = dot(not_before, jnp.concatenate(moved, axis=1))
            for j in range(2):
                over = jnp.sum(
                    reach[:, j * tokens : (j + 1) * tokens] * below, axis=1, keepdims=True
                )
                crossing = crossing + jnp.where(head_lane == 2 * q + j, over, 0.0)
        d_affinity.append(sum_affinity.astype(BF16))
    read_out = []
    for g in range(groups):
        at = slice(g * wide, (g + 1) * wide)
        by = slice(g * STATE, (g + 1) * STATE)
        incoming = coming_ref[g * per_group : (g + 1) * per_group].reshape(wide, entries)
        read_out.append(dot(c_ref[:, by], incoming, ((1,), (1,))))
        dc_ref[:, by] = (
            dot(d_affinity[g], b_ref[:, by]) + dot(since_low[:, at], incoming)
        ).astype(BF16)
    reading = by_head(since_grad * jnp.concatenate(read_out, axis=1), owner)

    kept_back.wait()

    def finish_back(d, carry):
        back_copy(d).wait()
        return carry

    lax.fori_loop(1, n_sp, finish_back, 0)
    until = spread(jnp.exp(last - cum), owner)
    ending = scaled * until
    ending_low = ending.astype(BF16)
    from_later = []
    for g in range(groups):
        at = slice(g * wide, (g + 1) * wide)
        by = slice(g * STATE, (g + 1) * STATE)
        after = later[g * per_group : (g + 1) * per_group].reshape(wide, entries)
        from_later.append(dot(b_ref[:, by], after, ((1,), (1,))))
        db_ref[:, by] = (
            dot(d_affinity[g], c_ref[:, by], ((0,), (0,))) + dot(ending_low[:, at], after)
        ).astype(BF16)
    closing = jnp.concatenate(from_later, axis=1)
    gradient = d_scaled[...] + until * closing
    dx_ref[...] = (gradient * steps).astype(BF16)
    direct = by_head(gradient * values, owner)
    stored = by_head(ending * closing, owner)
    kept_state = jnp.sum(
        (
            coming_ref[...].astype(F32).reshape(heads, HDIM, entries)
            * later[...].astype(F32).reshape(heads, HDIM, entries)
        ),
        axis=1,
    )
    passing = dot_split(
        kept_state, jnp.ones((8, entries), BF16), 3, ((1,), (1,)), left=False
    )[0:1, :]
    earlier = triangle(tokens, lambda t, s: s < t)
    d_decay = (
        crossing
        + dot_split(reading, not_before, 3, ((1,), (0,)), left=False)
        + dot_split(stored, earlier, 3, ((1,), (0,)), left=False)
        + passing * whole
    )
    ddt_ref[...] = direct - d_decay * rate_ref[...]

    total[...] = parts[chip].astype(F32)

    def finish_parts(d, carry):
        exchange(d).wait()
        total[...] += landed[lax.rem(chip + chips - d, chips)].astype(F32)
        return carry

    lax.fori_loop(1, chips, finish_parts, 0)
    pair(2, total, other).start()
    proj_ref[mine(core), :] = jnp.where(core == 0, total[:, :cols], total[:, cols:])
    pair(2, total, other).wait()
    proj_ref[mine(1 - core), :] = jnp.where(core == 0, other[:, :cols], other[:, cols:])


def tail(mix, weight, y, normed, x, dt, rate, extra, coming, b, c, gate, scale, n_sp, n_tp):
    dma = pltpu.SemaphoreType.DMA
    tokens, channels = x.shape
    heads = dt.shape[1]
    _, rows, entries = coming.shape
    width = mix.shape[1]
    half = channels // 2
    chips = n_sp // 2
    cols = width // n_sp
    return pl.pallas_call(
        functools.partial(tail_kernel, n_sp, n_tp),
        out_shape=(
            jax.ShapeDtypeStruct((channels, cols), F32),
            jax.ShapeDtypeStruct((tokens, channels), BF16),
            jax.ShapeDtypeStruct((tokens, heads), F32),
            jax.ShapeDtypeStruct(b.shape, BF16),
            jax.ShapeDtypeStruct(c.shape, BF16),
            jax.ShapeDtypeStruct((tokens, channels), BF16),
        ),
        in_specs=[vmem_spec(), any_spec()] + [vmem_spec()] * 11,
        out_specs=(vmem_spec(),) * 6,
        scratch_shapes=[
            pltpu.VMEM((channels, width), BF16),
            pltpu.VMEM((tokens, half), BF16),
            pltpu.VMEM((tokens, width), BF16),
            pltpu.VMEM((chips, half, 2 * cols), BF16),
            pltpu.VMEM((chips, half, 2 * cols), BF16),
            pltpu.VMEM((half, 2 * cols), F32),
            pltpu.VMEM((half, 2 * cols), F32),
            pltpu.VMEM((n_sp, rows, entries), BF16),
            pltpu.VMEM((n_sp, 1, entries), F32),
            pltpu.VMEM((n_sp, rows, entries), BF16),
            pltpu.VMEM((n_sp, 1, entries), F32),
            pltpu.VMEM((n_sp, rows, entries), BF16),
            pltpu.VMEM((n_sp, rows, entries), BF16),
            pltpu.VMEM((tokens, channels), F32),
            dma,
            dma,
            dma,
            dma((3,)),
            dma((3,)),
            dma((chips,)),
            dma((chips,)),
        ]
        + [dma((n_sp,))] * 6,
        compiler_params=pltpu.CompilerParams(
            collective_id=2, has_side_effects=True, vmem_limit_bytes=VMEM_BYTES
        ),
        name="tail",
    )(mix, weight, y, normed, x, dt, rate, extra, coming, b, c, gate, scale)


def body(
    n_sp,
    n_tp,
    mixer_output_stream,
    layer_output_gradient,
    routes,
    expert_combine_weight,
    expert_gate_weight,
    expert_up_weight,
    expert_down_weight,
    head_mixer_input,
    head_step_size,
    head_decay_rate,
    extra_log_decay,
    state_entering_span,
    state_input_vectors,
    state_readout_vectors,
    gate_preactivation,
    group_norm_scale,
    mixer_output_weight,
):
    packed = pack(routes, expert_combine_weight, mixer_output_stream, layer_output_gradient, n_sp)
    heads = head_step_size.shape[1]
    part_rows = heads * HDIM // n_sp
    entering = lax.dynamic_index_in_dim(
        state_entering_span.reshape(n_sp, part_rows, STATE), lax.axis_index(SP), 0, keepdims=False
    )
    rate = head_decay_rate[None, :]
    scale = group_norm_scale[None, :]
    arrived, scan_out, normed_low, coming = front(
        packed,
        head_mixer_input,
        head_step_size,
        rate,
        extra_log_decay,
        entering,
        state_input_vectors,
        state_readout_vectors,
        gate_preactivation,
        scale,
        n_sp,
        n_tp,
    )
    mix_grad, grad_g, grad_u, grad_d = experts_backward(
        arrived,
        expert_gate_weight,
        expert_up_weight,
        expert_down_weight,
        routes,
        layer_output_gradient,
        n_sp,
        n_tp,
    )
    weight = lax.all_gather(mixer_output_weight, SP, axis=1, tiled=True)
    proj_grad, input_grad, step_grad, b_grad, c_grad, gate_grad_in = tail(
        mix_grad,
        weight,
        scan_out,
        normed_low,
        head_mixer_input,
        head_step_size,
        rate,
        extra_log_decay,
        coming,
        state_input_vectors,
        state_readout_vectors,
        gate_preactivation,
        scale,
        n_sp,
        n_tp,
    )
    return (
        grad_g,
        grad_u,
        grad_d,
        proj_grad,
        input_grad,
        step_grad,
        b_grad,
        c_grad,
        gate_grad_in,
    )


def solution(mesh):
    placed = (
        P(SP, "tp"),
        P(SP, "tp"),
        P(SP, None),
        P(SP, None),
        P(SP, None, "tp"),
        P(SP, None, "tp"),
        P(SP, "tp", None),
        P(SP, "tp"),
        P(SP, "tp"),
        P("tp"),
        P(SP, "tp"),
        P("tp", None, None),
        P(SP, "tp"),
        P(SP, "tp"),
        P(SP, "tp"),
        P("tp"),
        P("tp", SP),
    )
    return jax.shard_map(
        functools.partial(body, mesh.shape["sp"], mesh.shape["tp"]),
        mesh=mesh,
        in_specs=placed,
        out_specs=(
            P(SP, None, "tp"),
            P(SP, None, "tp"),
            P(SP, "tp", None),
            P("tp", SP),
            P(SP, "tp"),
            P(SP, "tp"),
            P(SP, "tp"),
            P(SP, "tp"),
            P(SP, "tp"),
        ),
        check_vma=False,
    )
```

```python
import functools

import jax
import jax.numpy as jnp
from jax import lax
from jax.experimental import pallas as pl
from jax.experimental.pallas import tpu as pltpu
from jax.sharding import PartitionSpec as P

HDIM = 64
STATE = 128
SP = "sp"
CAP = 12
MESH = pl.DeviceIdType.MESH
F32 = jnp.float32
BF16 = jnp.bfloat16

norm_eps = 1e-05
VMEM_BYTES = 60 * 1024 * 1024


def vmem_spec():
    return pl.BlockSpec(memory_space=pltpu.VMEM)


def any_spec():
    return pl.BlockSpec(memory_space=pl.ANY)


def dot(a, b, contract=((1,), (0,))):
    return lax.dot_general(a, b, (contract, ((), ())), preferred_element_type=F32)


def iota(shape, dim):
    return lax.broadcasted_iota(jnp.int32, shape, dim)


def divide(x, by):
    return ((x.astype(F32) + 0.5) * (1.0 / by)).astype(jnp.int32)


def slots_in_rows(routes, experts):
    top, tokens = routes.shape
    ids = iota((experts, tokens), 0)
    earlier = (iota((tokens, tokens), 0) < iota((tokens, tokens), 1)).astype(BF16)
    before = jnp.zeros((experts, 1), F32)
    rows = []
    for k in range(top):
        hits = (ids == routes[k : k + 1, :]).astype(F32)
        rank = dot(hits.astype(BF16), earlier) + before
        rows.append(jnp.sum(hits * rank, axis=0, keepdims=True))
        before = before + jnp.sum(hits, axis=1, keepdims=True)
    return [routes[k : k + 1, :] * CAP + rows[k].astype(jnp.int32) for k in range(top)]


def pack_kernel(experts, routes_ref, weights_ref, stream_ref, grads_ref, out_ref):
    tokens = stream_ref.shape[0]
    half = stream_ref.shape[1] // 2
    slots = slots_in_rows(routes_ref[...], experts)
    row = iota((experts * 4 * CAP, 1), 0)
    expert = divide(row, 4 * CAP)
    inner = row - expert * (4 * CAP)
    part = divide(inner, CAP)
    slot = expert * CAP + inner - part * CAP
    first = (slot == slots[0]).astype(F32)
    second = (slot == slots[1]).astype(F32)
    match = (first + second).astype(BF16)
    weight = jnp.sum(
        first * weights_ref[0:1, :] + second * weights_ref[1:2, :], axis=1, keepdims=True
    )
    x0 = dot(match, stream_ref[:, :half])
    x1 = dot(match, stream_ref[:, half:])
    g0 = dot(match, grads_ref[:, :half])
    g1 = dot(match, grads_ref[:, half:])
    low = jnp.where(part == 0, x0, g0 * weight)
    high = jnp.where(part == 2, x1, g1 * weight)
    out_ref[...] = jnp.where(part < 2, low, high).astype(BF16)


def pack(routes, weights, stream, grads, experts):
    half = stream.shape[1] // 2
    packed = pl.pallas_call(
        functools.partial(pack_kernel, experts),
        out_shape=jax.ShapeDtypeStruct((experts * 4 * CAP, half), BF16),
        in_specs=[vmem_spec()] * 4,
        out_specs=vmem_spec(),
        compiler_params=pltpu.CompilerParams(vmem_limit_bytes=VMEM_BYTES),
        name="pack",
    )(routes.T, weights.T, stream, grads)
    return packed.reshape(experts, 4 * CAP, half)


def hop(i, n_sp):
    return lax.rem(i * 11, n_sp)


def ring_reduce(piece, place, to_right, to_left, from_left, from_right, sum_right, sum_left, sems):
    s_r, s_l, r_l, r_r = sems
    right, left, far = lax.rem(place + 1, 4), lax.rem(place + 3, 4), lax.rem(place + 2, 4)

    def right_copy(k, src):
        return pltpu.make_async_remote_copy(
            src, from_left.at[k], s_r.at[k], r_l.at[k], to_right, MESH
        )

    def left_copy(k, src):
        return pltpu.make_async_remote_copy(
            src, from_right.at[k], s_l.at[k], r_r.at[k], to_left, MESH
        )

    def start():
        right_copy(0, piece(far, 0)).start()
        left_copy(0, piece(far, 1)).start()
        right_copy(1, piece(right, 1)).start()
        left_copy(1, piece(left, 0)).start()

    def middle():
        right_copy(0, piece(far, 0)).wait()
        sum_right[...] = (piece(right, 0)[...].astype(F32) + from_left[0].astype(F32)).astype(BF16)
        left_copy(0, piece(far, 1)).wait()
        sum_left[...] = (piece(left, 1)[...].astype(F32) + from_right[0].astype(F32)).astype(BF16)
        right_copy(2, sum_right).start()
        left_copy(2, sum_left).start()

    def finish():
        right_copy(1, piece(right, 1)).wait()
        left_copy(1, piece(left, 0)).wait()
        right_copy(2, sum_right).wait()
        left_copy(2, sum_left).wait()

    def total(w, at=()):
        near, across = (from_left, from_right) if w == 0 else (from_right, from_left)
        return (
            piece(place, w)[at or Ellipsis].astype(F32)
            + near[(2,) + at].astype(F32)
            + across[(1,) + at].astype(F32)
        )

    return start, middle, finish, total


def greet(me, tp, n_sp, n_tp, step=1, ring=False, partner=None):
    barrier = pltpu.get_barrier_semaphore()

    def hello(d, carry):
        pl.semaphore_signal(
            barrier, inc=1, device_id=(lax.rem(me + d * step, n_sp), tp), device_id_type=MESH
        )
        return carry

    lax.fori_loop(1, n_sp // step, hello, 0)
    count = n_sp // step - 1
    if partner is not None:
        pl.semaphore_signal(barrier, inc=1, device_id=(partner, tp), device_id_type=MESH)
        count += 1
    if ring:
        for other in (lax.rem(tp + 1, n_tp), lax.rem(tp + n_tp - 1, n_tp)):
            pl.semaphore_signal(barrier, inc=1, device_id=(me, other), device_id_type=MESH)
        count += 2
    pl.semaphore_wait(barrier, count)


def split(x, pieces):
    terms = []
    for _ in range(pieces):
        term = x.astype(BF16)
        terms.append(term)
        x = x - term.astype(F32)
    return terms


def dot_split(x, exact, pieces, contract, left=True):
    total = None
    for term in split(x, pieces):
        part = dot(term, exact, contract) if left else dot(exact, term, contract)
        total = part if total is None else total + part
    return total


def triangle(n, keep):
    return keep(iota((n, n), 0), iota((n, n), 1)).astype(BF16)


def head_spread(heads, size):
    channel, head = iota((heads, heads * size), 1), iota((heads, heads * size), 0)
    return ((channel >= head * size) & (channel < (head + 1) * size)).astype(BF16)


def spread(x, owner):
    return dot_split(x, owner, 2, ((1,), (0,)))


def by_head(x, owner):
    return dot_split(x, owner, 2, ((1,), (1,)))


def cumulative_decay(time_step, rate, extra):
    log_decay = extra - time_step * rate
    upto = triangle(log_decay.shape[0], lambda t, s: s <= t)
    return dot_split(log_decay, upto, 3, ((1,), (0,)), left=False)


def turned(x):
    n = x.shape[1]
    return dot_split(x, triangle(n, lambda a, b: a == b), 3, ((1,), (1,)), left=False)


def decay_between(cum, cum_rows, h):
    gap = cum[:, h : h + 1] - cum_rows[h : h + 1, :]
    n = gap.shape[0]
    return jnp.exp(jnp.where(iota((n, n), 1) <= iota((n, n), 0), gap, -1e30))


def halves(pair):
    lane = iota(pair.shape, 1)
    zero = jnp.zeros_like(pair)
    size = pair.shape[1] // 2
    return jnp.concatenate([jnp.where(lane < size, pair, zero), jnp.where(lane < size, zero, pair)], axis=0)


def front_kernel(
    n_sp,
    n_tp,
    in_ref,
    x_ref,
    dt_ref,
    rate_ref,
    extra_ref,
    first_hbm,
    b_ref,
    c_ref,
    gate_ref,
    scale_ref,
    out_ref,
    y_ref,
    normed_ref,
    coming,
    state_mine,
    decay_mine,
    states,
    decays,
    carries,
    diag,
    own,
    one,
    two,
    a_send,
    a_recv,
    s_right,
    s_left,
    r_left,
    r_right,
    f_send,
    f_recv,
    sends,
    recvs,
    d_sends,
    d_recvs,
    b_sends,
    b_recvs,
    first_ref,
    first_sem,
):
    me, tp = lax.axis_index("sp"), lax.axis_index("tp")
    entering = pltpu.make_async_copy(first_hbm.at[me], first_ref, first_sem)
    entering.start()
    right, left = lax.rem(tp + 1, n_tp), lax.rem(tp + n_tp - 1, n_tp)
    far = lax.rem(tp + 2, n_tp)
    greet(me, tp, n_sp, n_tp, ring=True)

    def origin(d):
        return lax.rem(me + n_sp - d, n_sp)

    def exchange(d):
        to = lax.rem(me + d, n_sp)
        return pltpu.make_async_remote_copy(
            in_ref.at[to], out_ref.at[tp, me], a_send.at[d], a_recv.at[d], (to, tp), MESH
        )

    def arrived(d):
        return pltpu.make_async_remote_copy(
            in_ref.at[me], out_ref.at[tp, origin(d)], a_send.at[d], a_recv.at[d], (me, tp), MESH
        )

    def to_right(d, block):
        piece = out_ref.at[block, origin(d)]
        return pltpu.make_async_remote_copy(
            piece, piece, s_right.at[d], r_left.at[d], (me, right), MESH
        )

    def to_left(d, block):
        piece = out_ref.at[block, origin(d)]
        return pltpu.make_async_remote_copy(
            piece, piece, s_left.at[d], r_right.at[d], (me, left), MESH
        )

    def onward(d, block, to):
        piece = out_ref.at[block, origin(d)]
        return pltpu.make_async_remote_copy(
            piece, piece, f_send.at[d], f_recv.at[d], (me, to), MESH
        )

    def start_exchange(d, carry):
        exchange(hop(d, n_sp)).start()
        return carry

    lax.fori_loop(1, n_sp, start_exchange, 0)
    mine = pltpu.make_async_copy(in_ref.at[me], out_ref.at[tp, me], own)
    mine.start()

    heads, tokens = dt_ref.shape
    channels = x_ref.shape[1]
    groups = b_ref.shape[1] // STATE
    wide = channels // groups
    owner = head_spread(heads, HDIM)
    dt = turned(dt_ref[...])
    cum = cumulative_decay(dt, rate_ref[...], turned(extra_ref[...]))
    cum_rows = turned(cum)
    last = cum[tokens - 1 : tokens, :]
    values = x_ref[...].astype(F32)
    ending = (values * spread(dt * jnp.exp(last - cum), owner)).astype(BF16)
    parts, rows, entries = state_mine.shape
    per_group = parts // groups
    for g in range(groups):
        state = dot(
            ending[:, g * wide : (g + 1) * wide],
            b_ref[:, g * STATE : (g + 1) * STATE],
            ((0,), (0,)),
        )
        state_mine[g * per_group : (g + 1) * per_group] = state.astype(BF16).reshape(
            per_group, rows, entries
        )
    total = jnp.exp(last)
    for p in range(parts):
        h = p * rows // HDIM
        decay_mine[p] = jnp.broadcast_to(total[:, h : h + 1], (1, entries))

    mine.wait()
    to_right(0, tp).start()
    to_left(0, tp).start()

    def state_copy(d):
        to = lax.rem(me + d, n_sp)
        return pltpu.make_async_remote_copy(
            state_mine.at[to], states.at[me], sends.at[d], recvs.at[d], (to, tp), MESH
        )

    def decay_copy(d):
        to = lax.rem(me + d, n_sp)
        return pltpu.make_async_remote_copy(
            decay_mine.at[to], decays.at[me], d_sends.at[d], d_recvs.at[d], (to, tp), MESH
        )

    def back_copy(d):
        to = lax.rem(me + d, n_sp)
        return pltpu.make_async_remote_copy(
            carries.at[to], coming.at[me], b_sends.at[d], b_recvs.at[d], (to, tp), MESH
        )

    def start_states(d, carry):
        decay_copy(hop(d, n_sp)).start()
        state_copy(hop(d, n_sp)).start()
        return carry

    lax.fori_loop(1, n_sp, start_states, 0)
    kept = pltpu.make_async_copy(state_mine.at[me], states.at[me], one)
    kept_too = pltpu.make_async_copy(decay_mine.at[me], decays.at[me], two)
    kept.start()
    kept_too.start()

    def spread_out(i, carry):
        d = hop(i, n_sp)
        arrived(d).wait_recv()
        to_right(d, tp).start()
        to_left(d, tp).start()
        return carry

    lax.fori_loop(1, n_sp, spread_out, 0)

    scaled = (values * spread(dt, owner)).astype(BF16)
    affinity = [
        dot(
            c_ref[:, g * STATE : (g + 1) * STATE],
            b_ref[:, g * STATE : (g + 1) * STATE],
            ((1,), (1,)),
        )
        for g in range(groups)
    ]
    for q in range(heads // 2):
        g = q // (heads // 2 // groups)
        both = jnp.concatenate(
            [(affinity[g] * decay_between(cum, cum_rows, 2 * q + j)).astype(BF16) for j in range(2)],
            axis=1,
        )
        at = slice(q * 2 * HDIM, (q + 1) * 2 * HDIM)
        diag[:, at] = dot(both, halves(scaled[:, at]))

    kept.wait()
    kept_too.wait()

    def finish_states(d, carry):
        decay_copy(d).wait()
        state_copy(d).wait()
        return carry

    lax.fori_loop(1, n_sp, finish_states, 0)
    entering.wait()
    running = first_ref[...]
    for i in range(n_sp):
        carries[i] = running.astype(BF16)
        running = decays[i] * running + states[i].astype(F32)

    def start_back(d, carry):
        back_copy(hop(d, n_sp)).start()
        return carry

    lax.fori_loop(1, n_sp, start_back, 0)
    kept_back = pltpu.make_async_copy(carries.at[me], coming.at[me], one)
    kept_back.start()

    def relay(q, carry):
        d, e = hop(2 * q, n_sp), hop(2 * q + 1, n_sp)
        to_right(d, left).wait_recv()
        onward(d, left, right).start()
        to_left(e, right).wait_recv()
        onward(e, right, left).start()
        return carry

    lax.fori_loop(0, n_sp // 2, relay, 0)
    kept_back.wait()

    def finish_back(d, carry):
        back_copy(d).wait()
        return carry

    lax.fori_loop(1, n_sp, finish_back, 0)
    since = spread(jnp.exp(cum), owner)
    for g in range(groups):
        at = slice(g * wide, (g + 1) * wide)
        incoming = coming[g * per_group : (g + 1) * per_group].reshape(wide, entries)
        y = diag[:, at] + since[:, at] * dot(
            c_ref[:, g * STATE : (g + 1) * STATE], incoming, ((1,), (1,))
        )
        y_ref[:, at] = y
        gate = gate_ref[:, at].astype(F32)
        gated = y * gate * jax.nn.sigmoid(gate)
        factor = lax.rsqrt(jnp.mean(gated * gated, axis=1, keepdims=True) + norm_eps)
        normed_ref[:, at] = (gated * factor * scale_ref[:, at]).astype(BF16)

    def finish(q, carry):
        d, e = hop(2 * q, n_sp), hop(2 * q + 1, n_sp)
        to_left(d, right).wait_recv()
        to_right(e, left).wait_recv()
        onward(d, far, right).wait()
        onward(e, far, left).wait()
        to_right(d, tp).wait_send()
        to_left(d, tp).wait_send()
        to_right(e, tp).wait_send()
        to_left(e, tp).wait_send()
        return carry

    lax.fori_loop(0, n_sp // 2, finish, 0)

    def drain(d, carry):
        exchange(d).wait_send()
        return carry

    lax.fori_loop(1, n_sp, drain, 0)


def front(packed, x, dt, rate, extra, first, b, c, gate, scale, n_sp, n_tp):
    dma = pltpu.SemaphoreType.DMA
    tokens, channels = x.shape
    _, rows, entries = first.shape
    return pl.pallas_call(
        functools.partial(front_kernel, n_sp, n_tp),
        out_shape=(
            jax.ShapeDtypeStruct((n_tp,) + packed.shape, BF16),
            jax.ShapeDtypeStruct((tokens, channels), F32),
            jax.ShapeDtypeStruct((tokens, channels), BF16),
            jax.ShapeDtypeStruct((n_sp, rows, entries), BF16),
        ),
        in_specs=[vmem_spec()] * 5 + [any_spec()] + [vmem_spec()] * 4,
        out_specs=(vmem_spec(),) * 4,
        scratch_shapes=[
            pltpu.VMEM((n_sp, rows, entries), BF16),
            pltpu.VMEM((n_sp, 1, entries), F32),
            pltpu.VMEM((n_sp, rows, entries), BF16),
            pltpu.VMEM((n_sp, 1, entries), F32),
            pltpu.VMEM((n_sp, rows, entries), BF16),
            pltpu.VMEM((tokens, channels), F32),
            dma,
            dma,
            dma,
        ]
        + [dma((n_sp,))] * 14
        + [pltpu.VMEM((rows, entries), F32), dma],
        compiler_params=pltpu.CompilerParams(
            collective_id=0, has_side_effects=True, vmem_limit_bytes=VMEM_BYTES
        ),
        name="front",
    )(packed, x, dt, rate, extra, first, b, c, gate, scale)


def expert_kernel(
    n_sp,
    n_tp,
    in_ref,
    gate_hbm,
    up_hbm,
    down_hbm,
    routes_ref,
    grads_ref,
    own_hbm,
    mix_ref,
    all_hbm,
    dgate_hbm,
    dup_hbm,
    ddown_hbm,
    w_gate,
    w_up,
    w_down,
    d_gate,
    d_up,
    d_down,
    x,
    x_t,
    g,
    gate_grad,
    up_grad,
    hidden,
    part_ref,
    from_left,
    from_right,
    sum_right,
    sum_left,
    out_blocks,
    back,
    own_cols,
    loads,
    stores,
    s_r,
    s_l,
    r_l,
    r_r,
    a_send,
    a_recv,
    g_send,
    g_recv,
    local,
    w_own,
    w_sends,
    w_recvs,
):
    me, tp = lax.axis_index("sp"), lax.axis_index("tp")
    right, left = lax.rem(tp + 1, n_tp), lax.rem(tp + n_tp - 1, n_tp)
    far = lax.rem(tp + 2, n_tp)
    tokens, width = grads_ref.shape
    half, quarter = width // 2, width // 4
    model, units = w_gate.shape
    rows = x.shape[0]
    cuts = [(i, min(256, units - i)) for i in range(0, units, 256)]
    fetches = []
    for k, (start, size) in enumerate(cuts):
        at = pl.ds(start, size)
        fetches.append(
            [
                pltpu.make_async_copy(gate_hbm.at[0, :, at], w_gate.at[:, at], loads.at[3 * k]),
                pltpu.make_async_copy(up_hbm.at[0, :, at], w_up.at[:, at], loads.at[3 * k + 1]),
                pltpu.make_async_copy(down_hbm.at[0, at, :], w_down.at[at, :], loads.at[3 * k + 2]),
            ]
        )
        for fetch in fetches[-1]:
            fetch.start()
    greet(me, tp, n_sp, n_tp, ring=True)

    core = lax.rem(me, 2)
    lane_y, lane_z = lax.rem(lax.div(me, 2), 4), lax.div(me, 8)

    def at_y(y):
        return lane_z * 8 + y * 2 + core

    def at_z(z):
        return z * 8 + lane_y * 2 + core

    def weight_copy(k, src, dst, to):
        return pltpu.make_async_remote_copy(
            src, dst, w_sends.at[k], w_recvs.at[k], (to, tp), MESH
        )

    own_weight = pltpu.make_async_copy(own_hbm, all_hbm.at[core, lane_z, lane_y], w_own)
    own_weight.start()

    def first_stage(j, sending):
        y, z = (lane_y, lane_z) if sending else (lax.rem(lane_y + 4 - j, 4), lax.rem(lane_z + 4 - j, 4))
        return [
            weight_copy(
                j - 1, own_hbm.at[0], all_hbm.at[core, lane_z, y, 0], at_y(lax.rem(lane_y + j, 4))
            ),
            weight_copy(
                j + 2, own_hbm.at[1], all_hbm.at[core, z, lane_y, 1], at_z(lax.rem(lane_z + j, 4))
            ),
        ]

    def second_stage(j, sending):
        y, z = (lane_y, lane_z) if sending else (lax.rem(lane_y + 4 - j, 4), lax.rem(lane_z + 4 - j, 4))
        by_z, by_y = all_hbm.at[core, z, :, 0], all_hbm.at[core, :, y, 1]
        return [
            weight_copy(j + 5, by_z, by_z, at_z(lax.rem(lane_z + j, 4))),
            weight_copy(j + 8, by_y, by_y, at_y(lax.rem(lane_y + j, 4))),
        ]

    def third_stage(c):
        return weight_copy(12, all_hbm.at[c], all_hbm.at[c], me + 1 - 2 * core)

    for j in range(1, 4):
        for copy in first_stage(j, True):
            copy.start()

    tall = in_ref.shape[2]
    group_of = 8
    span = group_of * CAP
    spots = iota((1, group_of * tall), 1)
    src = divide(spots, tall)
    inner = spots - src * tall
    which = divide(inner, CAP)
    row = src * CAP + inner - which * CAP
    lines = iota((span, 1), 0)
    pick = [((row == lines) & (which == p)).astype(BF16) for p in range(4)]
    for t in range(n_tp):
        for k in range(n_sp // group_of):
            block = in_ref[t, k * group_of : (k + 1) * group_of].reshape(group_of * tall, half)
            at = slice(k * span, (k + 1) * span)
            for c in range(2):
                cols = slice((2 * t + c) * half, (2 * t + c + 1) * half)
                x[at, cols] = dot(pick[2 * c], block).astype(BF16)
                g[at, cols] = dot(pick[2 * c + 1], block).astype(BF16)

    for k, (start, size) in enumerate(cuts):
        for fetch in fetches[k]:
            fetch.wait()
        at = slice(start, start + size)
        pre_gate = dot(x[...], w_gate[:, at])
        pre_up = dot(x[...], w_up[:, at])
        hidden_grad = dot(g[...], w_down[at, :], ((1,), (1,)))
        sigmoid_gate = jax.nn.sigmoid(pre_gate)
        activated = pre_gate * sigmoid_gate
        hidden[:, at] = (activated * pre_up).astype(BF16)
        gate_grad[:, at] = (
            hidden_grad * pre_up * sigmoid_gate * (1.0 + pre_gate * (1.0 - sigmoid_gate))
        ).astype(BF16)
        up_grad[:, at] = (hidden_grad * activated).astype(BF16)

    own_weight.wait()
    for j in range(1, 4):
        for copy in first_stage(j, False):
            copy.wait_recv()
    for j in range(1, 4):
        for copy in second_stage(j, True):
            copy.start()

    def row_block(b):
        for c in range(2):
            cols = pl.ds(pl.multiple_of(b * width + c * half, half), half)
            part_ref[2 * b + c] = (
                dot(gate_grad[...], w_gate[cols, :], ((1,), (1,)))
                + dot(up_grad[...], w_up[cols, :], ((1,), (1,)))
            ).astype(BF16)

    def block(b, which):
        return part_ref.at[2 * b + which]

    def right_copy(k, src):
        return pltpu.make_async_remote_copy(
            src, from_left.at[k], s_r.at[k], r_l.at[k], (me, right), MESH
        )

    def left_copy(k, src):
        return pltpu.make_async_remote_copy(
            src, from_right.at[k], s_l.at[k], r_r.at[k], (me, left), MESH
        )

    row_block(far)
    row_block(right)
    right_copy(0, block(far, 0)).start()
    left_copy(0, block(far, 1)).start()
    row_block(left)
    right_copy(1, block(right, 1)).start()
    row_block(tp)
    left_copy(1, block(left, 0)).start()

    saves = []

    def save(k, src, dst):
        copy = pltpu.make_async_copy(src, dst, stores.at[k])
        copy.start()
        saves.append(copy)

    def passed_right():
        right_copy(0, block(far, 0)).wait()
        sum_right[...] = (block(right, 0)[...].astype(F32) + from_left[0].astype(F32)).astype(BF16)
        left_copy(0, block(far, 1)).wait()
        sum_left[...] = (block(left, 1)[...].astype(F32) + from_right[0].astype(F32)).astype(BF16)

    def gate_up_rows(i):
        at = slice(i * 256, (i + 1) * 256)
        x_t[at, :] = jnp.transpose(x[:, at])
        d_gate[at, :] = dot(x_t[at, :], gate_grad[...]).astype(BF16)
        save(2 * i, d_gate.at[at, :], dgate_hbm.at[0, at, :])
        d_up[at, :] = dot(x_t[at, :], up_grad[...]).astype(BF16)
        save(2 * i + 1, d_up.at[at, :], dup_hbm.at[0, at, :])

    for i in range(4):
        gate_up_rows(i)
    passed_right()
    right_copy(2, sum_right).start()
    left_copy(2, sum_left).start()
    for i in range(4, 8):
        gate_up_rows(i)

    for k, (start, size) in enumerate(cuts):
        at = slice(start, start + size)
        d_down[at, :] = dot(hidden[:, at], g[...], ((0,), (0,))).astype(BF16)
        save(16 + k, d_down.at[at, :], ddown_hbm.at[0, at, :])

    for j in range(1, 4):
        for copy in second_stage(j, False):
            copy.wait_recv()
    third_stage(core).start()

    by_token = slots_in_rows(routes_ref[...], n_sp)
    line = iota((8, tokens), 0)
    slots = turned(
        jnp.where(line == 0, by_token[0], jnp.where(line == 1, by_token[1], 0)).astype(F32)
    ).astype(jnp.int32)
    column = iota((1, n_sp * 4 * CAP), 1)
    expert = divide(column, 4 * CAP)
    place_in = column - expert * (4 * CAP)
    piece = divide(place_in, CAP)
    slot = expert * CAP + place_in - piece * CAP
    match = (slots[:, 0:1] == slot) | (slots[:, 1:2] == slot)

    right_copy(1, block(right, 1)).wait()
    left_copy(1, block(left, 0)).wait()
    right_copy(2, sum_right).wait()
    left_copy(2, sum_left).wait()

    tall_out = iota((group_of * 4 * CAP, 1), 0)
    out_src = divide(tall_out, 4 * CAP)
    out_in = tall_out - out_src * (4 * CAP)
    out_piece = divide(out_in, CAP)
    out_row = out_src * CAP + out_in - out_piece * CAP
    pair_at = iota((1, span), 1)
    place = [((out_row == pair_at) & (out_piece == c)).astype(BF16) for c in range(4)]
    for k in range(rows // span):
        at = slice(k * span, (k + 1) * span)
        low = (
            part_ref[2 * tp, at, :].astype(F32)
            + from_left[2, at, :].astype(F32)
            + from_right[1, at, :].astype(F32)
        ).astype(BF16)
        high = (
            part_ref[2 * tp + 1, at, :].astype(F32)
            + from_right[2, at, :].astype(F32)
            + from_left[1, at, :].astype(F32)
        ).astype(BF16)
        laid = (
            dot(place[0], low[:, :quarter])
            + dot(place[1], low[:, quarter:])
            + dot(place[2], high[:, :quarter])
            + dot(place[3], high[:, quarter:])
        )
        out_blocks[k * group_of : (k + 1) * group_of] = laid.astype(BF16).reshape(
            group_of, 4 * CAP, quarter
        )

    def exchange(d):
        to = lax.rem(me + d, n_sp)
        return pltpu.make_async_remote_copy(
            out_blocks.at[to], back.at[me], a_send.at[d], a_recv.at[d], (to, tp), MESH
        )

    def start_exchange(d, carry):
        exchange(hop(d, n_sp)).start()
        return carry

    lax.fori_loop(1, n_sp, start_exchange, 0)
    mine = pltpu.make_async_copy(out_blocks.at[me], back.at[me], local)
    mine.start()
    mine.wait()

    def finish_exchange(d, carry):
        exchange(d).wait()
        return carry

    lax.fori_loop(1, n_sp, finish_exchange, 0)
    returned = back[...].reshape(n_sp * 4 * CAP, quarter)
    for c in range(4):
        chosen = jnp.where(match & (piece == c), 1.0, 0.0).astype(BF16)
        cols = slice(c * quarter, (c + 1) * quarter)
        own_cols[:, cols] = (grads_ref[:, cols].astype(F32) + dot(chosen, returned)).astype(BF16)

    def spot(b):
        return mix_ref.at[:, pl.ds(pl.multiple_of(b * width, width), width)]

    def spot_half(b, which):
        return mix_ref.at[:, pl.ds(pl.multiple_of(b * width + which * half, half), half)]

    def gather(k, src, dst, to):
        return pltpu.make_async_remote_copy(
            src, dst, g_send.at[k], g_recv.at[k], (me, to), MESH
        )

    gather(0, own_cols, spot(tp), right).start()
    gather(1, own_cols, spot(tp), left).start()
    spot(tp)[...] = own_cols[...]
    gather(0, own_cols, spot(left), right).wait_recv()
    gather(2, spot_half(left, 0), spot_half(left, 0), right).start()
    gather(1, own_cols, spot(right), left).wait_recv()
    gather(3, spot_half(right, 1), spot_half(right, 1), left).start()
    gather(2, spot_half(far, 0), spot_half(far, 0), right).wait()
    gather(3, spot_half(far, 1), spot_half(far, 1), left).wait()
    gather(0, own_cols, spot(tp), right).wait_send()
    gather(1, own_cols, spot(tp), left).wait_send()
    for copy in saves:
        copy.wait()
    for j in range(1, 4):
        for copy in first_stage(j, True) + second_stage(j, True):
            copy.wait_send()
    third_stage(core).wait_send()
    third_stage(1 - core).wait_recv()


def experts_backward(arrived, w_gate, w_up, w_down, routes, grads, own, n_sp, n_tp):
    _, model, units = w_gate.shape
    rows = n_sp * CAP
    tokens, width = grads.shape
    half, quarter = width // 2, width // 4
    dma = pltpu.SemaphoreType.DMA
    return pl.pallas_call(
        functools.partial(expert_kernel, n_sp, n_tp),
        out_shape=(
            jax.ShapeDtypeStruct((tokens, width * n_tp), BF16),
            jax.ShapeDtypeStruct((2, 4, 4) + own.shape, BF16),
            jax.ShapeDtypeStruct(w_gate.shape, BF16),
            jax.ShapeDtypeStruct(w_up.shape, BF16),
            jax.ShapeDtypeStruct(w_down.shape, BF16),
        ),
        in_specs=[vmem_spec()] + [any_spec()] * 3 + [vmem_spec()] * 2 + [any_spec()],
        out_specs=(vmem_spec(),) + (any_spec(),) * 4,
        scratch_shapes=[
            pltpu.VMEM((model, units), BF16),
            pltpu.VMEM((model, units), BF16),
            pltpu.VMEM((units, model), BF16),
            pltpu.VMEM((model, units), BF16),
            pltpu.VMEM((model, units), BF16),
            pltpu.VMEM((units, model), BF16),
            pltpu.VMEM((rows, model), BF16),
            pltpu.VMEM((model, rows), BF16),
            pltpu.VMEM((rows, model), BF16),
            pltpu.VMEM((rows, units), BF16),
            pltpu.VMEM((rows, units), BF16),
            pltpu.VMEM((rows, units), BF16),
            pltpu.VMEM((2 * n_tp, rows, half), BF16),
            pltpu.VMEM((3, rows, half), BF16),
            pltpu.VMEM((3, rows, half), BF16),
            pltpu.VMEM((rows, half), BF16),
            pltpu.VMEM((rows, half), BF16),
            pltpu.VMEM((n_sp, 4 * CAP, quarter), BF16),
            pltpu.VMEM((n_sp, 4 * CAP, quarter), BF16),
            pltpu.VMEM((tokens, width), BF16),
            dma((12,)),
            dma((20,)),
            dma((3,)),
            dma((3,)),
            dma((3,)),
            dma((3,)),
            dma((n_sp,)),
            dma((n_sp,)),
            dma((4,)),
            dma((4,)),
            dma,
            dma,
            dma((13,)),
            dma((13,)),
        ],
        compiler_params=pltpu.CompilerParams(
            collective_id=1, has_side_effects=True, vmem_limit_bytes=VMEM_BYTES
        ),
        name="experts",
    )(arrived, w_gate, w_up, w_down, routes, grads, own)


def tail_kernel(
    n_sp,
    n_tp,
    mix_ref,
    weight_hbm,
    y_ref,
    normed_ref,
    x_ref,
    dt_ref,
    rate_ref,
    extra_ref,
    coming_ref,
    b_ref,
    c_ref,
    gate_ref,
    scale_ref,
    proj_ref,
    dx_ref,
    ddt_ref,
    db_ref,
    dc_ref,
    dgate_ref,
    weight,
    normed2,
    mix2,
    parts,
    big_in,
    big_sum,
    small_in,
    small_sum,
    reduced,
    total,
    state_mine,
    decay_mine,
    states,
    decays,
    carries,
    later,
    d_scaled,
    one,
    two,
    load,
    p_send,
    p_recv,
    ring_sems,
    sends,
    recvs,
    d_sends,
    d_recvs,
    b_sends,
    b_recvs,
):
    me, tp = lax.axis_index("sp"), lax.axis_index("tp")
    core = lax.rem(me, 2)
    partner = me + 1 - 2 * core
    chip = lax.div(me, 2)
    chips = n_sp // 2
    fetches = [
        pltpu.make_async_copy(weight_hbm.at[c], weight.at[:, c], load.at[c]) for c in range(2)
    ]
    for fetch in fetches:
        fetch.start()
    greet(me, tp, n_sp, n_tp)
    heads, tokens = dt_ref.shape
    channels = x_ref.shape[1]
    groups = b_ref.shape[1] // STATE
    wide = channels // groups
    half = channels // 2
    cols = proj_ref.shape[0]
    n_parts, rows, entries = state_mine.shape
    per_group = n_parts // groups

    def pair(k, src, dst):
        return pltpu.make_async_remote_copy(
            src, dst, p_send.at[k], p_recv.at[k], (partner, tp), MESH
        )

    def mine(c):
        return pl.ds(pl.multiple_of(c * half, half), half)

    pair(0, normed_ref.at[:, mine(1 - core)], normed2).start()
    pair(1, mix_ref, mix2).start()

    owner = head_spread(heads, HDIM)
    dt = turned(dt_ref[...])
    cum = cumulative_decay(dt, rate_ref[...], turned(extra_ref[...]))
    cum_rows = turned(cum)
    last = cum[tokens - 1 : tokens, :]
    since = spread(jnp.exp(cum), owner)

    mix_t = jnp.transpose(mix_ref[...])
    pair(0, normed_ref.at[:, mine(1 - core)], normed2).wait()
    pair(1, mix_ref, mix2).wait()
    both_mix = jnp.concatenate([mix_t, jnp.transpose(mix2[...])], axis=1)
    both_normed = jnp.concatenate([normed_ref[:, mine(core)], normed2[...]], axis=0)
    piece_rows = cols // 2
    for z in range(4):
        at = slice(z * 8 * cols, (z + 1) * 8 * cols)
        parts[z] = (
            dot(both_mix[at, :], both_normed).astype(BF16).reshape(4, 2, 2, piece_rows, half)
        )

    lane_y, lane_z = lax.rem(chip, 4), lax.div(chip, 4)

    def at_y(y):
        return (lane_z * 8 + lax.rem(y, 4) * 2 + core, tp)

    def at_z(z):
        return (lax.rem(z, 4) * 8 + lane_y * 2 + core, tp)

    y_ring = (lane_y, at_y(lane_y + 1), at_y(lane_y + 3))
    z_ring = (lane_z, at_z(lane_z + 1), at_z(lane_z + 3))

    def four(ref, k):
        return [ref.at[k, i] for i in range(4)]

    def bufs(landing, sums, k):
        return [landing.at[k, 0], landing.at[k, 1], sums.at[k, 0], sums.at[k, 1]]

    stages = [
        ring_reduce(lambda b, w: parts.at[:, b, 0, w], *y_ring, *bufs(big_in, big_sum, 0), four(ring_sems, 0)),
        ring_reduce(lambda b, w: parts.at[b, :, 1, w], *z_ring, *bufs(big_in, big_sum, 1), four(ring_sems, 1)),
        ring_reduce(lambda b, w: reduced.at[0, w, b], *z_ring, *bufs(small_in, small_sum, 0), four(ring_sems, 2)),
        ring_reduce(lambda b, w: reduced.at[1, w, b], *y_ring, *bufs(small_in, small_sum, 1), four(ring_sems, 3)),
    ]
    stages[0][0]()
    stages[1][0]()

    for fetch in fetches:
        fetch.wait()
    whole_weight = weight[...].reshape(mix_ref.shape[1], channels)
    d_y = []
    for g in range(groups):
        at = slice(g * wide, (g + 1) * wide)
        normed_grad = dot(mix_ref[...], whole_weight[:, at])
        y = y_ref[:, at]
        gate = gate_ref[:, at].astype(F32)
        sigmoid_gate = jax.nn.sigmoid(gate)
        activated = gate * sigmoid_gate
        gated = y * activated
        factor = lax.rsqrt(jnp.mean(gated * gated, axis=1, keepdims=True) + norm_eps)
        scaled_grad = normed_grad * scale_ref[:, at]
        along = jnp.mean(scaled_grad * gated, axis=1, keepdims=True) * factor * factor
        gated_grad = factor * (scaled_grad - gated * along)
        d_y.append(gated_grad * activated)
        dgate_ref[:, at] = (
            gated_grad * y * (sigmoid_gate * (1.0 + gate * (1.0 - sigmoid_gate)))
        ).astype(BF16)
    d_out = jnp.concatenate(d_y, axis=1)
    since_grad = since * d_out
    since_low = since_grad.astype(BF16)
    for g in range(groups):
        state = dot(
            since_low[:, g * wide : (g + 1) * wide],
            c_ref[:, g * STATE : (g + 1) * STATE],
            ((0,), (0,)),
        )
        state_mine[g * per_group : (g + 1) * per_group] = state.astype(BF16).reshape(
            per_group, rows, entries
        )
    whole = jnp.exp(last)
    for p in range(n_parts):
        h = p * rows // HDIM
        decay_mine[p] = jnp.broadcast_to(whole[:, h : h + 1], (1, entries))

    def state_copy(d):
        to = lax.rem(me + d, n_sp)
        return pltpu.make_async_remote_copy(
            state_mine.at[to], states.at[me], sends.at[d], recvs.at[d], (to, tp), MESH
        )

    def decay_copy(d):
        to = lax.rem(me + d, n_sp)
        return pltpu.make_async_remote_copy(
            decay_mine.at[to], decays.at[me], d_sends.at[d], d_recvs.at[d], (to, tp), MESH
        )

    def back_copy(d):
        to = lax.rem(me + d, n_sp)
        return pltpu.make_async_remote_copy(
            carries.at[to], later.at[me], b_sends.at[d], b_recvs.at[d], (to, tp), MESH
        )

    def start_states(d, carry):
        decay_copy(hop(d, n_sp)).start()
        state_copy(hop(d, n_sp)).start()
        return carry

    lax.fori_loop(1, n_sp, start_states, 0)
    kept = pltpu.make_async_copy(state_mine.at[me], states.at[me], one)
    kept_too = pltpu.make_async_copy(decay_mine.at[me], decays.at[me], two)
    kept.start()
    kept_too.start()

    values = x_ref[...].astype(F32)
    steps = spread(dt, owner)
    scaled = values * steps
    scaled_low = scaled.astype(BF16)
    d_low = d_out.astype(BF16)
    not_before = triangle(tokens, lambda t, s: s >= t)
    below = (iota((tokens, tokens), 1) < iota((tokens, tokens), 0)).astype(F32)
    head_lane = iota((1, heads), 1)
    crossing = [jnp.zeros((tokens, heads), F32)]
    d_affinity = []

    def inside(g):
        affinity = dot(
            c_ref[:, g * STATE : (g + 1) * STATE],
            b_ref[:, g * STATE : (g + 1) * STATE],
            ((1,), (1,)),
        )
        sum_affinity = jnp.zeros((tokens, tokens), F32)
        first = g * (heads // 2 // groups)
        for q in range(first, first + heads // 2 // groups):
            at = slice(q * 2 * HDIM, (q + 1) * 2 * HDIM)
            d_halves = halves(d_low[:, at])
            d_weights = dot(d_halves, scaled_low[:, at], ((1,), (1,)))
            weights, moved = [], []
            for j in range(2):
                between = decay_between(cum, cum_rows, 2 * q + j)
                weights.append((affinity * between).astype(BF16))
                d_between = d_weights[j * tokens : (j + 1) * tokens] * between
                sum_affinity = sum_affinity + d_between
                moved.append((d_between * affinity).astype(BF16))
            d_scaled[:, at] = dot(jnp.concatenate(weights, axis=0), d_halves, ((0,), (0,)))
            reach = dot(not_before, jnp.concatenate(moved, axis=1))
            for j in range(2):
                over = jnp.sum(
                    reach[:, j * tokens : (j + 1) * tokens] * below, axis=1, keepdims=True
                )
                crossing[0] = crossing[0] + jnp.where(head_lane == 2 * q + j, over, 0.0)
        d_affinity.append(sum_affinity.astype(BF16))

    inside(0)
    stages[0][1]()
    stages[1][1]()
    kept.wait()
    kept_too.wait()

    def finish_states(d, carry):
        decay_copy(d).wait()
        state_copy(d).wait()
        return carry

    lax.fori_loop(1, n_sp, finish_states, 0)
    running = jnp.zeros((rows, entries), F32)
    for step in range(n_sp):
        i = n_sp - 1 - step
        carries[i] = running.astype(BF16)
        running = decays[i] * running + states[i].astype(F32)

    def start_back(d, carry):
        back_copy(hop(d, n_sp)).start()
        return carry

    lax.fori_loop(1, n_sp, start_back, 0)
    kept_back = pltpu.make_async_copy(carries.at[me], later.at[me], one)
    kept_back.start()

    for g in range(1, groups):
        inside(g)
    for k in range(2):
        stages[k][2]()
        for w in range(2):
            reduced[k, w] = stages[k][3](w).astype(BF16)
    stages[2][0]()
    stages[3][0]()
    read_out = []
    for g in range(groups):
        at = slice(g * wide, (g + 1) * wide)
        by = slice(g * STATE, (g + 1) * STATE)
        incoming = coming_ref[g * per_group : (g + 1) * per_group].reshape(wide, entries)
        read_out.append(dot(c_ref[:, by], incoming, ((1,), (1,))))
        dc_ref[:, by] = (
            dot(d_affinity[g], b_ref[:, by]) + dot(since_low[:, at], incoming)
        ).astype(BF16)
    reading = by_head(since_grad * jnp.concatenate(read_out, axis=1), owner)

    stages[2][1]()
    stages[3][1]()

    kept_back.wait()

    def finish_back(d, carry):
        back_copy(d).wait()
        return carry

    lax.fori_loop(1, n_sp, finish_back, 0)
    until = spread(jnp.exp(last - cum), owner)
    ending = scaled * until
    ending_low = ending.astype(BF16)
    from_later = []
    for g in range(groups):
        at = slice(g * wide, (g + 1) * wide)
        by = slice(g * STATE, (g + 1) * STATE)
        after = later[g * per_group : (g + 1) * per_group].reshape(wide, entries)
        from_later.append(dot(b_ref[:, by], after, ((1,), (1,))))
        db_ref[:, by] = (
            dot(d_affinity[g], c_ref[:, by], ((0,), (0,))) + dot(ending_low[:, at], after)
        ).astype(BF16)
    closing = jnp.concatenate(from_later, axis=1)
    gradient = d_scaled[...] + until * closing
    dx_ref[...] = (gradient * steps).astype(BF16)
    direct = by_head(gradient * values, owner)
    stored = by_head(ending * closing, owner)
    kept_state = jnp.sum(
        (
            coming_ref[...].astype(F32).reshape(heads, HDIM, entries)
            * later[...].astype(F32).reshape(heads, HDIM, entries)
        ),
        axis=1,
    )
    passing = dot_split(
        kept_state, jnp.ones((8, entries), BF16), 3, ((1,), (1,)), left=False
    )[0:1, :]
    earlier = triangle(tokens, lambda t, s: s < t)
    d_decay = (
        crossing[0]
        + dot_split(reading, not_before, 3, ((1,), (0,)), left=False)
        + dot_split(stored, earlier, 3, ((1,), (0,)), left=False)
        + passing * whole
    )
    ddt_ref[...] = turned(direct - d_decay * rate_ref[...])

    for k in range(2):
        stages[2 + k][2]()
        for w in range(2):
            first = (2 * k + w) * piece_rows
            total[first : first + piece_rows, :] = stages[2 + k][3](w)

    def lines(c):
        return pl.ds(pl.multiple_of(c * cols, cols), cols)

    given = pair(2, total.at[lines(1 - core), :], proj_ref.at[:, mine(core)])
    given.start()
    proj_ref[:, mine(core)] = total[lines(core), :]
    given.wait_send()
    pair(2, total.at[lines(core), :], proj_ref.at[:, mine(1 - core)]).wait_recv()


def tail(mix, weight, y, normed, x, dt, rate, extra, coming, b, c, gate, scale, n_sp, n_tp):
    dma = pltpu.SemaphoreType.DMA
    tokens, channels = x.shape
    heads = dt.shape[0]
    _, rows, entries = coming.shape
    width = mix.shape[1]
    half = channels // 2
    chips = n_sp // 2
    cols = width // n_sp
    return pl.pallas_call(
        functools.partial(tail_kernel, n_sp, n_tp),
        out_shape=(
            jax.ShapeDtypeStruct((cols, channels), F32),
            jax.ShapeDtypeStruct((tokens, channels), BF16),
            jax.ShapeDtypeStruct((heads, tokens), F32),
            jax.ShapeDtypeStruct(b.shape, BF16),
            jax.ShapeDtypeStruct(c.shape, BF16),
            jax.ShapeDtypeStruct((tokens, channels), BF16),
        ),
        in_specs=[vmem_spec(), any_spec()] + [vmem_spec()] * 11,
        out_specs=(vmem_spec(),) * 6,
        scratch_shapes=[
            pltpu.VMEM((chips, 2, cols, channels), BF16),
            pltpu.VMEM((tokens, half), BF16),
            pltpu.VMEM((tokens, width), BF16),
            pltpu.VMEM((4, 4, 2, 2, cols // 2, half), BF16),
            pltpu.VMEM((2, 2, 3, 4, cols // 2, half), BF16),
            pltpu.VMEM((2, 2, 4, cols // 2, half), BF16),
            pltpu.VMEM((2, 2, 3, cols // 2, half), BF16),
            pltpu.VMEM((2, 2, cols // 2, half), BF16),
            pltpu.VMEM((2, 2, 4, cols // 2, half), BF16),
            pltpu.VMEM((2 * cols, half), F32),
            pltpu.VMEM((n_sp, rows, entries), BF16),
            pltpu.VMEM((n_sp, 1, entries), F32),
            pltpu.VMEM((n_sp, rows, entries), BF16),
            pltpu.VMEM((n_sp, 1, entries), F32),
            pltpu.VMEM((n_sp, rows, entries), BF16),
            pltpu.VMEM((n_sp, rows, entries), BF16),
            pltpu.VMEM((tokens, channels), F32),
            dma,
            dma,
            dma((2,)),
            dma((3,)),
            dma((3,)),
            dma((4, 4, 3)),
        ]
        + [dma((n_sp,))] * 6,
        compiler_params=pltpu.CompilerParams(
            collective_id=2, has_side_effects=True, vmem_limit_bytes=VMEM_BYTES
        ),
        name="tail",
    )(mix, weight, y, normed, x, dt, rate, extra, coming, b, c, gate, scale)


def finish_kernel(count, *refs):
    sources, results, held = refs[:count], refs[count : 2 * count], refs[2 * count : 3 * count]
    loads, stores = refs[3 * count :]
    copies = []
    for i in range(count):
        lines = sources[i].shape[-2]
        pieces = 4 if lines > 512 else 1
        for p in range(pieces):
            at = pl.ds(p * (lines // pieces), lines // pieces)
            views = [
                ref.at[0, at, :] if len(ref.shape) == 3 else ref.at[at, :]
                for ref in (sources[i], held[i], results[i])
            ]
            k = len(copies)
            copies.append(
                (
                    pltpu.make_async_copy(views[0], views[1], loads.at[k]),
                    pltpu.make_async_copy(views[1], views[2], stores.at[k]),
                )
            )
    for load, _ in copies:
        load.start()
    for load, store in copies:
        load.wait()
        store.start()
    for _, store in copies:
        store.wait()


def finish(*arrays):
    count = len(arrays)
    dma = pltpu.SemaphoreType.DMA
    return pl.pallas_call(
        functools.partial(finish_kernel, count),
        out_shape=tuple(jax.ShapeDtypeStruct(a.shape, a.dtype) for a in arrays),
        in_specs=[any_spec()] * count,
        out_specs=(any_spec(),) * count,
        scratch_shapes=[pltpu.VMEM(a.shape, a.dtype) for a in arrays]
        + [dma((4 * count,)), dma((4 * count,))],
        compiler_params=pltpu.CompilerParams(vmem_limit_bytes=VMEM_BYTES),
        name="finish",
    )(*arrays)


def body(
    n_sp,
    n_tp,
    mixer_output_stream,
    layer_output_gradient,
    routes,
    expert_combine_weight,
    expert_gate_weight,
    expert_up_weight,
    expert_down_weight,
    head_mixer_input,
    head_step_size,
    head_decay_rate,
    extra_log_decay,
    state_entering_span,
    state_input_vectors,
    state_readout_vectors,
    gate_preactivation,
    group_norm_scale,
    mixer_output_weight,
):
    packed = pack(routes, expert_combine_weight, mixer_output_stream, layer_output_gradient, n_sp)
    heads = head_step_size.shape[1]
    part_rows = heads * HDIM // n_sp
    entering = state_entering_span.reshape(n_sp, part_rows, STATE)
    rate = head_decay_rate[None, :]
    scale = group_norm_scale[None, :]
    arrived, scan_out, normed_low, coming = front(
        packed,
        head_mixer_input,
        head_step_size.T,
        rate,
        extra_log_decay.T,
        entering,
        state_input_vectors,
        state_readout_vectors,
        gate_preactivation,
        scale,
        n_sp,
        n_tp,
    )
    mix_grad, weight, grad_g, grad_u, grad_d = experts_backward(
        arrived,
        expert_gate_weight,
        expert_up_weight,
        expert_down_weight,
        routes.T,
        layer_output_gradient,
        mixer_output_weight.T.reshape(2, -1, mixer_output_weight.shape[0]),
        n_sp,
        n_tp,
    )
    weight = weight.reshape(2, n_sp // 2, -1, mixer_output_weight.shape[0])
    proj_grad, input_grad, step_grad, b_grad, c_grad, gate_grad_in = tail(
        mix_grad,
        weight,
        scan_out,
        normed_low,
        head_mixer_input,
        head_step_size.T,
        rate,
        extra_log_decay.T,
        coming,
        state_input_vectors,
        state_readout_vectors,
        gate_preactivation,
        scale,
        n_sp,
        n_tp,
    )
    proj_grad, input_grad, step_grad, b_grad, c_grad, gate_grad_in, grad_g, grad_u, grad_d = finish(
        proj_grad,
        input_grad,
        step_grad,
        b_grad,
        c_grad,
        gate_grad_in,
        grad_g,
        grad_u,
        grad_d,
    )
    return (
        grad_g,
        grad_u,
        grad_d,
        proj_grad.T,
        input_grad,
        step_grad.T,
        b_grad,
        c_grad,
        gate_grad_in,
    )


def solution(mesh):
    placed = (
        P(SP, "tp"),
        P(SP, "tp"),
        P(SP, None),
        P(SP, None),
        P(SP, None, "tp"),
        P(SP, None, "tp"),
        P(SP, "tp", None),
        P(SP, "tp"),
        P(SP, "tp"),
        P("tp"),
        P(SP, "tp"),
        P("tp", None, None),
        P(SP, "tp"),
        P(SP, "tp"),
        P(SP, "tp"),
        P("tp"),
        P("tp", SP),
    )
    return jax.shard_map(
        functools.partial(body, mesh.shape["sp"], mesh.shape["tp"]),
        mesh=mesh,
        in_specs=placed,
        out_specs=(
            P(SP, None, "tp"),
            P(SP, None, "tp"),
            P(SP, "tp", None),
            P("tp", SP),
            P(SP, "tp"),
            P(SP, "tp"),
            P(SP, "tp"),
            P(SP, "tp"),
            P(SP, "tp"),
        ),
        check_vma=False,
    )
```

```python
import functools

import jax
import jax.numpy as jnp
from jax import lax
from jax.experimental import pallas as pl
from jax.experimental.pallas import tpu as pltpu
from jax.sharding import PartitionSpec as P

HDIM = 64
STATE = 128
SP = "sp"
CAP = 12
MESH = pl.DeviceIdType.MESH
F32 = jnp.float32
BF16 = jnp.bfloat16

norm_eps = 1e-05
VMEM_BYTES = 60 * 1024 * 1024


def vmem_spec():
    return pl.BlockSpec(memory_space=pltpu.VMEM)


def any_spec():
    return pl.BlockSpec(memory_space=pl.ANY)


def dot(a, b, contract=((1,), (0,))):
    return lax.dot_general(a, b, (contract, ((), ())), preferred_element_type=F32)


def iota(shape, dim):
    return lax.broadcasted_iota(jnp.int32, shape, dim)


def divide(x, by):
    return ((x.astype(F32) + 0.5) * (1.0 / by)).astype(jnp.int32)


def slots_in_rows(routes, experts):
    top, tokens = routes.shape
    ids = iota((experts, tokens), 0)
    earlier = (iota((tokens, tokens), 0) < iota((tokens, tokens), 1)).astype(BF16)
    before = jnp.zeros((experts, 1), F32)
    rows = []
    for k in range(top):
        hits = (ids == routes[k : k + 1, :]).astype(F32)
        rank = dot(hits.astype(BF16), earlier) + before
        rows.append(jnp.sum(hits * rank, axis=0, keepdims=True))
        before = before + jnp.sum(hits, axis=1, keepdims=True)
    return [routes[k : k + 1, :] * CAP + rows[k].astype(jnp.int32) for k in range(top)]


def pack(experts, routes_ref, weights_ref, stream_ref, grads_ref, out_ref):
    tokens = stream_ref.shape[0]
    half = stream_ref.shape[1] // 2
    slots = slots_in_rows(routes_ref[...], experts)
    row = iota((experts * 4 * CAP, 1), 0)
    expert = divide(row, 4 * CAP)
    inner = row - expert * (4 * CAP)
    part = divide(inner, CAP)
    slot = expert * CAP + inner - part * CAP
    first = (slot == slots[0]).astype(F32)
    second = (slot == slots[1]).astype(F32)
    match = (first + second).astype(BF16)
    weight = jnp.sum(
        first * weights_ref[0:1, :] + second * weights_ref[1:2, :], axis=1, keepdims=True
    )
    x0 = dot(match, stream_ref[:, :half])
    x1 = dot(match, stream_ref[:, half:])
    g0 = dot(match, grads_ref[:, :half])
    g1 = dot(match, grads_ref[:, half:])
    low = jnp.where(part == 0, x0, g0 * weight)
    high = jnp.where(part == 2, x1, g1 * weight)
    out_ref[...] = jnp.where(part < 2, low, high).astype(BF16).reshape(out_ref.shape)


def hop(i, n_sp):
    return lax.rem(i * 11, n_sp)


def ring_reduce(piece, place, to_right, to_left, from_left, from_right, sum_right, sum_left, sems):
    s_r, s_l, r_l, r_r = sems
    right, left, far = lax.rem(place + 1, 4), lax.rem(place + 3, 4), lax.rem(place + 2, 4)

    def right_copy(k, src):
        return pltpu.make_async_remote_copy(
            src, from_left.at[k], s_r.at[k], r_l.at[k], to_right, MESH
        )

    def left_copy(k, src):
        return pltpu.make_async_remote_copy(
            src, from_right.at[k], s_l.at[k], r_r.at[k], to_left, MESH
        )

    def start():
        right_copy(0, piece(far, 0)).start()
        left_copy(0, piece(far, 1)).start()
        right_copy(1, piece(right, 1)).start()
        left_copy(1, piece(left, 0)).start()

    def middle():
        right_copy(0, piece(far, 0)).wait()
        sum_right[...] = (piece(right, 0)[...].astype(F32) + from_left[0].astype(F32)).astype(BF16)
        left_copy(0, piece(far, 1)).wait()
        sum_left[...] = (piece(left, 1)[...].astype(F32) + from_right[0].astype(F32)).astype(BF16)
        right_copy(2, sum_right).start()
        left_copy(2, sum_left).start()

    def finish():
        right_copy(1, piece(right, 1)).wait()
        left_copy(1, piece(left, 0)).wait()
        right_copy(2, sum_right).wait()
        left_copy(2, sum_left).wait()

    def total(w, at=()):
        near, across = (from_left, from_right) if w == 0 else (from_right, from_left)
        return (
            piece(place, w)[at or Ellipsis].astype(F32)
            + near[(2,) + at].astype(F32)
            + across[(1,) + at].astype(F32)
        )

    return start, middle, finish, total


def greet(me, tp, n_sp, n_tp, ring=False):
    barrier = pltpu.get_barrier_semaphore()

    def hello(d, carry):
        pl.semaphore_signal(
            barrier, inc=1, device_id=(lax.rem(me + d, n_sp), tp), device_id_type=MESH
        )
        return carry

    lax.fori_loop(1, n_sp, hello, 0)
    count = n_sp - 1
    if ring:
        for other in (lax.rem(tp + 1, n_tp), lax.rem(tp + n_tp - 1, n_tp)):
            pl.semaphore_signal(barrier, inc=1, device_id=(me, other), device_id_type=MESH)
        count += 2
    return lambda: pl.semaphore_wait(barrier, count)


def split(x, pieces):
    terms = []
    for _ in range(pieces):
        term = x.astype(BF16)
        terms.append(term)
        x = x - term.astype(F32)
    return terms


def dot_split(x, exact, pieces, contract, left=True):
    total = None
    for term in split(x, pieces):
        part = dot(term, exact, contract) if left else dot(exact, term, contract)
        total = part if total is None else total + part
    return total


def triangle(n, keep):
    return keep(iota((n, n), 0), iota((n, n), 1)).astype(BF16)


def head_spread(heads, size):
    channel, head = iota((heads, heads * size), 1), iota((heads, heads * size), 0)
    return ((channel >= head * size) & (channel < (head + 1) * size)).astype(BF16)


def spread(x, owner):
    return dot_split(x, owner, 2, ((1,), (0,)))


def by_head(x, owner):
    return dot_split(x, owner, 2, ((1,), (1,)))


def cumulative_decay(time_step, rate, extra):
    log_decay = extra - time_step * rate
    upto = triangle(log_decay.shape[0], lambda t, s: s <= t)
    return dot_split(log_decay, upto, 3, ((1,), (0,)), left=False)


def turned(x):
    n = x.shape[1]
    return dot_split(x, triangle(n, lambda a, b: a == b), 3, ((1,), (1,)), left=False)


def decay_between(cum, cum_rows, h):
    gap = cum[:, h : h + 1] - cum_rows[h : h + 1, :]
    n = gap.shape[0]
    return jnp.exp(jnp.where(iota((n, n), 1) <= iota((n, n), 0), gap, -1e30))


def halves(pair):
    lane = iota(pair.shape, 1)
    zero = jnp.zeros_like(pair)
    size = pair.shape[1] // 2
    return jnp.concatenate([jnp.where(lane < size, pair, zero), jnp.where(lane < size, zero, pair)], axis=0)


def front_part(
    n_sp,
    n_tp,
    begin,
    prepare,
    between,
    in_ref,
    x_ref,
    dt_ref,
    rate_ref,
    extra_ref,
    first_hbm,
    b_ref,
    c_ref,
    gate_ref,
    scale_ref,
    out_ref,
    y_ref,
    normed_ref,
    coming,
    decays,
    state_mine,
    decay_mine,
    states,
    carries,
    diag,
    own,
    one,
    two,
    a_send,
    a_recv,
    s_right,
    s_left,
    r_left,
    r_right,
    f_send,
    f_recv,
    sends,
    recvs,
    d_sends,
    d_recvs,
    b_sends,
    b_recvs,
    first_ref,
    first_sem,
):
    me, tp = lax.axis_index("sp"), lax.axis_index("tp")
    entering = pltpu.make_async_copy(first_hbm.at[me], first_ref, first_sem)
    entering.start()
    begin()
    right, left = lax.rem(tp + 1, n_tp), lax.rem(tp + n_tp - 1, n_tp)
    far = lax.rem(tp + 2, n_tp)
    met = greet(me, tp, n_sp, n_tp, ring=True)
    prepare()
    met()

    low, plane = lax.rem(me, 8), lax.div(me, 8)
    away = (0, 1, 3, 2)

    def planes_off(j):
        return lax.rem(plane + 4 - away[j], 4)

    def exchange(j, k):
        to = lax.rem(plane + away[j], 4) * 8 + lax.rem(low + k, 8)
        return pltpu.make_async_remote_copy(
            in_ref.at[to],
            out_ref.at[tp, me],
            a_send.at[8 * j + k],
            a_recv.at[8 * j + k],
            (to, tp),
            MESH,
        )

    def arrived(j, k):
        source = planes_off(j) * 8 + lax.rem(low + 8 - k, 8)
        return pltpu.make_async_remote_copy(
            in_ref.at[me],
            out_ref.at[tp, source],
            a_send.at[8 * j + k],
            a_recv.at[8 * j + k],
            (me, tp),
            MESH,
        )

    def to_right(j, block):
        piece = out_ref.at[block, pl.ds(pl.multiple_of(planes_off(j) * 8, 8), 8)]
        return pltpu.make_async_remote_copy(
            piece, piece, s_right.at[j], r_left.at[j], (me, right), MESH
        )

    def to_left(j, block):
        piece = out_ref.at[block, pl.ds(pl.multiple_of(planes_off(j) * 8, 8), 8)]
        return pltpu.make_async_remote_copy(
            piece, piece, s_left.at[j], r_right.at[j], (me, left), MESH
        )

    def onward(j, block, rightward):
        first = planes_off(j) * 8 + (0 if rightward else 4)
        piece = out_ref.at[block, pl.ds(pl.multiple_of(first, 4), 4)]
        at = j if rightward else 4 + j
        return pltpu.make_async_remote_copy(
            piece, piece, f_send.at[at], f_recv.at[at], (me, right if rightward else left), MESH
        )

    for j in range(4):

        def start_exchange(k, carry, j=j):
            exchange(j, k).start()
            return carry

        lax.fori_loop(1 if j == 0 else 0, 8, start_exchange, 0)

    def pass_on(j):
        def await_chunk(k, carry):
            arrived(j, k).wait_recv()
            return carry

        lax.fori_loop(1 if j == 0 else 0, 8, await_chunk, 0)
        to_right(j, tp).start()
        to_left(j, tp).start()

    mine = pltpu.make_async_copy(in_ref.at[me], out_ref.at[tp, me], own)
    mine.start()

    mine.wait()
    pass_on(0)

    heads, tokens = dt_ref.shape
    channels = x_ref.shape[1]
    groups = b_ref.shape[1] // STATE
    wide = channels // groups
    owner = head_spread(heads, HDIM)
    dt = turned(dt_ref[...])
    cum = cumulative_decay(dt, rate_ref[...], turned(extra_ref[...]))
    cum_rows = turned(cum)
    last = cum[tokens - 1 : tokens, :]
    values = x_ref[...].astype(F32)
    ending = (values * spread(dt * jnp.exp(last - cum), owner)).astype(BF16)
    parts, rows, entries = state_mine.shape
    per_group = parts // groups
    for g in range(groups):
        state = dot(
            ending[:, g * wide : (g + 1) * wide],
            b_ref[:, g * STATE : (g + 1) * STATE],
            ((0,), (0,)),
        )
        state_mine[g * per_group : (g + 1) * per_group] = state.astype(BF16).reshape(
            per_group, rows, entries
        )
    total = jnp.exp(last)
    for p in range(parts):
        h = p * rows // HDIM
        decay_mine[p] = jnp.broadcast_to(total[:, h : h + 1], (1, entries))


    def state_copy(d):
        to = lax.rem(me + d, n_sp)
        return pltpu.make_async_remote_copy(
            state_mine.at[to], states.at[me], sends.at[d], recvs.at[d], (to, tp), MESH
        )

    def decay_copy(d):
        to = lax.rem(me + d, n_sp)
        return pltpu.make_async_remote_copy(
            decay_mine.at[to], decays.at[me], d_sends.at[d], d_recvs.at[d], (to, tp), MESH
        )

    def back_copy(d):
        to = lax.rem(me + d, n_sp)
        return pltpu.make_async_remote_copy(
            carries.at[to], coming.at[me], b_sends.at[d], b_recvs.at[d], (to, tp), MESH
        )

    def start_states(d, carry):
        decay_copy(hop(d, n_sp)).start()
        state_copy(hop(d, n_sp)).start()
        return carry

    lax.fori_loop(1, n_sp, start_states, 0)
    kept = pltpu.make_async_copy(state_mine.at[me], states.at[me], one)
    kept_too = pltpu.make_async_copy(decay_mine.at[me], decays.at[me], two)
    kept.start()
    kept_too.start()

    pass_on(1)

    scaled = (values * spread(dt, owner)).astype(BF16)
    affinity = [
        dot(
            c_ref[:, g * STATE : (g + 1) * STATE],
            b_ref[:, g * STATE : (g + 1) * STATE],
            ((1,), (1,)),
        )
        for g in range(groups)
    ]
    for q in range(heads // 2):
        g = q // (heads // 2 // groups)
        both = jnp.concatenate(
            [(affinity[g] * decay_between(cum, cum_rows, 2 * q + j)).astype(BF16) for j in range(2)],
            axis=1,
        )
        at = slice(q * 2 * HDIM, (q + 1) * 2 * HDIM)
        diag[:, at] = dot(both, halves(scaled[:, at]))
        if q == heads // 4 - 1:
            pass_on(2)
    pass_on(3)

    kept.wait()
    kept_too.wait()

    def finish_states(d, carry):
        decay_copy(d).wait()
        state_copy(d).wait()
        return carry

    lax.fori_loop(1, n_sp, finish_states, 0)
    entering.wait()
    running = first_ref[...]
    for i in range(n_sp):
        carries[i] = running.astype(BF16)
        running = decays[i] * running + states[i].astype(F32)

    def start_back(d, carry):
        back_copy(hop(d, n_sp)).start()
        return carry

    lax.fori_loop(1, n_sp, start_back, 0)
    kept_back = pltpu.make_async_copy(carries.at[me], coming.at[me], one)
    kept_back.start()

    for j in range(4):
        to_right(j, left).wait_recv()
        onward(j, left, True).start()
        to_left(j, right).wait_recv()
        onward(j, right, False).start()
    kept_back.wait()

    def finish_back(d, carry):
        back_copy(d).wait()
        return carry

    lax.fori_loop(1, n_sp, finish_back, 0)
    since = spread(jnp.exp(cum), owner)
    for g in range(groups):
        at = slice(g * wide, (g + 1) * wide)
        incoming = coming[g * per_group : (g + 1) * per_group].reshape(wide, entries)
        y = diag[:, at] + since[:, at] * dot(
            c_ref[:, g * STATE : (g + 1) * STATE], incoming, ((1,), (1,))
        )
        y_ref[:, at] = y
        gate = gate_ref[:, at].astype(F32)
        gated = y * gate * jax.nn.sigmoid(gate)
        factor = lax.rsqrt(jnp.mean(gated * gated, axis=1, keepdims=True) + norm_eps)
        normed_ref[:, at] = (gated * factor * scale_ref[:, at]).astype(BF16)

    between()
    for j in range(4):
        onward(j, far, True).wait()
        onward(j, far, False).wait()
        to_right(j, tp).wait_send()
        to_left(j, tp).wait_send()

        def drain(k, carry, j=j):
            exchange(j, k).wait_send()
            return carry

        lax.fori_loop(1 if j == 0 else 0, 8, drain, 0)


def expert_part(
    n_sp,
    n_tp,
    in_ref,
    gate_hbm,
    up_hbm,
    down_hbm,
    routes_ref,
    grads_ref,
    own_hbm,
    mix_ref,
    all_hbm,
    dgate_hbm,
    dup_hbm,
    ddown_hbm,
    w_gate,
    w_up,
    w_down,
    d_gate,
    d_up,
    d_down,
    x,
    x_t,
    g,
    gate_grad,
    up_grad,
    hidden,
    part_ref,
    from_left,
    from_right,
    sum_right,
    sum_left,
    out_blocks,
    back,
    own_cols,
    loads,
    stores,
    s_r,
    s_l,
    r_l,
    r_r,
    a_send,
    a_recv,
    g_send,
    g_recv,
    local,
    w_own,
    w_sends,
    w_recvs,
    so_far,
):
    me, tp = lax.axis_index("sp"), lax.axis_index("tp")
    right, left = lax.rem(tp + 1, n_tp), lax.rem(tp + n_tp - 1, n_tp)
    far = lax.rem(tp + 2, n_tp)
    tokens, width = grads_ref.shape
    half, quarter = width // 2, width // 4
    model, units = w_gate.shape
    rows = x.shape[0]
    cuts = [(i, min(256, units - i)) for i in range(0, units, 256)]
    fetches = []
    for k, (start, size) in enumerate(cuts):
        at = pl.ds(start, size)
        fetches.append(
            [
                pltpu.make_async_copy(gate_hbm.at[0, :, at], w_gate.at[:, at], loads.at[3 * k]),
                pltpu.make_async_copy(up_hbm.at[0, :, at], w_up.at[:, at], loads.at[3 * k + 1]),
                pltpu.make_async_copy(down_hbm.at[0, at, :], w_down.at[at, :], loads.at[3 * k + 2]),
            ]
        )
        for fetch in fetches[-1]:
            fetch.start()
    yield

    core = lax.rem(me, 2)
    lane_y, lane_z = lax.rem(lax.div(me, 2), 4), lax.div(me, 8)

    def at_y(y):
        return lane_z * 8 + y * 2 + core

    def at_z(z):
        return z * 8 + lane_y * 2 + core

    def weight_copy(k, src, dst, to):
        return pltpu.make_async_remote_copy(
            src, dst, w_sends.at[k], w_recvs.at[k], (to, tp), MESH
        )

    own_weight = pltpu.make_async_copy(own_hbm, all_hbm.at[core, lane_z, lane_y], w_own)
    own_weight.start()

    def first_stage(j, sending):
        y, z = (lane_y, lane_z) if sending else (lax.rem(lane_y + 4 - j, 4), lax.rem(lane_z + 4 - j, 4))
        return [
            weight_copy(
                j - 1, own_hbm.at[0], all_hbm.at[core, lane_z, y, 0], at_y(lax.rem(lane_y + j, 4))
            ),
            weight_copy(
                j + 2, own_hbm.at[1], all_hbm.at[core, z, lane_y, 1], at_z(lax.rem(lane_z + j, 4))
            ),
        ]

    def second_stage(j, sending):
        y, z = (lane_y, lane_z) if sending else (lax.rem(lane_y + 4 - j, 4), lax.rem(lane_z + 4 - j, 4))
        by_z, by_y = all_hbm.at[core, z, :, 0], all_hbm.at[core, :, y, 1]
        return [
            weight_copy(j + 5, by_z, by_z, at_z(lax.rem(lane_z + j, 4))),
            weight_copy(j + 8, by_y, by_y, at_y(lax.rem(lane_y + j, 4))),
        ]

    def third_stage(c):
        return weight_copy(12, all_hbm.at[c], all_hbm.at[c], me + 1 - 2 * core)

    for j in range(1, 4):
        for copy in first_stage(j, True):
            copy.start()

    tall = in_ref.shape[2]
    group_of = 8
    span = group_of * CAP
    spots = iota((1, group_of * tall), 1)
    src = divide(spots, tall)
    inner = spots - src * tall
    which = divide(inner, CAP)
    row = src * CAP + inner - which * CAP
    lines = iota((span, 1), 0)
    pick = [((row == lines) & (which == p)).astype(BF16) for p in range(4)]

    def columns_of(b):
        return pl.ds(pl.multiple_of(b * width, width), width)

    def select(b):
        for k in range(n_sp // group_of):
            block = in_ref[b, k * group_of : (k + 1) * group_of].reshape(group_of * tall, half)
            at = slice(k * span, (k + 1) * span)
            for c in range(2):
                cols = pl.ds(pl.multiple_of(b * width + c * half, half), half)
                x[at, cols] = dot(pick[2 * c], block).astype(BF16)
                g[at, cols] = dot(pick[2 * c + 1], block).astype(BF16)

    def products(b, at):
        cols = columns_of(b)
        return (
            dot(x[:, cols], w_gate[cols, at]),
            dot(x[:, cols], w_up[cols, at]),
            dot(g[:, cols], w_down[at, cols], ((1,), (1,))),
        )

    near = (tp, left, right)
    for b in near:
        select(b)
    for k, (start, size) in enumerate(cuts):
        for fetch in fetches[k]:
            fetch.wait()
        at = slice(start, start + size)
        sums = [products(b, at) for b in near]
        for i in range(3):
            so_far[i, :, at] = sums[0][i] + sums[1][i] + sums[2][i]
    yield
    select(far)
    for start, size in cuts:
        at = slice(start, start + size)
        last_gate, last_up, last_grad = products(far, at)
        pre_gate = so_far[0, :, at] + last_gate
        pre_up = so_far[1, :, at] + last_up
        hidden_grad = so_far[2, :, at] + last_grad
        sigmoid_gate = jax.nn.sigmoid(pre_gate)
        activated = pre_gate * sigmoid_gate
        hidden[:, at] = (activated * pre_up).astype(BF16)
        gate_grad[:, at] = (
            hidden_grad * pre_up * sigmoid_gate * (1.0 + pre_gate * (1.0 - sigmoid_gate))
        ).astype(BF16)
        up_grad[:, at] = (hidden_grad * activated).astype(BF16)

    own_weight.wait()
    for j in range(1, 4):
        for copy in first_stage(j, False):
            copy.wait_recv()
    for j in range(1, 4):
        for copy in second_stage(j, True):
            copy.start()

    def row_block(b):
        for c in range(2):
            cols = pl.ds(pl.multiple_of(b * width + c * half, half), half)
            part_ref[2 * b + c] = (
                dot(gate_grad[...], w_gate[cols, :], ((1,), (1,)))
                + dot(up_grad[...], w_up[cols, :], ((1,), (1,)))
            ).astype(BF16)

    def block(b, which):
        return part_ref.at[2 * b + which]

    def right_copy(k, src):
        return pltpu.make_async_remote_copy(
            src, from_left.at[k], s_r.at[k], r_l.at[k], (me, right), MESH
        )

    def left_copy(k, src):
        return pltpu.make_async_remote_copy(
            src, from_right.at[k], s_l.at[k], r_r.at[k], (me, left), MESH
        )

    row_block(far)
    row_block(right)
    right_copy(0, block(far, 0)).start()
    left_copy(0, block(far, 1)).start()
    row_block(left)
    right_copy(1, block(right, 1)).start()
    row_block(tp)
    left_copy(1, block(left, 0)).start()

    saves = []

    def save(k, src, dst):
        copy = pltpu.make_async_copy(src, dst, stores.at[k])
        copy.start()
        saves.append(copy)

    def passed_right():
        right_copy(0, block(far, 0)).wait()
        sum_right[...] = (block(right, 0)[...].astype(F32) + from_left[0].astype(F32)).astype(BF16)
        left_copy(0, block(far, 1)).wait()
        sum_left[...] = (block(left, 1)[...].astype(F32) + from_right[0].astype(F32)).astype(BF16)

    def gate_up_rows(i):
        at = slice(i * 256, (i + 1) * 256)
        x_t[at, :] = jnp.transpose(x[:, at])
        d_gate[at, :] = dot(x_t[at, :], gate_grad[...]).astype(BF16)
        save(2 * i, d_gate.at[at, :], dgate_hbm.at[0, at, :])
        d_up[at, :] = dot(x_t[at, :], up_grad[...]).astype(BF16)
        save(2 * i + 1, d_up.at[at, :], dup_hbm.at[0, at, :])

    for i in range(4):
        gate_up_rows(i)
    passed_right()
    right_copy(2, sum_right).start()
    left_copy(2, sum_left).start()
    for i in range(4, 8):
        gate_up_rows(i)

    for k, (start, size) in enumerate(cuts):
        at = slice(start, start + size)
        d_down[at, :] = dot(hidden[:, at], g[...], ((0,), (0,))).astype(BF16)
        save(16 + k, d_down.at[at, :], ddown_hbm.at[0, at, :])

    for j in range(1, 4):
        for copy in second_stage(j, False):
            copy.wait_recv()
    third_stage(core).start()

    by_token = slots_in_rows(routes_ref[...], n_sp)
    line = iota((8, tokens), 0)
    slots = turned(
        jnp.where(line == 0, by_token[0], jnp.where(line == 1, by_token[1], 0)).astype(F32)
    ).astype(jnp.int32)
    column = iota((1, n_sp * 4 * CAP), 1)
    expert = divide(column, 4 * CAP)
    place_in = column - expert * (4 * CAP)
    piece = divide(place_in, CAP)
    slot = expert * CAP + place_in - piece * CAP
    match = (slots[:, 0:1] == slot) | (slots[:, 1:2] == slot)

    right_copy(1, block(right, 1)).wait()
    left_copy(1, block(left, 0)).wait()
    right_copy(2, sum_right).wait()
    left_copy(2, sum_left).wait()

    tall_out = iota((group_of * 4 * CAP, 1), 0)
    out_src = divide(tall_out, 4 * CAP)
    out_in = tall_out - out_src * (4 * CAP)
    out_piece = divide(out_in, CAP)
    out_row = out_src * CAP + out_in - out_piece * CAP
    pair_at = iota((1, span), 1)
    place = [((out_row == pair_at) & (out_piece == c)).astype(BF16) for c in range(4)]
    for k in range(rows // span):
        at = slice(k * span, (k + 1) * span)
        low = (
            part_ref[2 * tp, at, :].astype(F32)
            + from_left[2, at, :].astype(F32)
            + from_right[1, at, :].astype(F32)
        ).astype(BF16)
        high = (
            part_ref[2 * tp + 1, at, :].astype(F32)
            + from_right[2, at, :].astype(F32)
            + from_left[1, at, :].astype(F32)
        ).astype(BF16)
        laid = (
            dot(place[0], low[:, :quarter])
            + dot(place[1], low[:, quarter:])
            + dot(place[2], high[:, :quarter])
            + dot(place[3], high[:, quarter:])
        )
        out_blocks[k * group_of : (k + 1) * group_of] = laid.astype(BF16).reshape(
            group_of, 4 * CAP, quarter
        )

    def exchange(d):
        to = lax.rem(me + d, n_sp)
        return pltpu.make_async_remote_copy(
            out_blocks.at[to], back.at[me], a_send.at[d], a_recv.at[d], (to, tp), MESH
        )

    def start_exchange(d, carry):
        exchange(hop(d, n_sp)).start()
        return carry

    lax.fori_loop(1, n_sp, start_exchange, 0)
    mine = pltpu.make_async_copy(out_blocks.at[me], back.at[me], local)
    mine.start()
    mine.wait()

    def finish_exchange(d, carry):
        exchange(d).wait()
        return carry

    lax.fori_loop(1, n_sp, finish_exchange, 0)
    returned = back[...].reshape(n_sp * 4 * CAP, quarter)
    for c in range(4):
        chosen = jnp.where(match & (piece == c), 1.0, 0.0).astype(BF16)
        cols = slice(c * quarter, (c + 1) * quarter)
        own_cols[:, cols] = (grads_ref[:, cols].astype(F32) + dot(chosen, returned)).astype(BF16)

    def spot(b):
        return mix_ref.at[:, pl.ds(pl.multiple_of(b * width, width), width)]

    def spot_half(b, which):
        return mix_ref.at[:, pl.ds(pl.multiple_of(b * width + which * half, half), half)]

    def gather(k, src, dst, to):
        return pltpu.make_async_remote_copy(
            src, dst, g_send.at[k], g_recv.at[k], (me, to), MESH
        )

    gather(0, own_cols, spot(tp), right).start()
    gather(1, own_cols, spot(tp), left).start()
    spot(tp)[...] = own_cols[...]
    gather(0, own_cols, spot(left), right).wait_recv()
    gather(2, spot_half(left, 0), spot_half(left, 0), right).start()
    gather(1, own_cols, spot(right), left).wait_recv()
    gather(3, spot_half(right, 1), spot_half(right, 1), left).start()
    gather(2, spot_half(far, 0), spot_half(far, 0), right).wait()
    gather(3, spot_half(far, 1), spot_half(far, 1), left).wait()
    gather(0, own_cols, spot(tp), right).wait_send()
    gather(1, own_cols, spot(tp), left).wait_send()
    for copy in saves:
        copy.wait()
    for j in range(1, 4):
        for copy in first_stage(j, True) + second_stage(j, True):
            copy.wait_send()
    third_stage(core).wait_send()
    third_stage(1 - core).wait_recv()


FRONT_SCRATCH = 24


def main_kernel(n_sp, n_tp, *refs):
    (stream, weights, x, dt, rate, extra, first, b, c, gate, scale) = refs[:11]
    (w_gate, w_up, w_down, routes, grads, own) = refs[11:17]
    (y, normed, coming, decays) = refs[17:21]
    expert_outs = refs[21:26]
    packed, arrived = refs[26:28]
    front_scratch = refs[28 : 28 + FRONT_SCRATCH]
    expert_scratch = refs[28 + FRONT_SCRATCH :]
    steps = expert_part(
        n_sp,
        n_tp,
        arrived,
        w_gate,
        w_up,
        w_down,
        routes,
        grads,
        own,
        *expert_outs,
        *expert_scratch,
    )
    front_part(
        n_sp,
        n_tp,
        lambda: next(steps),
        lambda: pack(n_sp, routes, weights, stream, grads, packed),
        lambda: next(steps),
        packed,
        x,
        dt,
        rate,
        extra,
        first,
        b,
        c,
        gate,
        scale,
        arrived,
        y,
        normed,
        coming,
        decays,
        *front_scratch,
    )
    for _ in steps:
        pass


def main(
    stream, weights, x, dt, rate, extra, first, b, c, gate, scale, w_gate, w_up, w_down, routes, grads, own, n_sp, n_tp
):
    dma = pltpu.SemaphoreType.DMA
    tokens, channels = x.shape
    _, rows, entries = first.shape
    _, model, units = w_gate.shape
    pairs = n_sp * CAP
    width = grads.shape[1]
    half, quarter = width // 2, width // 4
    front_scratch = (
        [
            pltpu.VMEM((n_sp, rows, entries), BF16),
            pltpu.VMEM((n_sp, 1, entries), F32),
            pltpu.VMEM((n_sp, rows, entries), BF16),
            pltpu.VMEM((n_sp, rows, entries), BF16),
            pltpu.VMEM((tokens, channels), F32),
            dma,
            dma,
            dma,
        ]
        + [dma((n_sp,))] * 2
        + [dma((4,))] * 4
        + [dma((8,))] * 2
        + [dma((n_sp,))] * 6
        + [pltpu.VMEM((rows, entries), F32), dma]
    )
    expert_scratch = [
        pltpu.VMEM((model, units), BF16),
        pltpu.VMEM((model, units), BF16),
        pltpu.VMEM((units, model), BF16),
        pltpu.VMEM((model, units), BF16),
        pltpu.VMEM((model, units), BF16),
        pltpu.VMEM((units, model), BF16),
        pltpu.VMEM((pairs, model), BF16),
        pltpu.VMEM((model, pairs), BF16),
        pltpu.VMEM((pairs, model), BF16),
        pltpu.VMEM((pairs, units), BF16),
        pltpu.VMEM((pairs, units), BF16),
        pltpu.VMEM((pairs, units), BF16),
        pltpu.VMEM((2 * n_tp, pairs, half), BF16),
        pltpu.VMEM((3, pairs, half), BF16),
        pltpu.VMEM((3, pairs, half), BF16),
        pltpu.VMEM((pairs, half), BF16),
        pltpu.VMEM((pairs, half), BF16),
        pltpu.VMEM((n_sp, 4 * CAP, quarter), BF16),
        pltpu.VMEM((n_sp, 4 * CAP, quarter), BF16),
        pltpu.VMEM((tokens, width), BF16),
        dma((12,)),
        dma((20,)),
        dma((3,)),
        dma((3,)),
        dma((3,)),
        dma((3,)),
        dma((n_sp,)),
        dma((n_sp,)),
        dma((4,)),
        dma((4,)),
        dma,
        dma,
        dma((13,)),
        dma((13,)),
        pltpu.VMEM((3, pairs, units), F32),
    ]
    return pl.pallas_call(
        functools.partial(main_kernel, n_sp, n_tp),
        out_shape=(
            jax.ShapeDtypeStruct((tokens, channels), F32),
            jax.ShapeDtypeStruct((tokens, channels), BF16),
            jax.ShapeDtypeStruct((n_sp, rows, entries), BF16),
            jax.ShapeDtypeStruct((n_sp, 1, entries), F32),
            jax.ShapeDtypeStruct((tokens, width * n_tp), BF16),
            jax.ShapeDtypeStruct((2, 4, 4) + own.shape, BF16),
            jax.ShapeDtypeStruct(w_gate.shape, BF16),
            jax.ShapeDtypeStruct(w_up.shape, BF16),
            jax.ShapeDtypeStruct(w_down.shape, BF16),
        ),
        in_specs=[vmem_spec()] * 6
        + [any_spec()]
        + [vmem_spec()] * 4
        + [any_spec()] * 3
        + [vmem_spec()] * 2
        + [any_spec()],
        out_specs=(vmem_spec(),) * 5 + (any_spec(),) * 4,
        scratch_shapes=[
            pltpu.VMEM((n_sp, 4 * CAP, half), BF16),
            pltpu.VMEM((n_tp, n_sp, 4 * CAP, half), BF16),
        ]
        + front_scratch
        + expert_scratch,
        compiler_params=pltpu.CompilerParams(
            collective_id=0, has_side_effects=True, vmem_limit_bytes=VMEM_BYTES
        ),
        name="main",
    )(
        stream, weights, x, dt, rate, extra, first, b, c, gate, scale, w_gate, w_up, w_down, routes, grads, own
    )


def tail_kernel(
    n_sp,
    n_tp,
    mix_ref,
    weight_hbm,
    y_ref,
    normed_ref,
    x_ref,
    dt_ref,
    rate_ref,
    extra_ref,
    coming_ref,
    decays,
    b_ref,
    c_ref,
    gate_ref,
    scale_ref,
    proj_ref,
    dx_ref,
    ddt_ref,
    db_ref,
    dc_ref,
    dgate_ref,
    weight,
    normed2,
    mix2,
    parts,
    big_in,
    big_sum,
    small_in,
    small_sum,
    reduced,
    total,
    state_mine,
    states,
    carries,
    later,
    d_scaled,
    one,
    load,
    p_send,
    p_recv,
    ring_sems,
    sends,
    recvs,
    b_sends,
    b_recvs,
):
    me, tp = lax.axis_index("sp"), lax.axis_index("tp")
    core = lax.rem(me, 2)
    partner = me + 1 - 2 * core
    chip = lax.div(me, 2)
    chips = n_sp // 2
    fetches = [
        pltpu.make_async_copy(weight_hbm.at[c], weight.at[:, c], load.at[c]) for c in range(2)
    ]
    for fetch in fetches:
        fetch.start()
    met = greet(me, tp, n_sp, n_tp)
    heads, tokens = dt_ref.shape
    channels = x_ref.shape[1]
    groups = b_ref.shape[1] // STATE
    wide = channels // groups
    half = channels // 2
    cols = proj_ref.shape[0]
    n_parts, rows, entries = state_mine.shape
    per_group = n_parts // groups

    def pair(k, src, dst):
        return pltpu.make_async_remote_copy(
            src, dst, p_send.at[k], p_recv.at[k], (partner, tp), MESH
        )

    def mine(c):
        return pl.ds(pl.multiple_of(c * half, half), half)

    owner = head_spread(heads, HDIM)
    dt = turned(dt_ref[...])
    cum = cumulative_decay(dt, rate_ref[...], turned(extra_ref[...]))
    cum_rows = turned(cum)
    last = cum[tokens - 1 : tokens, :]
    since = spread(jnp.exp(cum), owner)

    for fetch in fetches:
        fetch.wait()
    whole_weight = weight[...].reshape(mix_ref.shape[1], channels)
    normed_grads = [
        dot(mix_ref[...], whole_weight[:, g * wide : (g + 1) * wide]) for g in range(groups)
    ]
    mix_t = jnp.transpose(mix_ref[...])
    met()
    pair(0, normed_ref.at[:, mine(1 - core)], normed2).start()
    pair(1, mix_ref, mix2).start()
    d_y = []
    for g in range(groups):
        at = slice(g * wide, (g + 1) * wide)
        normed_grad = normed_grads[g]
        y = y_ref[:, at]
        gate = gate_ref[:, at].astype(F32)
        sigmoid_gate = jax.nn.sigmoid(gate)
        activated = gate * sigmoid_gate
        gated = y * activated
        factor = lax.rsqrt(jnp.mean(gated * gated, axis=1, keepdims=True) + norm_eps)
        scaled_grad = normed_grad * scale_ref[:, at]
        along = jnp.mean(scaled_grad * gated, axis=1, keepdims=True) * factor * factor
        gated_grad = factor * (scaled_grad - gated * along)
        d_y.append(gated_grad * activated)
        dgate_ref[:, at] = (
            gated_grad * y * (sigmoid_gate * (1.0 + gate * (1.0 - sigmoid_gate)))
        ).astype(BF16)
    d_out = jnp.concatenate(d_y, axis=1)
    since_grad = since * d_out
    since_low = since_grad.astype(BF16)
    for g in range(groups):
        state = dot(
            since_low[:, g * wide : (g + 1) * wide],
            c_ref[:, g * STATE : (g + 1) * STATE],
            ((0,), (0,)),
        )
        state_mine[g * per_group : (g + 1) * per_group] = state.astype(BF16).reshape(
            per_group, rows, entries
        )
    whole = jnp.exp(last)

    def state_copy(d):
        to = lax.rem(me + d, n_sp)
        return pltpu.make_async_remote_copy(
            state_mine.at[to], states.at[me], sends.at[d], recvs.at[d], (to, tp), MESH
        )

    def back_copy(d):
        to = lax.rem(me + d, n_sp)
        return pltpu.make_async_remote_copy(
            carries.at[to], later.at[me], b_sends.at[d], b_recvs.at[d], (to, tp), MESH
        )

    def start_states(d, carry):
        state_copy(hop(d, n_sp)).start()
        return carry

    lax.fori_loop(1, n_sp, start_states, 0)
    kept = pltpu.make_async_copy(state_mine.at[me], states.at[me], one)
    kept.start()

    pair(0, normed_ref.at[:, mine(1 - core)], normed2).wait()
    pair(1, mix_ref, mix2).wait()
    both_mix = jnp.concatenate([mix_t, jnp.transpose(mix2[...])], axis=1)
    both_normed = jnp.concatenate([normed_ref[:, mine(core)], normed2[...]], axis=0)
    piece_rows = cols // 2
    for z in range(4):
        at = slice(z * 8 * cols, (z + 1) * 8 * cols)
        parts[z] = (
            dot(both_mix[at, :], both_normed).astype(BF16).reshape(4, 2, 2, piece_rows, half)
        )

    lane_y, lane_z = lax.rem(chip, 4), lax.div(chip, 4)

    def at_y(y):
        return (lane_z * 8 + lax.rem(y, 4) * 2 + core, tp)

    def at_z(z):
        return (lax.rem(z, 4) * 8 + lane_y * 2 + core, tp)

    y_ring = (lane_y, at_y(lane_y + 1), at_y(lane_y + 3))
    z_ring = (lane_z, at_z(lane_z + 1), at_z(lane_z + 3))

    def four(ref, k):
        return [ref.at[k, i] for i in range(4)]

    def bufs(landing, sums, k):
        return [landing.at[k, 0], landing.at[k, 1], sums.at[k, 0], sums.at[k, 1]]

    stages = [
        ring_reduce(lambda b, w: parts.at[:, b, 0, w], *y_ring, *bufs(big_in, big_sum, 0), four(ring_sems, 0)),
        ring_reduce(lambda b, w: parts.at[b, :, 1, w], *z_ring, *bufs(big_in, big_sum, 1), four(ring_sems, 1)),
        ring_reduce(lambda b, w: reduced.at[0, w, b], *z_ring, *bufs(small_in, small_sum, 0), four(ring_sems, 2)),
        ring_reduce(lambda b, w: reduced.at[1, w, b], *y_ring, *bufs(small_in, small_sum, 1), four(ring_sems, 3)),
    ]
    stages[0][0]()
    stages[1][0]()


    values = x_ref[...].astype(F32)
    steps = spread(dt, owner)
    scaled = values * steps
    scaled_low = scaled.astype(BF16)
    d_low = d_out.astype(BF16)
    not_before = triangle(tokens, lambda t, s: s >= t)
    below = (iota((tokens, tokens), 1) < iota((tokens, tokens), 0)).astype(F32)
    head_lane = iota((1, heads), 1)
    crossing = [jnp.zeros((tokens, heads), F32)]
    d_affinity = []

    def inside(g):
        affinity = dot(
            c_ref[:, g * STATE : (g + 1) * STATE],
            b_ref[:, g * STATE : (g + 1) * STATE],
            ((1,), (1,)),
        )
        sum_affinity = jnp.zeros((tokens, tokens), F32)
        first = g * (heads // 2 // groups)
        for q in range(first, first + heads // 2 // groups):
            at = slice(q * 2 * HDIM, (q + 1) * 2 * HDIM)
            d_halves = halves(d_low[:, at])
            d_weights = dot(d_halves, scaled_low[:, at], ((1,), (1,)))
            weights, moved = [], []
            for j in range(2):
                between = decay_between(cum, cum_rows, 2 * q + j)
                weights.append((affinity * between).astype(BF16))
                d_between = d_weights[j * tokens : (j + 1) * tokens] * between
                sum_affinity = sum_affinity + d_between
                moved.append((d_between * affinity).astype(BF16))
            d_scaled[:, at] = dot(jnp.concatenate(weights, axis=0), d_halves, ((0,), (0,)))
            reach = dot(not_before, jnp.concatenate(moved, axis=1))
            for j in range(2):
                over = jnp.sum(
                    reach[:, j * tokens : (j + 1) * tokens] * below, axis=1, keepdims=True
                )
                crossing[0] = crossing[0] + jnp.where(head_lane == 2 * q + j, over, 0.0)
        d_affinity.append(sum_affinity.astype(BF16))

    inside(0)
    kept.wait()

    def finish_states(d, carry):
        state_copy(d).wait()
        return carry

    lax.fori_loop(1, n_sp, finish_states, 0)
    running = jnp.zeros((rows, entries), F32)
    for step in range(n_sp):
        i = n_sp - 1 - step
        carries[i] = running.astype(BF16)
        running = decays[i] * running + states[i].astype(F32)

    def start_back(d, carry):
        back_copy(hop(d, n_sp)).start()
        return carry

    lax.fori_loop(1, n_sp, start_back, 0)
    kept_back = pltpu.make_async_copy(carries.at[me], later.at[me], one)
    kept_back.start()

    for g in range(1, groups):
        inside(g)
    stages[0][1]()
    stages[1][1]()
    read_out = []
    for g in range(groups):
        at = slice(g * wide, (g + 1) * wide)
        by = slice(g * STATE, (g + 1) * STATE)
        incoming = coming_ref[g * per_group : (g + 1) * per_group].reshape(wide, entries)
        read_out.append(dot(c_ref[:, by], incoming, ((1,), (1,))))
        dc_ref[:, by] = (
            dot(d_affinity[g], b_ref[:, by]) + dot(since_low[:, at], incoming)
        ).astype(BF16)
    for k in range(2):
        stages[k][2]()
        for w in range(2):
            reduced[k, w] = stages[k][3](w).astype(BF16)
    stages[2][0]()
    stages[3][0]()
    reading = by_head(since_grad * jnp.concatenate(read_out, axis=1), owner)

    kept_back.wait()

    def finish_back(d, carry):
        back_copy(d).wait()
        return carry

    lax.fori_loop(1, n_sp, finish_back, 0)
    until = spread(jnp.exp(last - cum), owner)
    ending = scaled * until
    ending_low = ending.astype(BF16)
    from_later = []
    for g in range(groups):
        at = slice(g * wide, (g + 1) * wide)
        by = slice(g * STATE, (g + 1) * STATE)
        after = later[g * per_group : (g + 1) * per_group].reshape(wide, entries)
        from_later.append(dot(b_ref[:, by], after, ((1,), (1,))))
        db_ref[:, by] = (
            dot(d_affinity[g], c_ref[:, by], ((0,), (0,))) + dot(ending_low[:, at], after)
        ).astype(BF16)
    stages[2][1]()
    stages[3][1]()
    closing = jnp.concatenate(from_later, axis=1)
    gradient = d_scaled[...] + until * closing
    dx_ref[...] = (gradient * steps).astype(BF16)
    direct = by_head(gradient * values, owner)
    stored = by_head(ending * closing, owner)
    kept_state = jnp.sum(
        (
            coming_ref[...].astype(F32).reshape(heads, HDIM, entries)
            * later[...].astype(F32).reshape(heads, HDIM, entries)
        ),
        axis=1,
    )
    passing = dot_split(
        kept_state, jnp.ones((8, entries), BF16), 3, ((1,), (1,)), left=False
    )[0:1, :]
    earlier = triangle(tokens, lambda t, s: s < t)
    d_decay = (
        crossing[0]
        + dot_split(reading, not_before, 3, ((1,), (0,)), left=False)
        + dot_split(stored, earlier, 3, ((1,), (0,)), left=False)
        + passing * whole
    )
    ddt_ref[...] = turned(direct - d_decay * rate_ref[...])

    for k in range(2):
        stages[2 + k][2]()
        for w in range(2):
            first = (2 * k + w) * piece_rows
            total[first : first + piece_rows, :] = stages[2 + k][3](w)

    def lines(c):
        return pl.ds(pl.multiple_of(c * cols, cols), cols)

    given = pair(2, total.at[lines(1 - core), :], proj_ref.at[:, mine(core)])
    given.start()
    proj_ref[:, mine(core)] = total[lines(core), :]
    given.wait_send()
    pair(2, total.at[lines(core), :], proj_ref.at[:, mine(1 - core)]).wait_recv()


def tail(
    mix, weight, y, normed, x, dt, rate, extra, coming, decays, b, c, gate, scale, n_sp, n_tp
):
    dma = pltpu.SemaphoreType.DMA
    tokens, channels = x.shape
    heads = dt.shape[0]
    _, rows, entries = coming.shape
    width = mix.shape[1]
    half = channels // 2
    chips = n_sp // 2
    cols = width // n_sp
    return pl.pallas_call(
        functools.partial(tail_kernel, n_sp, n_tp),
        out_shape=(
            jax.ShapeDtypeStruct((cols, channels), F32),
            jax.ShapeDtypeStruct((tokens, channels), BF16),
            jax.ShapeDtypeStruct((heads, tokens), F32),
            jax.ShapeDtypeStruct(b.shape, BF16),
            jax.ShapeDtypeStruct(c.shape, BF16),
            jax.ShapeDtypeStruct((tokens, channels), BF16),
        ),
        in_specs=[vmem_spec(), any_spec()] + [vmem_spec()] * 12,
        out_specs=(vmem_spec(),) * 6,
        scratch_shapes=[
            pltpu.VMEM((chips, 2, cols, channels), BF16),
            pltpu.VMEM((tokens, half), BF16),
            pltpu.VMEM((tokens, width), BF16),
            pltpu.VMEM((4, 4, 2, 2, cols // 2, half), BF16),
            pltpu.VMEM((2, 2, 3, 4, cols // 2, half), BF16),
            pltpu.VMEM((2, 2, 4, cols // 2, half), BF16),
            pltpu.VMEM((2, 2, 3, cols // 2, half), BF16),
            pltpu.VMEM((2, 2, cols // 2, half), BF16),
            pltpu.VMEM((2, 2, 4, cols // 2, half), BF16),
            pltpu.VMEM((2 * cols, half), F32),
            pltpu.VMEM((n_sp, rows, entries), BF16),
            pltpu.VMEM((n_sp, rows, entries), BF16),
            pltpu.VMEM((n_sp, rows, entries), BF16),
            pltpu.VMEM((n_sp, rows, entries), BF16),
            pltpu.VMEM((tokens, channels), F32),
            dma,
            dma((2,)),
            dma((3,)),
            dma((3,)),
            dma((4, 4, 3)),
        ]
        + [dma((n_sp,))] * 4,
        compiler_params=pltpu.CompilerParams(
            collective_id=2, has_side_effects=True, vmem_limit_bytes=VMEM_BYTES
        ),
        name="tail",
    )(mix, weight, y, normed, x, dt, rate, extra, coming, decays, b, c, gate, scale)


def finish_kernel(count, *refs):
    sources, results, held = refs[:count], refs[count : 2 * count], refs[2 * count : 3 * count]
    loads, stores = refs[3 * count :]
    copies = []
    for i in range(count):
        lines = sources[i].shape[-2]
        pieces = 4 if lines > 512 else 1
        for p in range(pieces):
            at = pl.ds(p * (lines // pieces), lines // pieces)
            views = [
                ref.at[0, at, :] if len(ref.shape) == 3 else ref.at[at, :]
                for ref in (sources[i], held[i], results[i])
            ]
            k = len(copies)
            copies.append(
                (
                    pltpu.make_async_copy(views[0], views[1], loads.at[k]),
                    pltpu.make_async_copy(views[1], views[2], stores.at[k]),
                )
            )
    for load, _ in copies:
        load.start()
    for load, store in copies:
        load.wait()
        store.start()
    for _, store in copies:
        store.wait()


def finish(*arrays):
    count = len(arrays)
    dma = pltpu.SemaphoreType.DMA
    return pl.pallas_call(
        functools.partial(finish_kernel, count),
        out_shape=tuple(jax.ShapeDtypeStruct(a.shape, a.dtype) for a in arrays),
        in_specs=[any_spec()] * count,
        out_specs=(any_spec(),) * count,
        scratch_shapes=[pltpu.VMEM(a.shape, a.dtype) for a in arrays]
        + [dma((4 * count,)), dma((4 * count,))],
        compiler_params=pltpu.CompilerParams(vmem_limit_bytes=VMEM_BYTES),
        name="finish",
    )(*arrays)


def body(
    n_sp,
    n_tp,
    mixer_output_stream,
    layer_output_gradient,
    routes,
    expert_combine_weight,
    expert_gate_weight,
    expert_up_weight,
    expert_down_weight,
    head_mixer_input,
    head_step_size,
    head_decay_rate,
    extra_log_decay,
    state_entering_span,
    state_input_vectors,
    state_readout_vectors,
    gate_preactivation,
    group_norm_scale,
    mixer_output_weight,
):
    heads = head_step_size.shape[1]
    part_rows = heads * HDIM // n_sp
    entering = state_entering_span.reshape(n_sp, part_rows, STATE)
    rate = head_decay_rate[None, :]
    scale = group_norm_scale[None, :]
    scan_out, normed_low, coming, decays, mix_grad, weight, grad_g, grad_u, grad_d = main(
        mixer_output_stream,
        expert_combine_weight.T,
        head_mixer_input,
        head_step_size.T,
        rate,
        extra_log_decay.T,
        entering,
        state_input_vectors,
        state_readout_vectors,
        gate_preactivation,
        scale,
        expert_gate_weight,
        expert_up_weight,
        expert_down_weight,
        routes.T,
        layer_output_gradient,
        mixer_output_weight.T.reshape(2, -1, mixer_output_weight.shape[0]),
        n_sp,
        n_tp,
    )
    weight = weight.reshape(2, n_sp // 2, -1, mixer_output_weight.shape[0])
    proj_grad, input_grad, step_grad, b_grad, c_grad, gate_grad_in = tail(
        mix_grad,
        weight,
        scan_out,
        normed_low,
        head_mixer_input,
        head_step_size.T,
        rate,
        extra_log_decay.T,
        coming,
        decays,
        state_input_vectors,
        state_readout_vectors,
        gate_preactivation,
        scale,
        n_sp,
        n_tp,
    )
    proj_grad, input_grad, step_grad, b_grad, c_grad, gate_grad_in, grad_g, grad_u, grad_d = finish(
        proj_grad,
        input_grad,
        step_grad,
        b_grad,
        c_grad,
        gate_grad_in,
        grad_g,
        grad_u,
        grad_d,
    )
    return (
        grad_g,
        grad_u,
        grad_d,
        proj_grad.T,
        input_grad,
        step_grad.T,
        b_grad,
        c_grad,
        gate_grad_in,
    )


def solution(mesh):
    placed = (
        P(SP, "tp"),
        P(SP, "tp"),
        P(SP, None),
        P(SP, None),
        P(SP, None, "tp"),
        P(SP, None, "tp"),
        P(SP, "tp", None),
        P(SP, "tp"),
        P(SP, "tp"),
        P("tp"),
        P(SP, "tp"),
        P("tp", None, None),
        P(SP, "tp"),
        P(SP, "tp"),
        P(SP, "tp"),
        P("tp"),
        P("tp", SP),
    )
    return jax.shard_map(
        functools.partial(body, mesh.shape["sp"], mesh.shape["tp"]),
        mesh=mesh,
        in_specs=placed,
        out_specs=(
            P(SP, None, "tp"),
            P(SP, None, "tp"),
            P(SP, "tp", None),
            P("tp", SP),
            P(SP, "tp"),
            P(SP, "tp"),
            P(SP, "tp"),
            P(SP, "tp"),
            P(SP, "tp"),
        ),
        check_vma=False,
    )
```

```python
import functools

import jax
import jax.numpy as jnp
from jax import lax
from jax.experimental import pallas as pl
from jax.experimental.pallas import tpu as pltpu
from jax.sharding import PartitionSpec as P

HDIM = 64
STATE = 128
SP = "sp"
CAP = 12
MESH = pl.DeviceIdType.MESH
F32 = jnp.float32
BF16 = jnp.bfloat16

norm_eps = 1e-05
VMEM_BYTES = 67043328 - 1024 * 1024


def vmem_spec():
    return pl.BlockSpec(memory_space=pltpu.VMEM)


def any_spec():
    return pl.BlockSpec(memory_space=pl.ANY)


def dot(a, b, contract=((1,), (0,))):
    return lax.dot_general(a, b, (contract, ((), ())), preferred_element_type=F32)


def iota(shape, dim):
    return lax.broadcasted_iota(jnp.int32, shape, dim)


def divide(x, by):
    return ((x.astype(F32) + 0.5) * (1.0 / by)).astype(jnp.int32)


def slots_in_rows(routes, experts):
    top, tokens = routes.shape
    ids = iota((experts, tokens), 0)
    earlier = (iota((tokens, tokens), 0) < iota((tokens, tokens), 1)).astype(BF16)
    before = jnp.zeros((experts, 1), F32)
    rows = []
    for k in range(top):
        hits = (ids == routes[k : k + 1, :]).astype(F32)
        rank = dot(hits.astype(BF16), earlier) + before
        rows.append(jnp.sum(hits * rank, axis=0, keepdims=True))
        before = before + jnp.sum(hits, axis=1, keepdims=True)
    return [routes[k : k + 1, :] * CAP + rows[k].astype(jnp.int32) for k in range(top)]


def pack(experts, routes_ref, weights_ref, stream_ref, grads_ref, out_ref):
    tokens = stream_ref.shape[0]
    half = stream_ref.shape[1] // 2
    slots = slots_in_rows(routes_ref[...], experts)
    row = iota((experts * 4 * CAP, 1), 0)
    expert = divide(row, 4 * CAP)
    inner = row - expert * (4 * CAP)
    part = divide(inner, CAP)
    slot = expert * CAP + inner - part * CAP
    first = (slot == slots[0]).astype(F32)
    second = (slot == slots[1]).astype(F32)
    match = (first + second).astype(BF16)
    weight = jnp.sum(
        first * weights_ref[0:1, :] + second * weights_ref[1:2, :], axis=1, keepdims=True
    )
    x0 = dot(match, stream_ref[:, :half])
    x1 = dot(match, stream_ref[:, half:])
    g0 = dot(match, grads_ref[:, :half])
    g1 = dot(match, grads_ref[:, half:])
    low = jnp.where(part == 0, x0, g0 * weight)
    high = jnp.where(part == 2, x1, g1 * weight)
    out_ref[...] = jnp.where(part < 2, low, high).astype(BF16).reshape(out_ref.shape)


def hop(i, n_sp):
    return lax.rem(i * 11, n_sp)


def ring_reduce(piece, place, to_right, to_left, from_left, from_right, sum_right, sum_left, sems):
    s_r, s_l, r_l, r_r = sems
    right, left, far = lax.rem(place + 1, 4), lax.rem(place + 3, 4), lax.rem(place + 2, 4)

    def right_copy(k, src):
        return pltpu.make_async_remote_copy(
            src, from_left.at[k], s_r.at[k], r_l.at[k], to_right, MESH
        )

    def left_copy(k, src):
        return pltpu.make_async_remote_copy(
            src, from_right.at[k], s_l.at[k], r_r.at[k], to_left, MESH
        )

    def start():
        right_copy(0, piece(far, 0)).start()
        left_copy(0, piece(far, 1)).start()
        right_copy(1, piece(right, 1)).start()
        left_copy(1, piece(left, 0)).start()

    def middle():
        right_copy(0, piece(far, 0)).wait()
        sum_right[...] = (piece(right, 0)[...].astype(F32) + from_left[0].astype(F32)).astype(BF16)
        left_copy(0, piece(far, 1)).wait()
        sum_left[...] = (piece(left, 1)[...].astype(F32) + from_right[0].astype(F32)).astype(BF16)
        right_copy(2, sum_right).start()
        left_copy(2, sum_left).start()

    def finish():
        right_copy(1, piece(right, 1)).wait()
        left_copy(1, piece(left, 0)).wait()
        right_copy(2, sum_right).wait()
        left_copy(2, sum_left).wait()

    def total(w, at=()):
        near, across = (from_left, from_right) if w == 0 else (from_right, from_left)
        return (
            piece(place, w)[at or Ellipsis].astype(F32)
            + near[(2,) + at].astype(F32)
            + across[(1,) + at].astype(F32)
        )

    return start, middle, finish, total


def greet(me, tp, n_sp, n_tp, ring=False):
    barrier = pltpu.get_barrier_semaphore()

    def hello(d, carry):
        pl.semaphore_signal(
            barrier, inc=1, device_id=(lax.rem(me + d, n_sp), tp), device_id_type=MESH
        )
        return carry

    lax.fori_loop(1, n_sp, hello, 0)
    count = n_sp - 1
    if ring:
        for other in (lax.rem(tp + 1, n_tp), lax.rem(tp + n_tp - 1, n_tp)):
            pl.semaphore_signal(barrier, inc=1, device_id=(me, other), device_id_type=MESH)
        count += 2
    return lambda: pl.semaphore_wait(barrier, count)


def split(x, pieces):
    terms = []
    for _ in range(pieces):
        term = x.astype(BF16)
        terms.append(term)
        x = x - term.astype(F32)
    return terms


def dot_split(x, exact, pieces, contract, left=True):
    total = None
    for term in split(x, pieces):
        part = dot(term, exact, contract) if left else dot(exact, term, contract)
        total = part if total is None else total + part
    return total


def triangle(n, keep):
    return keep(iota((n, n), 0), iota((n, n), 1)).astype(BF16)


def head_spread(heads, size):
    channel, head = iota((heads, heads * size), 1), iota((heads, heads * size), 0)
    return ((channel >= head * size) & (channel < (head + 1) * size)).astype(BF16)


def spread(x, owner):
    return dot_split(x, owner, 2, ((1,), (0,)))


def by_head(x, owner):
    return dot_split(x, owner, 2, ((1,), (1,)))


def cumulative_decay(time_step, rate, extra):
    log_decay = extra - time_step * rate
    upto = triangle(log_decay.shape[0], lambda t, s: s <= t)
    return dot_split(log_decay, upto, 3, ((1,), (0,)), left=False)


def turned(x):
    n = x.shape[1]
    return dot_split(x, triangle(n, lambda a, b: a == b), 3, ((1,), (1,)), left=False)


def decay_between(cum, cum_rows, h):
    gap = cum[:, h : h + 1] - cum_rows[h : h + 1, :]
    n = gap.shape[0]
    return jnp.exp(jnp.where(iota((n, n), 1) <= iota((n, n), 0), gap, -1e30))


def halves(pair):
    lane = iota(pair.shape, 1)
    zero = jnp.zeros_like(pair)
    size = pair.shape[1] // 2
    return jnp.concatenate([jnp.where(lane < size, pair, zero), jnp.where(lane < size, zero, pair)], axis=0)


def front_part(
    n_sp,
    n_tp,
    begin,
    prepare,
    between,
    in_ref,
    x_ref,
    dt_ref,
    rate_ref,
    extra_ref,
    first_hbm,
    b_ref,
    c_ref,
    gate_ref,
    scale_ref,
    out_ref,
    y_ref,
    normed_ref,
    coming,
    decays,
    state_mine,
    decay_mine,
    states,
    carries,
    diag,
    own,
    one,
    two,
    a_send,
    a_recv,
    s_right,
    s_left,
    r_left,
    r_right,
    f_send,
    f_recv,
    sends,
    recvs,
    d_sends,
    d_recvs,
    b_sends,
    b_recvs,
    first_ref,
    first_sem,
):
    me, tp = lax.axis_index("sp"), lax.axis_index("tp")
    entering = pltpu.make_async_copy(first_hbm.at[me], first_ref, first_sem)
    entering.start()
    begin()
    right, left = lax.rem(tp + 1, n_tp), lax.rem(tp + n_tp - 1, n_tp)
    far = lax.rem(tp + 2, n_tp)
    met = greet(me, tp, n_sp, n_tp, ring=True)
    prepare()
    met()

    low, plane = lax.rem(me, 8), lax.div(me, 8)
    away = (0, 1, 3, 2)

    def planes_off(j):
        return lax.rem(plane + 4 - away[j], 4)

    def exchange(j, k):
        to = lax.rem(plane + away[j], 4) * 8 + lax.rem(low + k, 8)
        return pltpu.make_async_remote_copy(
            in_ref.at[to],
            out_ref.at[tp, me],
            a_send.at[8 * j + k],
            a_recv.at[8 * j + k],
            (to, tp),
            MESH,
        )

    def arrived(j, k):
        source = planes_off(j) * 8 + lax.rem(low + 8 - k, 8)
        return pltpu.make_async_remote_copy(
            in_ref.at[me],
            out_ref.at[tp, source],
            a_send.at[8 * j + k],
            a_recv.at[8 * j + k],
            (me, tp),
            MESH,
        )

    def to_right(j, block):
        piece = out_ref.at[block, pl.ds(pl.multiple_of(planes_off(j) * 8, 8), 8)]
        return pltpu.make_async_remote_copy(
            piece, piece, s_right.at[j], r_left.at[j], (me, right), MESH
        )

    def to_left(j, block):
        piece = out_ref.at[block, pl.ds(pl.multiple_of(planes_off(j) * 8, 8), 8)]
        return pltpu.make_async_remote_copy(
            piece, piece, s_left.at[j], r_right.at[j], (me, left), MESH
        )

    def onward(j, block, rightward):
        first = planes_off(j) * 8 + (0 if rightward else 4)
        piece = out_ref.at[block, pl.ds(pl.multiple_of(first, 4), 4)]
        at = j if rightward else 4 + j
        return pltpu.make_async_remote_copy(
            piece, piece, f_send.at[at], f_recv.at[at], (me, right if rightward else left), MESH
        )

    for j in range(4):

        def start_exchange(k, carry, j=j):
            exchange(j, k).start()
            return carry

        lax.fori_loop(1 if j == 0 else 0, 8, start_exchange, 0)

    def pass_on(j):
        def await_chunk(k, carry):
            arrived(j, k).wait_recv()
            return carry

        lax.fori_loop(1 if j == 0 else 0, 8, await_chunk, 0)
        to_right(j, tp).start()
        to_left(j, tp).start()

    mine = pltpu.make_async_copy(in_ref.at[me], out_ref.at[tp, me], own)
    mine.start()

    mine.wait()
    pass_on(0)

    heads, tokens = dt_ref.shape
    channels = x_ref.shape[1]
    groups = b_ref.shape[1] // STATE
    wide = channels // groups
    owner = head_spread(heads, HDIM)
    dt = turned(dt_ref[...])
    cum = cumulative_decay(dt, rate_ref[...], turned(extra_ref[...]))
    cum_rows = turned(cum)
    last = cum[tokens - 1 : tokens, :]
    values = x_ref[...].astype(F32)
    ending = (values * spread(dt * jnp.exp(last - cum), owner)).astype(BF16)
    parts, rows, entries = state_mine.shape
    per_group = parts // groups
    for g in range(groups):
        state = dot(
            ending[:, g * wide : (g + 1) * wide],
            b_ref[:, g * STATE : (g + 1) * STATE],
            ((0,), (0,)),
        )
        state_mine[g * per_group : (g + 1) * per_group] = state.astype(BF16).reshape(
            per_group, rows, entries
        )
    total = jnp.exp(last)
    for p in range(parts):
        h = p * rows // HDIM
        decay_mine[p] = jnp.broadcast_to(total[:, h : h + 1], (1, entries))


    def state_copy(d):
        to = lax.rem(me + d, n_sp)
        return pltpu.make_async_remote_copy(
            state_mine.at[to], states.at[me], sends.at[d], recvs.at[d], (to, tp), MESH
        )

    def decay_copy(d):
        to = lax.rem(me + d, n_sp)
        return pltpu.make_async_remote_copy(
            decay_mine.at[to], decays.at[me], d_sends.at[d], d_recvs.at[d], (to, tp), MESH
        )

    def back_copy(d):
        to = lax.rem(me + d, n_sp)
        return pltpu.make_async_remote_copy(
            carries.at[to], coming.at[me], b_sends.at[d], b_recvs.at[d], (to, tp), MESH
        )

    def start_states(d, carry):
        decay_copy(hop(d, n_sp)).start()
        state_copy(hop(d, n_sp)).start()
        return carry

    lax.fori_loop(1, n_sp, start_states, 0)
    kept = pltpu.make_async_copy(state_mine.at[me], states.at[me], one)
    kept_too = pltpu.make_async_copy(decay_mine.at[me], decays.at[me], two)
    kept.start()
    kept_too.start()

    pass_on(1)

    scaled = (values * spread(dt, owner)).astype(BF16)
    affinity = [
        dot(
            c_ref[:, g * STATE : (g + 1) * STATE],
            b_ref[:, g * STATE : (g + 1) * STATE],
            ((1,), (1,)),
        )
        for g in range(groups)
    ]
    for q in range(heads // 2):
        g = q // (heads // 2 // groups)
        both = jnp.concatenate(
            [(affinity[g] * decay_between(cum, cum_rows, 2 * q + j)).astype(BF16) for j in range(2)],
            axis=1,
        )
        at = slice(q * 2 * HDIM, (q + 1) * 2 * HDIM)
        diag[:, at] = dot(both, halves(scaled[:, at]))
        if q == heads // 4 - 1:
            pass_on(2)
    pass_on(3)

    kept.wait()
    kept_too.wait()

    def finish_states(d, carry):
        decay_copy(d).wait()
        state_copy(d).wait()
        return carry

    lax.fori_loop(1, n_sp, finish_states, 0)
    entering.wait()
    running = first_ref[...]
    for i in range(n_sp):
        carries[i] = running.astype(BF16)
        running = decays[i] * running + states[i].astype(F32)

    def start_back(d, carry):
        back_copy(hop(d, n_sp)).start()
        return carry

    lax.fori_loop(1, n_sp, start_back, 0)
    kept_back = pltpu.make_async_copy(carries.at[me], coming.at[me], one)
    kept_back.start()

    for j in range(4):
        to_right(j, left).wait_recv()
        onward(j, left, True).start()
        to_left(j, right).wait_recv()
        onward(j, right, False).start()
    kept_back.wait()

    def finish_back(d, carry):
        back_copy(d).wait()
        return carry

    lax.fori_loop(1, n_sp, finish_back, 0)
    since = spread(jnp.exp(cum), owner)
    for g in range(groups):
        at = slice(g * wide, (g + 1) * wide)
        incoming = coming[g * per_group : (g + 1) * per_group].reshape(wide, entries)
        y = diag[:, at] + since[:, at] * dot(
            c_ref[:, g * STATE : (g + 1) * STATE], incoming, ((1,), (1,))
        )
        y_ref[:, at] = y
        gate = gate_ref[:, at].astype(F32)
        gated = y * gate * jax.nn.sigmoid(gate)
        factor = lax.rsqrt(jnp.mean(gated * gated, axis=1, keepdims=True) + norm_eps)
        normed_ref[:, at] = (gated * factor * scale_ref[:, at]).astype(BF16)

    between()
    for j in range(4):
        onward(j, far, True).wait()
        onward(j, far, False).wait()
        to_right(j, tp).wait_send()
        to_left(j, tp).wait_send()

        def drain(k, carry, j=j):
            exchange(j, k).wait_send()
            return carry

        lax.fori_loop(1 if j == 0 else 0, 8, drain, 0)


def expert_part(
    n_sp,
    n_tp,
    in_ref,
    gate_hbm,
    up_hbm,
    down_hbm,
    routes_ref,
    grads_ref,
    own_hbm,
    mix_ref,
    all_ref,
    dgate_hbm,
    dup_hbm,
    ddown_hbm,
    w_gate,
    w_up,
    w_down,
    d_gate,
    d_up,
    d_down,
    x,
    x_t,
    g,
    gate_grad,
    up_grad,
    hidden,
    part_ref,
    from_left,
    from_right,
    sum_right,
    sum_left,
    out_blocks,
    back,
    own_cols,
    loads,
    stores,
    s_r,
    s_l,
    r_l,
    r_r,
    a_send,
    a_recv,
    g_send,
    g_recv,
    local,
    w_own,
    w_sends,
    w_recvs,
    so_far,
):
    me, tp = lax.axis_index("sp"), lax.axis_index("tp")
    right, left = lax.rem(tp + 1, n_tp), lax.rem(tp + n_tp - 1, n_tp)
    far = lax.rem(tp + 2, n_tp)
    tokens, width = grads_ref.shape
    half, quarter = width // 2, width // 4
    model, units = w_gate.shape
    rows = x.shape[0]
    cuts = [(i, min(256, units - i)) for i in range(0, units, 256)]
    fetches = []
    for k, (start, size) in enumerate(cuts):
        at = pl.ds(start, size)
        fetches.append(
            [
                pltpu.make_async_copy(gate_hbm.at[0, :, at], w_gate.at[:, at], loads.at[3 * k]),
                pltpu.make_async_copy(up_hbm.at[0, :, at], w_up.at[:, at], loads.at[3 * k + 1]),
                pltpu.make_async_copy(down_hbm.at[0, at, :], w_down.at[at, :], loads.at[3 * k + 2]),
            ]
        )
        for fetch in fetches[-1]:
            fetch.start()
    yield

    core = lax.rem(me, 2)
    lane_y, lane_z = lax.rem(lax.div(me, 2), 4), lax.div(me, 8)

    def at_y(y):
        return lane_z * 8 + y * 2 + core

    def at_z(z):
        return z * 8 + lane_y * 2 + core

    def weight_copy(k, src, dst, to):
        return pltpu.make_async_remote_copy(
            src, dst, w_sends.at[k], w_recvs.at[k], (to, tp), MESH
        )

    own_weight = pltpu.make_async_copy(own_hbm, all_ref.at[lane_z, lane_y, core], w_own)
    own_weight.start()

    def first_stage(j, sending):
        y, z = (lane_y, lane_z) if sending else (lax.rem(lane_y + 4 - j, 4), lax.rem(lane_z + 4 - j, 4))
        return [
            weight_copy(
                j - 1, own_hbm.at[0], all_ref.at[lane_z, y, core, 0], at_y(lax.rem(lane_y + j, 4))
            ),
            weight_copy(
                j + 2, own_hbm.at[1], all_ref.at[z, lane_y, core, 1], at_z(lax.rem(lane_z + j, 4))
            ),
        ]

    def second_stage(j, sending):
        y, z = (lane_y, lane_z) if sending else (lax.rem(lane_y + 4 - j, 4), lax.rem(lane_z + 4 - j, 4))
        by_z, by_y = all_ref.at[z, :, core, 0], all_ref.at[:, y, core, 1]
        return [
            weight_copy(j + 5, by_z, by_z, at_z(lax.rem(lane_z + j, 4))),
            weight_copy(j + 8, by_y, by_y, at_y(lax.rem(lane_y + j, 4))),
        ]

    def third_stage(c):
        return weight_copy(12, all_ref.at[:, :, c], all_ref.at[:, :, c], me + 1 - 2 * core)

    for j in range(1, 4):
        for copy in first_stage(j, True):
            copy.start()

    tall = in_ref.shape[2]
    group_of = 8
    span = group_of * CAP
    spots = iota((1, group_of * tall), 1)
    src = divide(spots, tall)
    inner = spots - src * tall
    which = divide(inner, CAP)
    row = src * CAP + inner - which * CAP
    lines = iota((span, 1), 0)
    pick = [((row == lines) & (which == p)).astype(BF16) for p in range(4)]

    def columns_of(b):
        return pl.ds(pl.multiple_of(b * width, width), width)

    def select(b):
        for k in range(n_sp // group_of):
            block = in_ref[b, k * group_of : (k + 1) * group_of].reshape(group_of * tall, half)
            at = slice(k * span, (k + 1) * span)
            for c in range(2):
                cols = pl.ds(pl.multiple_of(b * width + c * half, half), half)
                x[at, cols] = dot(pick[2 * c], block).astype(BF16)
                g[at, cols] = dot(pick[2 * c + 1], block).astype(BF16)

    def products(b, at):
        cols = columns_of(b)
        return (
            dot(x[:, cols], w_gate[cols, at]),
            dot(x[:, cols], w_up[cols, at]),
            dot(g[:, cols], w_down[at, cols], ((1,), (1,))),
        )

    near = (tp, left, right)
    for b in near:
        select(b)
    for k, (start, size) in enumerate(cuts):
        for fetch in fetches[k]:
            fetch.wait()
        at = slice(start, start + size)
        sums = [products(b, at) for b in near]
        for i in range(3):
            so_far[i, :, at] = sums[0][i] + sums[1][i] + sums[2][i]
    yield
    select(far)
    for start, size in cuts:
        at = slice(start, start + size)
        last_gate, last_up, last_grad = products(far, at)
        pre_gate = so_far[0, :, at] + last_gate
        pre_up = so_far[1, :, at] + last_up
        hidden_grad = so_far[2, :, at] + last_grad
        sigmoid_gate = jax.nn.sigmoid(pre_gate)
        activated = pre_gate * sigmoid_gate
        hidden[:, at] = (activated * pre_up).astype(BF16)
        gate_grad[:, at] = (
            hidden_grad * pre_up * sigmoid_gate * (1.0 + pre_gate * (1.0 - sigmoid_gate))
        ).astype(BF16)
        up_grad[:, at] = (hidden_grad * activated).astype(BF16)

    own_weight.wait()
    for j in range(1, 4):
        for copy in first_stage(j, False):
            copy.wait_recv()
    for j in range(1, 4):
        for copy in second_stage(j, True):
            copy.start()

    def row_block(b):
        for c in range(2):
            cols = pl.ds(pl.multiple_of(b * width + c * half, half), half)
            part_ref[2 * b + c] = (
                dot(gate_grad[...], w_gate[cols, :], ((1,), (1,)))
                + dot(up_grad[...], w_up[cols, :], ((1,), (1,)))
            ).astype(BF16)

    def block(b, which):
        return part_ref.at[2 * b + which]

    def right_copy(k, src):
        return pltpu.make_async_remote_copy(
            src, from_left.at[k], s_r.at[k], r_l.at[k], (me, right), MESH
        )

    def left_copy(k, src):
        return pltpu.make_async_remote_copy(
            src, from_right.at[k], s_l.at[k], r_r.at[k], (me, left), MESH
        )

    row_block(far)
    row_block(right)
    right_copy(0, block(far, 0)).start()
    left_copy(0, block(far, 1)).start()
    row_block(left)
    right_copy(1, block(right, 1)).start()
    row_block(tp)
    left_copy(1, block(left, 0)).start()

    saves = []

    def save(k, src, dst):
        copy = pltpu.make_async_copy(src, dst, stores.at[k])
        copy.start()
        saves.append(copy)

    def passed_right():
        right_copy(0, block(far, 0)).wait()
        sum_right[...] = (block(right, 0)[...].astype(F32) + from_left[0].astype(F32)).astype(BF16)
        left_copy(0, block(far, 1)).wait()
        sum_left[...] = (block(left, 1)[...].astype(F32) + from_right[0].astype(F32)).astype(BF16)

    def gate_up_rows(i):
        at = slice(i * 256, (i + 1) * 256)
        x_t[at, :] = jnp.transpose(x[:, at])
        d_gate[at, :] = dot(x_t[at, :], gate_grad[...]).astype(BF16)
        save(2 * i, d_gate.at[at, :], dgate_hbm.at[0, at, :])
        d_up[at, :] = dot(x_t[at, :], up_grad[...]).astype(BF16)
        save(2 * i + 1, d_up.at[at, :], dup_hbm.at[0, at, :])

    for i in range(4):
        gate_up_rows(i)
    passed_right()
    right_copy(2, sum_right).start()
    left_copy(2, sum_left).start()
    for i in range(4, 8):
        gate_up_rows(i)

    for k, (start, size) in enumerate(cuts):
        at = slice(start, start + size)
        d_down[at, :] = dot(hidden[:, at], g[...], ((0,), (0,))).astype(BF16)
        save(16 + k, d_down.at[at, :], ddown_hbm.at[0, at, :])

    for j in range(1, 4):
        for copy in second_stage(j, False):
            copy.wait_recv()
    third_stage(core).start()

    by_token = slots_in_rows(routes_ref[...], n_sp)
    line = iota((8, tokens), 0)
    slots = turned(
        jnp.where(line == 0, by_token[0], jnp.where(line == 1, by_token[1], 0)).astype(F32)
    ).astype(jnp.int32)
    column = iota((1, n_sp * 4 * CAP), 1)
    expert = divide(column, 4 * CAP)
    place_in = column - expert * (4 * CAP)
    piece = divide(place_in, CAP)
    slot = expert * CAP + place_in - piece * CAP
    match = (slots[:, 0:1] == slot) | (slots[:, 1:2] == slot)

    right_copy(1, block(right, 1)).wait()
    left_copy(1, block(left, 0)).wait()
    right_copy(2, sum_right).wait()
    left_copy(2, sum_left).wait()

    tall_out = iota((group_of * 4 * CAP, 1), 0)
    out_src = divide(tall_out, 4 * CAP)
    out_in = tall_out - out_src * (4 * CAP)
    out_piece = divide(out_in, CAP)
    out_row = out_src * CAP + out_in - out_piece * CAP
    pair_at = iota((1, span), 1)
    place = [((out_row == pair_at) & (out_piece == c)).astype(BF16) for c in range(4)]
    for k in range(rows // span):
        at = slice(k * span, (k + 1) * span)
        low = (
            part_ref[2 * tp, at, :].astype(F32)
            + from_left[2, at, :].astype(F32)
            + from_right[1, at, :].astype(F32)
        ).astype(BF16)
        high = (
            part_ref[2 * tp + 1, at, :].astype(F32)
            + from_right[2, at, :].astype(F32)
            + from_left[1, at, :].astype(F32)
        ).astype(BF16)
        laid = (
            dot(place[0], low[:, :quarter])
            + dot(place[1], low[:, quarter:])
            + dot(place[2], high[:, :quarter])
            + dot(place[3], high[:, quarter:])
        )
        out_blocks[k * group_of : (k + 1) * group_of] = laid.astype(BF16).reshape(
            group_of, 4 * CAP, quarter
        )

    def exchange(d):
        to = lax.rem(me + d, n_sp)
        return pltpu.make_async_remote_copy(
            out_blocks.at[to], back.at[me], a_send.at[d], a_recv.at[d], (to, tp), MESH
        )

    def start_exchange(d, carry):
        exchange(hop(d, n_sp)).start()
        return carry

    lax.fori_loop(1, n_sp, start_exchange, 0)
    mine = pltpu.make_async_copy(out_blocks.at[me], back.at[me], local)
    mine.start()
    mine.wait()

    def finish_exchange(d, carry):
        exchange(d).wait()
        return carry

    lax.fori_loop(1, n_sp, finish_exchange, 0)
    returned = back[...].reshape(n_sp * 4 * CAP, quarter)
    for c in range(4):
        chosen = jnp.where(match & (piece == c), 1.0, 0.0).astype(BF16)
        cols = slice(c * quarter, (c + 1) * quarter)
        own_cols[:, cols] = (grads_ref[:, cols].astype(F32) + dot(chosen, returned)).astype(BF16)

    def spot(b):
        return mix_ref.at[:, pl.ds(pl.multiple_of(b * width, width), width)]

    def spot_half(b, which):
        return mix_ref.at[:, pl.ds(pl.multiple_of(b * width + which * half, half), half)]

    def gather(k, src, dst, to):
        return pltpu.make_async_remote_copy(
            src, dst, g_send.at[k], g_recv.at[k], (me, to), MESH
        )

    gather(0, own_cols, spot(tp), right).start()
    gather(1, own_cols, spot(tp), left).start()
    spot(tp)[...] = own_cols[...]
    gather(0, own_cols, spot(left), right).wait_recv()
    gather(2, spot_half(left, 0), spot_half(left, 0), right).start()
    gather(1, own_cols, spot(right), left).wait_recv()
    gather(3, spot_half(right, 1), spot_half(right, 1), left).start()
    gather(2, spot_half(far, 0), spot_half(far, 0), right).wait()
    gather(3, spot_half(far, 1), spot_half(far, 1), left).wait()
    gather(0, own_cols, spot(tp), right).wait_send()
    gather(1, own_cols, spot(tp), left).wait_send()
    for copy in saves:
        copy.wait()
    for j in range(1, 4):
        for copy in first_stage(j, True) + second_stage(j, True):
            copy.wait_send()
    third_stage(core).wait_send()
    third_stage(1 - core).wait_recv()


def tail_part(
    n_sp,
    n_tp,
    mix_ref,
    weight,
    y_ref,
    normed_ref,
    x_ref,
    dt_ref,
    rate_ref,
    extra_ref,
    coming_ref,
    decays,
    b_ref,
    c_ref,
    gate_ref,
    scale_ref,
    proj_ref,
    dx_ref,
    ddt_ref,
    db_ref,
    dc_ref,
    dgate_ref,
    normed2,
    mix2,
    parts,
    big_in,
    big_sum,
    small_in,
    small_sum,
    reduced,
    total,
    state_mine,
    states,
    carries,
    later,
    d_scaled,
    one,
    p_send,
    p_recv,
    ring_sems,
    sends,
    recvs,
    b_sends,
    b_recvs,
):
    me, tp = lax.axis_index("sp"), lax.axis_index("tp")
    core = lax.rem(me, 2)
    partner = me + 1 - 2 * core
    chip = lax.div(me, 2)
    chips = n_sp // 2
    heads, tokens = dt_ref.shape
    channels = x_ref.shape[1]
    groups = b_ref.shape[1] // STATE
    wide = channels // groups
    half = channels // 2
    cols = proj_ref.shape[0]
    n_parts, rows, entries = state_mine.shape
    per_group = n_parts // groups

    def pair(k, src, dst):
        return pltpu.make_async_remote_copy(
            src, dst, p_send.at[k], p_recv.at[k], (partner, tp), MESH
        )

    def mine(c):
        return pl.ds(pl.multiple_of(c * half, half), half)

    owner = head_spread(heads, HDIM)
    dt = turned(dt_ref[...])
    cum = cumulative_decay(dt, rate_ref[...], turned(extra_ref[...]))
    cum_rows = turned(cum)
    last = cum[tokens - 1 : tokens, :]
    since = spread(jnp.exp(cum), owner)

    whole_weight = weight[...].reshape(mix_ref.shape[1], channels)
    normed_grads = [
        dot(mix_ref[...], whole_weight[:, g * wide : (g + 1) * wide]) for g in range(groups)
    ]
    mix_t = jnp.transpose(mix_ref[...])
    pair(0, normed_ref.at[:, mine(1 - core)], normed2).start()
    pair(1, mix_ref, mix2).start()
    d_y = []
    for g in range(groups):
        at = slice(g * wide, (g + 1) * wide)
        normed_grad = normed_grads[g]
        y = y_ref[:, at]
        gate = gate_ref[:, at].astype(F32)
        sigmoid_gate = jax.nn.sigmoid(gate)
        activated = gate * sigmoid_gate
        gated = y * activated
        factor = lax.rsqrt(jnp.mean(gated * gated, axis=1, keepdims=True) + norm_eps)
        scaled_grad = normed_grad * scale_ref[:, at]
        along = jnp.mean(scaled_grad * gated, axis=1, keepdims=True) * factor * factor
        gated_grad = factor * (scaled_grad - gated * along)
        d_y.append(gated_grad * activated)
        dgate_ref[:, at] = (
            gated_grad * y * (sigmoid_gate * (1.0 + gate * (1.0 - sigmoid_gate)))
        ).astype(BF16)
    d_out = jnp.concatenate(d_y, axis=1)
    since_grad = since * d_out
    since_low = since_grad.astype(BF16)
    for g in range(groups):
        state = dot(
            since_low[:, g * wide : (g + 1) * wide],
            c_ref[:, g * STATE : (g + 1) * STATE],
            ((0,), (0,)),
        )
        state_mine[g * per_group : (g + 1) * per_group] = state.astype(BF16).reshape(
            per_group, rows, entries
        )
    whole = jnp.exp(last)

    def state_copy(d):
        to = lax.rem(me + d, n_sp)
        return pltpu.make_async_remote_copy(
            state_mine.at[to], states.at[me], sends.at[d], recvs.at[d], (to, tp), MESH
        )

    def back_copy(d):
        to = lax.rem(me + d, n_sp)
        return pltpu.make_async_remote_copy(
            carries.at[to], later.at[me], b_sends.at[d], b_recvs.at[d], (to, tp), MESH
        )

    def start_states(d, carry):
        state_copy(hop(d, n_sp)).start()
        return carry

    lax.fori_loop(1, n_sp, start_states, 0)
    kept = pltpu.make_async_copy(state_mine.at[me], states.at[me], one)
    kept.start()

    pair(0, normed_ref.at[:, mine(1 - core)], normed2).wait()
    pair(1, mix_ref, mix2).wait()
    both_mix = jnp.concatenate([mix_t, jnp.transpose(mix2[...])], axis=1)
    both_normed = jnp.concatenate([normed_ref[:, mine(core)], normed2[...]], axis=0)
    piece_rows = cols // 2
    for z in range(4):
        at = slice(z * 8 * cols, (z + 1) * 8 * cols)
        parts[z] = (
            dot(both_mix[at, :], both_normed).astype(BF16).reshape(4, 2, 2, piece_rows, half)
        )

    lane_y, lane_z = lax.rem(chip, 4), lax.div(chip, 4)

    def at_y(y):
        return (lane_z * 8 + lax.rem(y, 4) * 2 + core, tp)

    def at_z(z):
        return (lax.rem(z, 4) * 8 + lane_y * 2 + core, tp)

    y_ring = (lane_y, at_y(lane_y + 1), at_y(lane_y + 3))
    z_ring = (lane_z, at_z(lane_z + 1), at_z(lane_z + 3))

    def four(ref, k):
        return [ref.at[k, i] for i in range(4)]

    def bufs(landing, sums, k):
        return [landing.at[k, 0], landing.at[k, 1], sums.at[k, 0], sums.at[k, 1]]

    stages = [
        ring_reduce(lambda b, w: parts.at[:, b, 0, w], *y_ring, *bufs(big_in, big_sum, 0), four(ring_sems, 0)),
        ring_reduce(lambda b, w: parts.at[b, :, 1, w], *z_ring, *bufs(big_in, big_sum, 1), four(ring_sems, 1)),
        ring_reduce(lambda b, w: reduced.at[0, w, b], *z_ring, *bufs(small_in, small_sum, 0), four(ring_sems, 2)),
        ring_reduce(lambda b, w: reduced.at[1, w, b], *y_ring, *bufs(small_in, small_sum, 1), four(ring_sems, 3)),
    ]
    stages[0][0]()
    stages[1][0]()


    values = x_ref[...].astype(F32)
    steps = spread(dt, owner)
    scaled = values * steps
    scaled_low = scaled.astype(BF16)
    d_low = d_out.astype(BF16)
    not_before = triangle(tokens, lambda t, s: s >= t)
    below = (iota((tokens, tokens), 1) < iota((tokens, tokens), 0)).astype(F32)
    head_lane = iota((1, heads), 1)
    crossing = [jnp.zeros((tokens, heads), F32)]
    d_affinity = []

    def inside(g):
        affinity = dot(
            c_ref[:, g * STATE : (g + 1) * STATE],
            b_ref[:, g * STATE : (g + 1) * STATE],
            ((1,), (1,)),
        )
        sum_affinity = jnp.zeros((tokens, tokens), F32)
        first = g * (heads // 2 // groups)
        for q in range(first, first + heads // 2 // groups):
            at = slice(q * 2 * HDIM, (q + 1) * 2 * HDIM)
            d_halves = halves(d_low[:, at])
            d_weights = dot(d_halves, scaled_low[:, at], ((1,), (1,)))
            weights, moved = [], []
            for j in range(2):
                between = decay_between(cum, cum_rows, 2 * q + j)
                weights.append((affinity * between).astype(BF16))
                d_between = d_weights[j * tokens : (j + 1) * tokens] * between
                sum_affinity = sum_affinity + d_between
                moved.append((d_between * affinity).astype(BF16))
            d_scaled[:, at] = dot(jnp.concatenate(weights, axis=0), d_halves, ((0,), (0,)))
            reach = dot(not_before, jnp.concatenate(moved, axis=1))
            for j in range(2):
                over = jnp.sum(
                    reach[:, j * tokens : (j + 1) * tokens] * below, axis=1, keepdims=True
                )
                crossing[0] = crossing[0] + jnp.where(head_lane == 2 * q + j, over, 0.0)
        d_affinity.append(sum_affinity.astype(BF16))

    inside(0)
    kept.wait()

    def finish_states(d, carry):
        state_copy(d).wait()
        return carry

    lax.fori_loop(1, n_sp, finish_states, 0)
    running = jnp.zeros((rows, entries), F32)
    for step in range(n_sp):
        i = n_sp - 1 - step
        carries[i] = running.astype(BF16)
        running = decays[i] * running + states[i].astype(F32)

    def start_back(d, carry):
        back_copy(hop(d, n_sp)).start()
        return carry

    lax.fori_loop(1, n_sp, start_back, 0)
    kept_back = pltpu.make_async_copy(carries.at[me], later.at[me], one)
    kept_back.start()

    for g in range(1, groups):
        inside(g)
    stages[0][1]()
    stages[1][1]()
    read_out = []
    for g in range(groups):
        at = slice(g * wide, (g + 1) * wide)
        by = slice(g * STATE, (g + 1) * STATE)
        incoming = coming_ref[g * per_group : (g + 1) * per_group].reshape(wide, entries)
        read_out.append(dot(c_ref[:, by], incoming, ((1,), (1,))))
        dc_ref[:, by] = (
            dot(d_affinity[g], b_ref[:, by]) + dot(since_low[:, at], incoming)
        ).astype(BF16)
    for k in range(2):
        stages[k][2]()
        for w in range(2):
            reduced[k, w] = stages[k][3](w).astype(BF16)
    stages[2][0]()
    stages[3][0]()
    reading = by_head(since_grad * jnp.concatenate(read_out, axis=1), owner)

    kept_back.wait()

    def finish_back(d, carry):
        back_copy(d).wait()
        return carry

    lax.fori_loop(1, n_sp, finish_back, 0)
    until = spread(jnp.exp(last - cum), owner)
    ending = scaled * until
    ending_low = ending.astype(BF16)
    from_later = []
    for g in range(groups):
        at = slice(g * wide, (g + 1) * wide)
        by = slice(g * STATE, (g + 1) * STATE)
        after = later[g * per_group : (g + 1) * per_group].reshape(wide, entries)
        from_later.append(dot(b_ref[:, by], after, ((1,), (1,))))
        db_ref[:, by] = (
            dot(d_affinity[g], c_ref[:, by], ((0,), (0,))) + dot(ending_low[:, at], after)
        ).astype(BF16)
    stages[2][1]()
    stages[3][1]()
    closing = jnp.concatenate(from_later, axis=1)
    gradient = d_scaled[...] + until * closing
    dx_ref[...] = (gradient * steps).astype(BF16)
    direct = by_head(gradient * values, owner)
    stored = by_head(ending * closing, owner)
    kept_state = jnp.sum(
        (
            coming_ref[...].astype(F32).reshape(heads, HDIM, entries)
            * later[...].astype(F32).reshape(heads, HDIM, entries)
        ),
        axis=1,
    )
    passing = dot_split(
        kept_state, jnp.ones((8, entries), BF16), 3, ((1,), (1,)), left=False
    )[0:1, :]
    earlier = triangle(tokens, lambda t, s: s < t)
    d_decay = (
        crossing[0]
        + dot_split(reading, not_before, 3, ((1,), (0,)), left=False)
        + dot_split(stored, earlier, 3, ((1,), (0,)), left=False)
        + passing * whole
    )
    ddt_ref[...] = turned(direct - d_decay * rate_ref[...])

    for k in range(2):
        stages[2 + k][2]()
        for w in range(2):
            first = (2 * k + w) * piece_rows
            total[first : first + piece_rows, :] = stages[2 + k][3](w)

    def lines(c):
        return pl.ds(pl.multiple_of(c * cols, cols), cols)

    given = pair(2, total.at[lines(1 - core), :], proj_ref.at[:, mine(core)])
    given.start()
    proj_ref[:, mine(core)] = total[lines(core), :]
    given.wait_send()
    pair(2, total.at[lines(core), :], proj_ref.at[:, mine(1 - core)]).wait_recv()


FRONT_SCRATCH = 24
EXPERT_SCRATCH = 35


def main_kernel(n_sp, n_tp, *refs):
    (stream, weights, x, dt, rate, extra, first, b, c, gate, scale) = refs[:11]
    (w_gate, w_up, w_down, routes, grads, own) = refs[11:17]
    tail_outs = refs[17:23]
    weight_grads = refs[23:26]
    (packed, arrived, y, normed, coming, decays, mix, all_weight) = refs[26:34]
    front_scratch = refs[34 : 34 + FRONT_SCRATCH]
    expert_scratch = refs[34 + FRONT_SCRATCH : 34 + FRONT_SCRATCH + EXPERT_SCRATCH]
    tail_scratch = refs[34 + FRONT_SCRATCH + EXPERT_SCRATCH :]
    steps = expert_part(
        n_sp,
        n_tp,
        arrived,
        w_gate,
        w_up,
        w_down,
        routes,
        grads,
        own,
        mix,
        all_weight,
        *weight_grads,
        *expert_scratch,
    )
    front_part(
        n_sp,
        n_tp,
        lambda: next(steps),
        lambda: pack(n_sp, routes, weights, stream, grads, packed),
        lambda: next(steps),
        packed,
        x,
        dt,
        rate,
        extra,
        first,
        b,
        c,
        gate,
        scale,
        arrived,
        y,
        normed,
        coming,
        decays,
        *front_scratch,
    )
    for _ in steps:
        pass
    tail_part(
        n_sp,
        n_tp,
        mix,
        all_weight,
        y,
        normed,
        x,
        dt,
        rate,
        extra,
        coming,
        decays,
        b,
        c,
        gate,
        scale,
        *tail_outs,
        *tail_scratch,
    )


def main(
    stream, weights, x, dt, rate, extra, first, b, c, gate, scale, w_gate, w_up, w_down, routes, grads, own, n_sp, n_tp
):
    dma = pltpu.SemaphoreType.DMA
    tokens, channels = x.shape
    _, rows, entries = first.shape
    _, model, units = w_gate.shape
    pairs = n_sp * CAP
    width = grads.shape[1]
    half, quarter = width // 2, width // 4
    front_scratch = (
        [
            pltpu.VMEM((n_sp, rows, entries), BF16),
            pltpu.VMEM((n_sp, 1, entries), F32),
            pltpu.VMEM((n_sp, rows, entries), BF16),
            pltpu.VMEM((n_sp, rows, entries), BF16),
            pltpu.VMEM((tokens, channels), F32),
            dma,
            dma,
            dma,
        ]
        + [dma((n_sp,))] * 2
        + [dma((4,))] * 4
        + [dma((8,))] * 2
        + [dma((n_sp,))] * 6
        + [pltpu.VMEM((rows, entries), F32), dma]
    )
    expert_scratch = [
        pltpu.VMEM((model, units), BF16),
        pltpu.VMEM((model, units), BF16),
        pltpu.VMEM((units, model), BF16),
        pltpu.VMEM((model, units), BF16),
        pltpu.VMEM((model, units), BF16),
        pltpu.VMEM((units, model), BF16),
        pltpu.VMEM((pairs, model), BF16),
        pltpu.VMEM((model, pairs), BF16),
        pltpu.VMEM((pairs, model), BF16),
        pltpu.VMEM((pairs, units), BF16),
        pltpu.VMEM((pairs, units), BF16),
        pltpu.VMEM((pairs, units), BF16),
        pltpu.VMEM((2 * n_tp, pairs, half), BF16),
        pltpu.VMEM((3, pairs, half), BF16),
        pltpu.VMEM((3, pairs, half), BF16),
        pltpu.VMEM((pairs, half), BF16),
        pltpu.VMEM((pairs, half), BF16),
        pltpu.VMEM((n_sp, 4 * CAP, quarter), BF16),
        pltpu.VMEM((n_sp, 4 * CAP, quarter), BF16),
        pltpu.VMEM((tokens, width), BF16),
        dma((12,)),
        dma((20,)),
        dma((3,)),
        dma((3,)),
        dma((3,)),
        dma((3,)),
        dma((n_sp,)),
        dma((n_sp,)),
        dma((4,)),
        dma((4,)),
        dma,
        dma,
        dma((13,)),
        dma((13,)),
        pltpu.VMEM((3, pairs, units), F32),
    ]
    cols = own.shape[0] * own.shape[1]
    tail_scratch = (
        [
            pltpu.VMEM((tokens, channels // 2), BF16),
            pltpu.VMEM((tokens, width * n_tp), BF16),
            pltpu.VMEM((4, 4, 2, 2, cols // 2, channels // 2), BF16),
            pltpu.VMEM((2, 2, 3, 4, cols // 2, channels // 2), BF16),
            pltpu.VMEM((2, 2, 4, cols // 2, channels // 2), BF16),
            pltpu.VMEM((2, 2, 3, cols // 2, channels // 2), BF16),
            pltpu.VMEM((2, 2, cols // 2, channels // 2), BF16),
            pltpu.VMEM((2, 2, 4, cols // 2, channels // 2), BF16),
            pltpu.VMEM((2 * cols, channels // 2), F32),
            pltpu.VMEM((n_sp, rows, entries), BF16),
            pltpu.VMEM((n_sp, rows, entries), BF16),
            pltpu.VMEM((n_sp, rows, entries), BF16),
            pltpu.VMEM((n_sp, rows, entries), BF16),
            pltpu.VMEM((tokens, channels), F32),
            dma,
            dma((3,)),
            dma((3,)),
            dma((4, 4, 3)),
        ]
        + [dma((n_sp,))] * 4
    )
    return pl.pallas_call(
        functools.partial(main_kernel, n_sp, n_tp),
        out_shape=(
            jax.ShapeDtypeStruct((own.shape[0] * own.shape[1], channels), F32),
            jax.ShapeDtypeStruct((tokens, channels), BF16),
            jax.ShapeDtypeStruct(dt.shape, F32),
            jax.ShapeDtypeStruct(b.shape, BF16),
            jax.ShapeDtypeStruct(c.shape, BF16),
            jax.ShapeDtypeStruct((tokens, channels), BF16),
            jax.ShapeDtypeStruct(w_gate.shape, BF16),
            jax.ShapeDtypeStruct(w_up.shape, BF16),
            jax.ShapeDtypeStruct(w_down.shape, BF16),
        ),
        in_specs=[vmem_spec()] * 6
        + [any_spec()]
        + [vmem_spec()] * 4
        + [any_spec()] * 3
        + [vmem_spec()] * 2
        + [any_spec()],
        out_specs=(vmem_spec(),) * 6 + (any_spec(),) * 3,
        scratch_shapes=[
            pltpu.VMEM((n_sp, 4 * CAP, half), BF16),
            pltpu.VMEM((n_tp, n_sp, 4 * CAP, half), BF16),
            pltpu.VMEM((tokens, channels), F32),
            pltpu.VMEM((tokens, channels), BF16),
            pltpu.VMEM((n_sp, rows, entries), BF16),
            pltpu.VMEM((n_sp, 1, entries), F32),
            pltpu.VMEM((tokens, width * n_tp), BF16),
            pltpu.VMEM((4, 4, 2) + own.shape, BF16),
        ]
        + front_scratch
        + expert_scratch
        + tail_scratch,
        compiler_params=pltpu.CompilerParams(
            collective_id=0, has_side_effects=True, vmem_limit_bytes=VMEM_BYTES
        ),
        name="main",
    )(
        stream, weights, x, dt, rate, extra, first, b, c, gate, scale, w_gate, w_up, w_down, routes, grads, own
    )


def finish_kernel(count, *refs):
    sources, results, held = refs[:count], refs[count : 2 * count], refs[2 * count : 3 * count]
    loads, stores = refs[3 * count :]
    copies = []
    for i in range(count):
        lines = sources[i].shape[-2]
        pieces = 4 if lines > 512 else 1
        for p in range(pieces):
            at = pl.ds(p * (lines // pieces), lines // pieces)
            views = [
                ref.at[0, at, :] if len(ref.shape) == 3 else ref.at[at, :]
                for ref in (sources[i], held[i], results[i])
            ]
            k = len(copies)
            copies.append(
                (
                    pltpu.make_async_copy(views[0], views[1], loads.at[k]),
                    pltpu.make_async_copy(views[1], views[2], stores.at[k]),
                )
            )
    for load, _ in copies:
        load.start()
    for load, store in copies:
        load.wait()
        store.start()
    for _, store in copies:
        store.wait()


def finish(*arrays):
    count = len(arrays)
    dma = pltpu.SemaphoreType.DMA
    return pl.pallas_call(
        functools.partial(finish_kernel, count),
        out_shape=tuple(jax.ShapeDtypeStruct(a.shape, a.dtype) for a in arrays),
        in_specs=[any_spec()] * count,
        out_specs=(any_spec(),) * count,
        scratch_shapes=[pltpu.VMEM(a.shape, a.dtype) for a in arrays]
        + [dma((4 * count,)), dma((4 * count,))],
        compiler_params=pltpu.CompilerParams(vmem_limit_bytes=VMEM_BYTES),
        name="finish",
    )(*arrays)


def body(
    n_sp,
    n_tp,
    mixer_output_stream,
    layer_output_gradient,
    routes,
    expert_combine_weight,
    expert_gate_weight,
    expert_up_weight,
    expert_down_weight,
    head_mixer_input,
    head_step_size,
    head_decay_rate,
    extra_log_decay,
    state_entering_span,
    state_input_vectors,
    state_readout_vectors,
    gate_preactivation,
    group_norm_scale,
    mixer_output_weight,
):
    heads = head_step_size.shape[1]
    part_rows = heads * HDIM // n_sp
    entering = state_entering_span.reshape(n_sp, part_rows, STATE)
    rate = head_decay_rate[None, :]
    scale = group_norm_scale[None, :]
    proj_grad, input_grad, step_grad, b_grad, c_grad, gate_grad_in, grad_g, grad_u, grad_d = main(
        mixer_output_stream,
        expert_combine_weight.T,
        head_mixer_input,
        head_step_size.T,
        rate,
        extra_log_decay.T,
        entering,
        state_input_vectors,
        state_readout_vectors,
        gate_preactivation,
        scale,
        expert_gate_weight,
        expert_up_weight,
        expert_down_weight,
        routes.T,
        layer_output_gradient,
        mixer_output_weight.T.reshape(2, -1, mixer_output_weight.shape[0]),
        n_sp,
        n_tp,
    )
    proj_grad, input_grad, step_grad, b_grad, c_grad, gate_grad_in, grad_g, grad_u, grad_d = finish(
        proj_grad,
        input_grad,
        step_grad,
        b_grad,
        c_grad,
        gate_grad_in,
        grad_g,
        grad_u,
        grad_d,
    )
    return (
        grad_g,
        grad_u,
        grad_d,
        proj_grad.T,
        input_grad,
        step_grad.T,
        b_grad,
        c_grad,
        gate_grad_in,
    )


def solution(mesh):
    placed = (
        P(SP, "tp"),
        P(SP, "tp"),
        P(SP, None),
        P(SP, None),
        P(SP, None, "tp"),
        P(SP, None, "tp"),
        P(SP, "tp", None),
        P(SP, "tp"),
        P(SP, "tp"),
        P("tp"),
        P(SP, "tp"),
        P("tp", None, None),
        P(SP, "tp"),
        P(SP, "tp"),
        P(SP, "tp"),
        P("tp"),
        P("tp", SP),
    )
    return jax.shard_map(
        functools.partial(body, mesh.shape["sp"], mesh.shape["tp"]),
        mesh=mesh,
        in_specs=placed,
        out_specs=(
            P(SP, None, "tp"),
            P(SP, None, "tp"),
            P(SP, "tp", None),
            P("tp", SP),
            P(SP, "tp"),
            P(SP, "tp"),
            P(SP, "tp"),
            P(SP, "tp"),
            P(SP, "tp"),
        ),
        check_vma=False,
    )
```

```python
import functools

import jax
import jax.numpy as jnp
from jax import lax
from jax.experimental import pallas as pl
from jax.experimental.pallas import tpu as pltpu
from jax.sharding import PartitionSpec as P

HDIM = 64
STATE = 128
SP = "sp"
CAP = 12
MESH = pl.DeviceIdType.MESH
F32 = jnp.float32
BF16 = jnp.bfloat16

norm_eps = 1e-05
VMEM_BYTES = 67043328 - 1024 * 1024


def vmem_spec():
    return pl.BlockSpec(memory_space=pltpu.VMEM)


def any_spec():
    return pl.BlockSpec(memory_space=pl.ANY)


def dot(a, b, contract=((1,), (0,))):
    return lax.dot_general(a, b, (contract, ((), ())), preferred_element_type=F32)


def iota(shape, dim):
    return lax.broadcasted_iota(jnp.int32, shape, dim)


def divide(x, by):
    return ((x.astype(F32) + 0.5) * (1.0 / by)).astype(jnp.int32)


def slots_in_rows(routes, experts):
    top, tokens = routes.shape
    ids = iota((experts, tokens), 0)
    earlier = (iota((tokens, tokens), 0) < iota((tokens, tokens), 1)).astype(BF16)
    before = jnp.zeros((experts, 1), F32)
    rows = []
    for k in range(top):
        hits = (ids == routes[k : k + 1, :]).astype(F32)
        rank = dot(hits.astype(BF16), earlier) + before
        rows.append(jnp.sum(hits * rank, axis=0, keepdims=True))
        before = before + jnp.sum(hits, axis=1, keepdims=True)
    return [routes[k : k + 1, :] * CAP + rows[k].astype(jnp.int32) for k in range(top)]


def pack(experts, routes_ref, weights_ref, stream_ref, grads_ref, out_ref):
    tokens = stream_ref.shape[0]
    half = stream_ref.shape[1] // 2
    slots = slots_in_rows(routes_ref[...], experts)
    row = iota((experts * 4 * CAP, 1), 0)
    expert = divide(row, 4 * CAP)
    inner = row - expert * (4 * CAP)
    part = divide(inner, CAP)
    slot = expert * CAP + inner - part * CAP
    first = (slot == slots[0]).astype(F32)
    second = (slot == slots[1]).astype(F32)
    match = (first + second).astype(BF16)
    weight = jnp.sum(
        first * weights_ref[0:1, :] + second * weights_ref[1:2, :], axis=1, keepdims=True
    )
    x0 = dot(match, stream_ref[:, :half])
    x1 = dot(match, stream_ref[:, half:])
    g0 = dot(match, grads_ref[:, :half])
    g1 = dot(match, grads_ref[:, half:])
    low = jnp.where(part == 0, x0, g0 * weight)
    high = jnp.where(part == 2, x1, g1 * weight)
    out_ref[...] = jnp.where(part < 2, low, high).astype(BF16).reshape(out_ref.shape)


def hop(i, n_sp):
    return lax.rem(i * 11, n_sp)


def ring_reduce(piece, place, to_right, to_left, from_left, from_right, sum_right, sum_left, sems):
    s_r, s_l, r_l, r_r = sems
    right, left, far = lax.rem(place + 1, 4), lax.rem(place + 3, 4), lax.rem(place + 2, 4)

    def right_copy(k, src):
        return pltpu.make_async_remote_copy(
            src, from_left.at[k], s_r.at[k], r_l.at[k], to_right, MESH
        )

    def left_copy(k, src):
        return pltpu.make_async_remote_copy(
            src, from_right.at[k], s_l.at[k], r_r.at[k], to_left, MESH
        )

    def start():
        right_copy(0, piece(far, 0)).start()
        left_copy(0, piece(far, 1)).start()
        right_copy(1, piece(right, 1)).start()
        left_copy(1, piece(left, 0)).start()

    def middle():
        right_copy(0, piece(far, 0)).wait()
        sum_right[...] = (piece(right, 0)[...].astype(F32) + from_left[0].astype(F32)).astype(BF16)
        left_copy(0, piece(far, 1)).wait()
        sum_left[...] = (piece(left, 1)[...].astype(F32) + from_right[0].astype(F32)).astype(BF16)
        right_copy(2, sum_right).start()
        left_copy(2, sum_left).start()

    def finish():
        right_copy(1, piece(right, 1)).wait()
        left_copy(1, piece(left, 0)).wait()
        right_copy(2, sum_right).wait()
        left_copy(2, sum_left).wait()

    def total(w, at=()):
        near, across = (from_left, from_right) if w == 0 else (from_right, from_left)
        return (
            piece(place, w)[at or Ellipsis].astype(F32)
            + near[(2,) + at].astype(F32)
            + across[(1,) + at].astype(F32)
        )

    return start, middle, finish, total


def greet(me, tp, n_sp, n_tp, ring=False):
    barrier = pltpu.get_barrier_semaphore()

    def hello(d, carry):
        pl.semaphore_signal(
            barrier, inc=1, device_id=(lax.rem(me + d, n_sp), tp), device_id_type=MESH
        )
        return carry

    lax.fori_loop(1, n_sp, hello, 0)
    count = n_sp - 1
    if ring:
        for other in (lax.rem(tp + 1, n_tp), lax.rem(tp + n_tp - 1, n_tp)):
            pl.semaphore_signal(barrier, inc=1, device_id=(me, other), device_id_type=MESH)
        count += 2
    return lambda: pl.semaphore_wait(barrier, count)


def split(x, pieces):
    terms = []
    for _ in range(pieces):
        term = x.astype(BF16)
        terms.append(term)
        x = x - term.astype(F32)
    return terms


def dot_split(x, exact, pieces, contract, left=True):
    total = None
    for term in split(x, pieces):
        part = dot(term, exact, contract) if left else dot(exact, term, contract)
        total = part if total is None else total + part
    return total


def triangle(n, keep):
    return keep(iota((n, n), 0), iota((n, n), 1)).astype(BF16)


def head_spread(heads, size):
    channel, head = iota((heads, heads * size), 1), iota((heads, heads * size), 0)
    return ((channel >= head * size) & (channel < (head + 1) * size)).astype(BF16)


def spread(x, owner):
    return dot_split(x, owner, 2, ((1,), (0,)))


def by_head(x, owner):
    return dot_split(x, owner, 2, ((1,), (1,)))


def cumulative_decay(time_step, rate, extra):
    log_decay = extra - time_step * rate
    upto = triangle(log_decay.shape[0], lambda t, s: s <= t)
    return dot_split(log_decay, upto, 3, ((1,), (0,)), left=False)


def turned(x):
    n = x.shape[1]
    return dot_split(x, triangle(n, lambda a, b: a == b), 3, ((1,), (1,)), left=False)


def decay_between(cum, cum_rows, h):
    gap = cum[:, h : h + 1] - cum_rows[h : h + 1, :]
    n = gap.shape[0]
    return jnp.exp(jnp.where(iota((n, n), 1) <= iota((n, n), 0), gap, -1e30))


def halves(pair):
    lane = iota(pair.shape, 1)
    zero = jnp.zeros_like(pair)
    size = pair.shape[1] // 2
    return jnp.concatenate([jnp.where(lane < size, pair, zero), jnp.where(lane < size, zero, pair)], axis=0)


def front_part(
    n_sp,
    n_tp,
    begin,
    prepare,
    between,
    in_ref,
    x_ref,
    dt_ref,
    rate_ref,
    extra_ref,
    first_hbm,
    b_ref,
    c_ref,
    gate_ref,
    scale_ref,
    out_ref,
    y_ref,
    normed_ref,
    coming,
    decays,
    state_mine,
    decay_mine,
    states,
    carries,
    diag,
    own,
    one,
    two,
    a_send,
    a_recv,
    s_right,
    s_left,
    r_left,
    r_right,
    f_send,
    f_recv,
    sends,
    recvs,
    d_sends,
    d_recvs,
    b_sends,
    b_recvs,
    first_ref,
    first_sem,
):
    me, tp = lax.axis_index("sp"), lax.axis_index("tp")
    entering = pltpu.make_async_copy(first_hbm.at[me], first_ref, first_sem)
    entering.start()
    begin()
    right, left = lax.rem(tp + 1, n_tp), lax.rem(tp + n_tp - 1, n_tp)
    far = lax.rem(tp + 2, n_tp)
    met = greet(me, tp, n_sp, n_tp, ring=True)
    prepare()
    met()

    low, plane = lax.rem(me, 8), lax.div(me, 8)
    away = (0, 1, 3, 2)

    def planes_off(j):
        return lax.rem(plane + 4 - away[j], 4)

    def exchange(j, k):
        to = lax.rem(plane + away[j], 4) * 8 + lax.rem(low + k, 8)
        return pltpu.make_async_remote_copy(
            in_ref.at[to],
            out_ref.at[tp, me],
            a_send.at[8 * j + k],
            a_recv.at[8 * j + k],
            (to, tp),
            MESH,
        )

    def arrived(j, k):
        source = planes_off(j) * 8 + lax.rem(low + 8 - k, 8)
        return pltpu.make_async_remote_copy(
            in_ref.at[me],
            out_ref.at[tp, source],
            a_send.at[8 * j + k],
            a_recv.at[8 * j + k],
            (me, tp),
            MESH,
        )

    def to_right(j, block):
        piece = out_ref.at[block, pl.ds(pl.multiple_of(planes_off(j) * 8, 8), 8)]
        return pltpu.make_async_remote_copy(
            piece, piece, s_right.at[j], r_left.at[j], (me, right), MESH
        )

    def to_left(j, block):
        piece = out_ref.at[block, pl.ds(pl.multiple_of(planes_off(j) * 8, 8), 8)]
        return pltpu.make_async_remote_copy(
            piece, piece, s_left.at[j], r_right.at[j], (me, left), MESH
        )

    def onward(j, block, rightward):
        first = planes_off(j) * 8 + (0 if rightward else 4)
        piece = out_ref.at[block, pl.ds(pl.multiple_of(first, 4), 4)]
        at = j if rightward else 4 + j
        return pltpu.make_async_remote_copy(
            piece, piece, f_send.at[at], f_recv.at[at], (me, right if rightward else left), MESH
        )

    for j in range(4):

        def start_exchange(k, carry, j=j):
            exchange(j, k).start()
            return carry

        lax.fori_loop(1 if j == 0 else 0, 8, start_exchange, 0)

    def pass_on(j):
        def await_chunk(k, carry):
            arrived(j, k).wait_recv()
            return carry

        lax.fori_loop(1 if j == 0 else 0, 8, await_chunk, 0)
        to_right(j, tp).start()
        to_left(j, tp).start()

    mine = pltpu.make_async_copy(in_ref.at[me], out_ref.at[tp, me], own)
    mine.start()

    mine.wait()
    pass_on(0)

    heads, tokens = dt_ref.shape
    channels = x_ref.shape[1]
    groups = b_ref.shape[1] // STATE
    wide = channels // groups
    owner = head_spread(heads, HDIM)
    dt = turned(dt_ref[...])
    cum = cumulative_decay(dt, rate_ref[...], turned(extra_ref[...]))
    cum_rows = turned(cum)
    last = cum[tokens - 1 : tokens, :]
    values = x_ref[...].astype(F32)
    ending = (values * spread(dt * jnp.exp(last - cum), owner)).astype(BF16)
    parts, rows, entries = state_mine.shape
    per_group = parts // groups
    for g in range(groups):
        state = dot(
            ending[:, g * wide : (g + 1) * wide],
            b_ref[:, g * STATE : (g + 1) * STATE],
            ((0,), (0,)),
        )
        state_mine[g * per_group : (g + 1) * per_group] = state.astype(BF16).reshape(
            per_group, rows, entries
        )
    total = jnp.exp(last)
    for p in range(parts):
        h = p * rows // HDIM
        decay_mine[p] = jnp.broadcast_to(total[:, h : h + 1], (1, entries))


    def state_copy(d):
        to = lax.rem(me + d, n_sp)
        return pltpu.make_async_remote_copy(
            state_mine.at[to], states.at[me], sends.at[d], recvs.at[d], (to, tp), MESH
        )

    def decay_copy(d):
        to = lax.rem(me + d, n_sp)
        return pltpu.make_async_remote_copy(
            decay_mine.at[to], decays.at[me], d_sends.at[d], d_recvs.at[d], (to, tp), MESH
        )

    def back_copy(d):
        to = lax.rem(me + d, n_sp)
        return pltpu.make_async_remote_copy(
            carries.at[to], coming.at[me], b_sends.at[d], b_recvs.at[d], (to, tp), MESH
        )

    def start_states(d, carry):
        decay_copy(hop(d, n_sp)).start()
        state_copy(hop(d, n_sp)).start()
        return carry

    lax.fori_loop(1, n_sp, start_states, 0)
    kept = pltpu.make_async_copy(state_mine.at[me], states.at[me], one)
    kept_too = pltpu.make_async_copy(decay_mine.at[me], decays.at[me], two)
    kept.start()
    kept_too.start()

    pass_on(1)

    scaled = (values * spread(dt, owner)).astype(BF16)
    affinity = [
        dot(
            c_ref[:, g * STATE : (g + 1) * STATE],
            b_ref[:, g * STATE : (g + 1) * STATE],
            ((1,), (1,)),
        )
        for g in range(groups)
    ]
    for q in range(heads // 2):
        g = q // (heads // 2 // groups)
        both = jnp.concatenate(
            [(affinity[g] * decay_between(cum, cum_rows, 2 * q + j)).astype(BF16) for j in range(2)],
            axis=1,
        )
        at = slice(q * 2 * HDIM, (q + 1) * 2 * HDIM)
        diag[:, at] = dot(both, halves(scaled[:, at]))
        if q == heads // 4 - 1:
            pass_on(2)
    pass_on(3)

    kept.wait()
    kept_too.wait()

    def finish_states(d, carry):
        decay_copy(d).wait()
        state_copy(d).wait()
        return carry

    lax.fori_loop(1, n_sp, finish_states, 0)
    entering.wait()
    running = first_ref[...]
    for i in range(n_sp):
        carries[i] = running.astype(BF16)
        running = decays[i] * running + states[i].astype(F32)

    def start_back(d, carry):
        back_copy(hop(d, n_sp)).start()
        return carry

    lax.fori_loop(1, n_sp, start_back, 0)
    kept_back = pltpu.make_async_copy(carries.at[me], coming.at[me], one)
    kept_back.start()

    for j in range(4):
        to_right(j, left).wait_recv()
        onward(j, left, True).start()
        to_left(j, right).wait_recv()
        onward(j, right, False).start()
    kept_back.wait()

    def finish_back(d, carry):
        back_copy(d).wait()
        return carry

    lax.fori_loop(1, n_sp, finish_back, 0)
    since = spread(jnp.exp(cum), owner)
    for g in range(groups):
        at = slice(g * wide, (g + 1) * wide)
        incoming = coming[g * per_group : (g + 1) * per_group].reshape(wide, entries)
        y = diag[:, at] + since[:, at] * dot(
            c_ref[:, g * STATE : (g + 1) * STATE], incoming, ((1,), (1,))
        )
        y_ref[:, at] = y
        gate = gate_ref[:, at].astype(F32)
        gated = y * gate * jax.nn.sigmoid(gate)
        factor = lax.rsqrt(jnp.mean(gated * gated, axis=1, keepdims=True) + norm_eps)
        normed_ref[:, at] = (gated * factor * scale_ref[:, at]).astype(BF16)

    between()
    for j in range(4):
        onward(j, far, True).wait()
        onward(j, far, False).wait()
        to_right(j, tp).wait_send()
        to_left(j, tp).wait_send()

        def drain(k, carry, j=j):
            exchange(j, k).wait_send()
            return carry

        lax.fori_loop(1 if j == 0 else 0, 8, drain, 0)


def expert_part(
    n_sp,
    n_tp,
    in_ref,
    gate_hbm,
    up_hbm,
    down_hbm,
    routes_ref,
    grads_ref,
    own_hbm,
    mix_ref,
    all_ref,
    dgate_hbm,
    dup_hbm,
    ddown_hbm,
    w_gate,
    w_up,
    w_down,
    d_gate,
    d_up,
    d_down,
    x,
    x_t,
    g,
    gate_grad,
    up_grad,
    hidden,
    part_ref,
    from_left,
    from_right,
    sum_right,
    sum_left,
    out_blocks,
    back,
    own_cols,
    loads,
    stores,
    s_r,
    s_l,
    r_l,
    r_r,
    a_send,
    a_recv,
    g_send,
    g_recv,
    local,
    w_own,
    w_sends,
    w_recvs,
    so_far,
):
    me, tp = lax.axis_index("sp"), lax.axis_index("tp")
    right, left = lax.rem(tp + 1, n_tp), lax.rem(tp + n_tp - 1, n_tp)
    far = lax.rem(tp + 2, n_tp)
    tokens, width = grads_ref.shape
    half, quarter = width // 2, width // 4
    model, units = w_gate.shape
    rows = x.shape[0]
    cuts = [(i, min(256, units - i)) for i in range(0, units, 256)]
    fetches = []
    for k, (start, size) in enumerate(cuts):
        at = pl.ds(start, size)
        fetches.append(
            [
                pltpu.make_async_copy(gate_hbm.at[0, :, at], w_gate.at[:, at], loads.at[3 * k]),
                pltpu.make_async_copy(up_hbm.at[0, :, at], w_up.at[:, at], loads.at[3 * k + 1]),
                pltpu.make_async_copy(down_hbm.at[0, at, :], w_down.at[at, :], loads.at[3 * k + 2]),
            ]
        )
        for fetch in fetches[-1]:
            fetch.start()
    yield

    core = lax.rem(me, 2)
    lane_y, lane_z = lax.rem(lax.div(me, 2), 4), lax.div(me, 8)

    def at_y(y):
        return lane_z * 8 + y * 2 + core

    def at_z(z):
        return z * 8 + lane_y * 2 + core

    def weight_copy(k, src, dst, to):
        return pltpu.make_async_remote_copy(
            src, dst, w_sends.at[k], w_recvs.at[k], (to, tp), MESH
        )

    own_weight = pltpu.make_async_copy(own_hbm, all_ref.at[lane_z, lane_y, core], w_own)
    own_weight.start()

    def first_stage(j, sending):
        y, z = (lane_y, lane_z) if sending else (lax.rem(lane_y + 4 - j, 4), lax.rem(lane_z + 4 - j, 4))
        return [
            weight_copy(
                j - 1, own_hbm.at[0], all_ref.at[lane_z, y, core, 0], at_y(lax.rem(lane_y + j, 4))
            ),
            weight_copy(
                j + 2, own_hbm.at[1], all_ref.at[z, lane_y, core, 1], at_z(lax.rem(lane_z + j, 4))
            ),
        ]

    def second_stage(j, sending):
        y, z = (lane_y, lane_z) if sending else (lax.rem(lane_y + 4 - j, 4), lax.rem(lane_z + 4 - j, 4))
        by_z, by_y = all_ref.at[z, :, core, 0], all_ref.at[:, y, core, 1]
        return [
            weight_copy(j + 5, by_z, by_z, at_z(lax.rem(lane_z + j, 4))),
            weight_copy(j + 8, by_y, by_y, at_y(lax.rem(lane_y + j, 4))),
        ]

    def third_stage(c):
        return weight_copy(12, all_ref.at[:, :, c], all_ref.at[:, :, c], me + 1 - 2 * core)

    for j in range(1, 4):
        for copy in first_stage(j, True):
            copy.start()

    tall = in_ref.shape[2]
    group_of = 8
    span = group_of * CAP
    spots = iota((1, group_of * tall), 1)
    src = divide(spots, tall)
    inner = spots - src * tall
    which = divide(inner, CAP)
    row = src * CAP + inner - which * CAP
    lines = iota((span, 1), 0)
    pick = [((row == lines) & (which == p)).astype(BF16) for p in range(4)]

    def columns_of(b):
        return pl.ds(pl.multiple_of(b * width, width), width)

    def select(b):
        for k in range(n_sp // group_of):
            block = in_ref[b, k * group_of : (k + 1) * group_of].reshape(group_of * tall, half)
            at = slice(k * span, (k + 1) * span)
            for c in range(2):
                cols = pl.ds(pl.multiple_of(b * width + c * half, half), half)
                x[at, cols] = dot(pick[2 * c], block).astype(BF16)
                g[at, cols] = dot(pick[2 * c + 1], block).astype(BF16)

    def products(b, at):
        cols = columns_of(b)
        return (
            dot(x[:, cols], w_gate[cols, at]),
            dot(x[:, cols], w_up[cols, at]),
            dot(g[:, cols], w_down[at, cols], ((1,), (1,))),
        )

    near = (tp, left, right)
    for b in near:
        select(b)
    for k, (start, size) in enumerate(cuts):
        for fetch in fetches[k]:
            fetch.wait()
        at = slice(start, start + size)
        sums = [products(b, at) for b in near]
        for i in range(3):
            so_far[i, :, at] = sums[0][i] + sums[1][i] + sums[2][i]
    yield
    select(far)
    for start, size in cuts:
        at = slice(start, start + size)
        last_gate, last_up, last_grad = products(far, at)
        pre_gate = so_far[0, :, at] + last_gate
        pre_up = so_far[1, :, at] + last_up
        hidden_grad = so_far[2, :, at] + last_grad
        sigmoid_gate = jax.nn.sigmoid(pre_gate)
        activated = pre_gate * sigmoid_gate
        hidden[:, at] = (activated * pre_up).astype(BF16)
        gate_grad[:, at] = (
            hidden_grad * pre_up * sigmoid_gate * (1.0 + pre_gate * (1.0 - sigmoid_gate))
        ).astype(BF16)
        up_grad[:, at] = (hidden_grad * activated).astype(BF16)

    own_weight.wait()
    for j in range(1, 4):
        for copy in first_stage(j, False):
            copy.wait_recv()
    for j in range(1, 4):
        for copy in second_stage(j, True):
            copy.start()

    def row_block(b):
        for c in range(2):
            cols = pl.ds(pl.multiple_of(b * width + c * half, half), half)
            part_ref[2 * b + c] = (
                dot(gate_grad[...], w_gate[cols, :], ((1,), (1,)))
                + dot(up_grad[...], w_up[cols, :], ((1,), (1,)))
            ).astype(BF16)

    def block(b, which):
        return part_ref.at[2 * b + which]

    def right_copy(k, src):
        return pltpu.make_async_remote_copy(
            src, from_left.at[k], s_r.at[k], r_l.at[k], (me, right), MESH
        )

    def left_copy(k, src):
        return pltpu.make_async_remote_copy(
            src, from_right.at[k], s_l.at[k], r_r.at[k], (me, left), MESH
        )

    row_block(far)
    row_block(right)
    right_copy(0, block(far, 0)).start()
    left_copy(0, block(far, 1)).start()
    row_block(left)
    right_copy(1, block(right, 1)).start()
    row_block(tp)
    left_copy(1, block(left, 0)).start()

    saves = []

    def save(k, src, dst):
        copy = pltpu.make_async_copy(src, dst, stores.at[k])
        copy.start()
        saves.append(copy)

    def passed_right():
        right_copy(0, block(far, 0)).wait()
        sum_right[...] = (block(right, 0)[...].astype(F32) + from_left[0].astype(F32)).astype(BF16)
        left_copy(0, block(far, 1)).wait()
        sum_left[...] = (block(left, 1)[...].astype(F32) + from_right[0].astype(F32)).astype(BF16)

    def gate_up_rows(i):
        at = slice(i * 256, (i + 1) * 256)
        x_t[at, :] = jnp.transpose(x[:, at])
        d_gate[at, :] = dot(x_t[at, :], gate_grad[...]).astype(BF16)
        save(2 * i, d_gate.at[at, :], dgate_hbm.at[0, at, :])
        d_up[at, :] = dot(x_t[at, :], up_grad[...]).astype(BF16)
        save(2 * i + 1, d_up.at[at, :], dup_hbm.at[0, at, :])

    for i in range(4):
        gate_up_rows(i)
    passed_right()
    right_copy(2, sum_right).start()
    left_copy(2, sum_left).start()
    for i in range(4, 8):
        gate_up_rows(i)

    for k, (start, size) in enumerate(cuts):
        at = slice(start, start + size)
        d_down[at, :] = dot(hidden[:, at], g[...], ((0,), (0,))).astype(BF16)
        save(16 + k, d_down.at[at, :], ddown_hbm.at[0, at, :])

    for j in range(1, 4):
        for copy in second_stage(j, False):
            copy.wait_recv()
    third_stage(core).start()

    by_token = slots_in_rows(routes_ref[...], n_sp)
    line = iota((8, tokens), 0)
    slots = turned(
        jnp.where(line == 0, by_token[0], jnp.where(line == 1, by_token[1], 0)).astype(F32)
    ).astype(jnp.int32)
    column = iota((1, n_sp * 4 * CAP), 1)
    expert = divide(column, 4 * CAP)
    place_in = column - expert * (4 * CAP)
    piece = divide(place_in, CAP)
    slot = expert * CAP + place_in - piece * CAP
    match = (slots[:, 0:1] == slot) | (slots[:, 1:2] == slot)

    right_copy(1, block(right, 1)).wait()
    left_copy(1, block(left, 0)).wait()
    right_copy(2, sum_right).wait()
    left_copy(2, sum_left).wait()

    tall_out = iota((group_of * 4 * CAP, 1), 0)
    out_src = divide(tall_out, 4 * CAP)
    out_in = tall_out - out_src * (4 * CAP)
    out_piece = divide(out_in, CAP)
    out_row = out_src * CAP + out_in - out_piece * CAP
    pair_at = iota((1, span), 1)
    place = [((out_row == pair_at) & (out_piece == c)).astype(BF16) for c in range(4)]
    for k in range(rows // span):
        at = slice(k * span, (k + 1) * span)
        low = (
            part_ref[2 * tp, at, :].astype(F32)
            + from_left[2, at, :].astype(F32)
            + from_right[1, at, :].astype(F32)
        ).astype(BF16)
        high = (
            part_ref[2 * tp + 1, at, :].astype(F32)
            + from_right[2, at, :].astype(F32)
            + from_left[1, at, :].astype(F32)
        ).astype(BF16)
        laid = (
            dot(place[0], low[:, :quarter])
            + dot(place[1], low[:, quarter:])
            + dot(place[2], high[:, :quarter])
            + dot(place[3], high[:, quarter:])
        )
        out_blocks[k * group_of : (k + 1) * group_of] = laid.astype(BF16).reshape(
            group_of, 4 * CAP, quarter
        )

    def exchange(d):
        to = lax.rem(me + d, n_sp)
        return pltpu.make_async_remote_copy(
            out_blocks.at[to], back.at[me], a_send.at[d], a_recv.at[d], (to, tp), MESH
        )

    def start_exchange(d, carry):
        exchange(hop(d, n_sp)).start()
        return carry

    lax.fori_loop(1, n_sp, start_exchange, 0)
    mine = pltpu.make_async_copy(out_blocks.at[me], back.at[me], local)
    mine.start()
    mine.wait()

    def finish_exchange(d, carry):
        exchange(d).wait()
        return carry

    lax.fori_loop(1, n_sp, finish_exchange, 0)
    returned = back[...].reshape(n_sp * 4 * CAP, quarter)
    for c in range(4):
        chosen = jnp.where(match & (piece == c), 1.0, 0.0).astype(BF16)
        cols = slice(c * quarter, (c + 1) * quarter)
        own_cols[:, cols] = (grads_ref[:, cols].astype(F32) + dot(chosen, returned)).astype(BF16)

    def spot(b):
        return mix_ref.at[:, pl.ds(pl.multiple_of(b * width, width), width)]

    def spot_half(b, which):
        return mix_ref.at[:, pl.ds(pl.multiple_of(b * width + which * half, half), half)]

    def gather(k, src, dst, to):
        return pltpu.make_async_remote_copy(
            src, dst, g_send.at[k], g_recv.at[k], (me, to), MESH
        )

    gather(0, own_cols, spot(tp), right).start()
    gather(1, own_cols, spot(tp), left).start()
    spot(tp)[...] = own_cols[...]
    gather(0, own_cols, spot(left), right).wait_recv()
    gather(2, spot_half(left, 0), spot_half(left, 0), right).start()
    gather(1, own_cols, spot(right), left).wait_recv()
    gather(3, spot_half(right, 1), spot_half(right, 1), left).start()
    gather(2, spot_half(far, 0), spot_half(far, 0), right).wait()
    gather(3, spot_half(far, 1), spot_half(far, 1), left).wait()
    gather(0, own_cols, spot(tp), right).wait_send()
    gather(1, own_cols, spot(tp), left).wait_send()
    for copy in saves:
        copy.wait()
    for j in range(1, 4):
        for copy in first_stage(j, True) + second_stage(j, True):
            copy.wait_send()
    third_stage(core).wait_send()
    third_stage(1 - core).wait_recv()


def tail_part(
    n_sp,
    n_tp,
    mix_ref,
    weight,
    y_ref,
    normed_ref,
    x_ref,
    dt_ref,
    rate_ref,
    extra_ref,
    coming_ref,
    decays,
    b_ref,
    c_ref,
    gate_ref,
    scale_ref,
    proj_ref,
    dx_ref,
    ddt_ref,
    db_ref,
    dc_ref,
    dgate_ref,
    normed2,
    mix2,
    parts,
    big_in,
    big_sum,
    small_in,
    small_sum,
    reduced,
    total,
    state_mine,
    states,
    carries,
    later,
    d_scaled,
    one,
    p_send,
    p_recv,
    ring_sems,
    sends,
    recvs,
    b_sends,
    b_recvs,
):
    me, tp = lax.axis_index("sp"), lax.axis_index("tp")
    core = lax.rem(me, 2)
    partner = me + 1 - 2 * core
    chip = lax.div(me, 2)
    chips = n_sp // 2
    heads, tokens = dt_ref.shape
    channels = x_ref.shape[1]
    groups = b_ref.shape[1] // STATE
    wide = channels // groups
    half = channels // 2
    cols = proj_ref.shape[0]
    n_parts, rows, entries = state_mine.shape
    per_group = n_parts // groups

    def pair(k, src, dst):
        return pltpu.make_async_remote_copy(
            src, dst, p_send.at[k], p_recv.at[k], (partner, tp), MESH
        )

    def mine(c):
        return pl.ds(pl.multiple_of(c * half, half), half)

    pair(0, normed_ref.at[:, mine(1 - core)], normed2).start()
    pair(1, mix_ref, mix2).start()

    owner = head_spread(heads, HDIM)
    dt = turned(dt_ref[...])
    cum = cumulative_decay(dt, rate_ref[...], turned(extra_ref[...]))
    cum_rows = turned(cum)
    last = cum[tokens - 1 : tokens, :]
    since = spread(jnp.exp(cum), owner)

    whole_weight = weight[...].reshape(mix_ref.shape[1], channels)
    normed_grads = [
        dot(mix_ref[...], whole_weight[:, g * wide : (g + 1) * wide]) for g in range(groups)
    ]
    mix_t = jnp.transpose(mix_ref[...])
    d_y = []
    for g in range(groups):
        at = slice(g * wide, (g + 1) * wide)
        normed_grad = normed_grads[g]
        y = y_ref[:, at]
        gate = gate_ref[:, at].astype(F32)
        sigmoid_gate = jax.nn.sigmoid(gate)
        activated = gate * sigmoid_gate
        gated = y * activated
        factor = lax.rsqrt(jnp.mean(gated * gated, axis=1, keepdims=True) + norm_eps)
        scaled_grad = normed_grad * scale_ref[:, at]
        along = jnp.mean(scaled_grad * gated, axis=1, keepdims=True) * factor * factor
        gated_grad = factor * (scaled_grad - gated * along)
        d_y.append(gated_grad * activated)
        dgate_ref[:, at] = (
            gated_grad * y * (sigmoid_gate * (1.0 + gate * (1.0 - sigmoid_gate)))
        ).astype(BF16)
    d_out = jnp.concatenate(d_y, axis=1)
    since_grad = since * d_out
    since_low = since_grad.astype(BF16)
    for g in range(groups):
        state = dot(
            since_low[:, g * wide : (g + 1) * wide],
            c_ref[:, g * STATE : (g + 1) * STATE],
            ((0,), (0,)),
        )
        state_mine[g * per_group : (g + 1) * per_group] = state.astype(BF16).reshape(
            per_group, rows, entries
        )
    whole = jnp.exp(last)

    def state_copy(d):
        to = lax.rem(me + d, n_sp)
        return pltpu.make_async_remote_copy(
            state_mine.at[to], states.at[me], sends.at[d], recvs.at[d], (to, tp), MESH
        )

    def back_copy(d):
        to = lax.rem(me + d, n_sp)
        return pltpu.make_async_remote_copy(
            carries.at[to], later.at[me], b_sends.at[d], b_recvs.at[d], (to, tp), MESH
        )

    def start_states(d, carry):
        state_copy(hop(d, n_sp)).start()
        return carry

    lax.fori_loop(1, n_sp, start_states, 0)
    kept = pltpu.make_async_copy(state_mine.at[me], states.at[me], one)
    kept.start()

    pair(0, normed_ref.at[:, mine(1 - core)], normed2).wait()
    pair(1, mix_ref, mix2).wait()
    both_mix = jnp.concatenate([mix_t, jnp.transpose(mix2[...])], axis=1)
    both_normed = jnp.concatenate([normed_ref[:, mine(core)], normed2[...]], axis=0)
    piece_rows = cols // 2
    for z in range(4):
        at = slice(z * 8 * cols, (z + 1) * 8 * cols)
        parts[z] = (
            dot(both_mix[at, :], both_normed).astype(BF16).reshape(4, 2, 2, piece_rows, half)
        )

    lane_y, lane_z = lax.rem(chip, 4), lax.div(chip, 4)

    def at_y(y):
        return (lane_z * 8 + lax.rem(y, 4) * 2 + core, tp)

    def at_z(z):
        return (lax.rem(z, 4) * 8 + lane_y * 2 + core, tp)

    y_ring = (lane_y, at_y(lane_y + 1), at_y(lane_y + 3))
    z_ring = (lane_z, at_z(lane_z + 1), at_z(lane_z + 3))

    def four(ref, k):
        return [ref.at[k, i] for i in range(4)]

    def bufs(landing, sums, k):
        return [landing.at[k, 0], landing.at[k, 1], sums.at[k, 0], sums.at[k, 1]]

    stages = [
        ring_reduce(lambda b, w: parts.at[:, b, 0, w], *y_ring, *bufs(big_in, big_sum, 0), four(ring_sems, 0)),
        ring_reduce(lambda b, w: parts.at[b, :, 1, w], *z_ring, *bufs(big_in, big_sum, 1), four(ring_sems, 1)),
        ring_reduce(lambda b, w: reduced.at[0, w, b], *z_ring, *bufs(small_in, small_sum, 0), four(ring_sems, 2)),
        ring_reduce(lambda b, w: reduced.at[1, w, b], *y_ring, *bufs(small_in, small_sum, 1), four(ring_sems, 3)),
    ]
    stages[0][0]()
    stages[1][0]()


    values = x_ref[...].astype(F32)
    steps = spread(dt, owner)
    scaled = values * steps
    scaled_low = scaled.astype(BF16)
    d_low = d_out.astype(BF16)
    not_before = triangle(tokens, lambda t, s: s >= t)
    below = (iota((tokens, tokens), 1) < iota((tokens, tokens), 0)).astype(F32)
    head_lane = iota((1, heads), 1)
    crossing = [jnp.zeros((tokens, heads), F32)]
    d_affinity = []

    def inside(g):
        affinity = dot(
            c_ref[:, g * STATE : (g + 1) * STATE],
            b_ref[:, g * STATE : (g + 1) * STATE],
            ((1,), (1,)),
        )
        sum_affinity = jnp.zeros((tokens, tokens), F32)
        first = g * (heads // 2 // groups)
        for q in range(first, first + heads // 2 // groups):
            at = slice(q * 2 * HDIM, (q + 1) * 2 * HDIM)
            d_halves = halves(d_low[:, at])
            d_weights = dot(d_halves, scaled_low[:, at], ((1,), (1,)))
            weights, moved = [], []
            for j in range(2):
                between = decay_between(cum, cum_rows, 2 * q + j)
                weights.append((affinity * between).astype(BF16))
                d_between = d_weights[j * tokens : (j + 1) * tokens] * between
                sum_affinity = sum_affinity + d_between
                moved.append((d_between * affinity).astype(BF16))
            d_scaled[:, at] = dot(jnp.concatenate(weights, axis=0), d_halves, ((0,), (0,)))
            reach = dot(not_before, jnp.concatenate(moved, axis=1))
            for j in range(2):
                over = jnp.sum(
                    reach[:, j * tokens : (j + 1) * tokens] * below, axis=1, keepdims=True
                )
                crossing[0] = crossing[0] + jnp.where(head_lane == 2 * q + j, over, 0.0)
        d_affinity.append(sum_affinity.astype(BF16))

    inside(0)
    kept.wait()

    def finish_states(d, carry):
        state_copy(d).wait()
        return carry

    lax.fori_loop(1, n_sp, finish_states, 0)
    running = jnp.zeros((rows, entries), F32)
    for step in range(n_sp):
        i = n_sp - 1 - step
        carries[i] = running.astype(BF16)
        running = decays[i] * running + states[i].astype(F32)

    def start_back(d, carry):
        back_copy(hop(d, n_sp)).start()
        return carry

    lax.fori_loop(1, n_sp, start_back, 0)
    kept_back = pltpu.make_async_copy(carries.at[me], later.at[me], one)
    kept_back.start()

    for g in range(1, groups):
        inside(g)
    stages[0][1]()
    stages[1][1]()
    read_out = []
    for g in range(groups):
        at = slice(g * wide, (g + 1) * wide)
        by = slice(g * STATE, (g + 1) * STATE)
        incoming = coming_ref[g * per_group : (g + 1) * per_group].reshape(wide, entries)
        read_out.append(dot(c_ref[:, by], incoming, ((1,), (1,))))
        dc_ref[:, by] = (
            dot(d_affinity[g], b_ref[:, by]) + dot(since_low[:, at], incoming)
        ).astype(BF16)
    for k in range(2):
        stages[k][2]()
        for w in range(2):
            reduced[k, w] = stages[k][3](w).astype(BF16)
    stages[2][0]()
    stages[3][0]()
    reading = by_head(since_grad * jnp.concatenate(read_out, axis=1), owner)

    kept_back.wait()

    def finish_back(d, carry):
        back_copy(d).wait()
        return carry

    lax.fori_loop(1, n_sp, finish_back, 0)
    until = spread(jnp.exp(last - cum), owner)
    ending = scaled * until
    ending_low = ending.astype(BF16)
    from_later = []
    for g in range(groups):
        at = slice(g * wide, (g + 1) * wide)
        by = slice(g * STATE, (g + 1) * STATE)
        after = later[g * per_group : (g + 1) * per_group].reshape(wide, entries)
        from_later.append(dot(b_ref[:, by], after, ((1,), (1,))))
        db_ref[:, by] = (
            dot(d_affinity[g], c_ref[:, by], ((0,), (0,))) + dot(ending_low[:, at], after)
        ).astype(BF16)
    stages[2][1]()
    stages[3][1]()
    closing = jnp.concatenate(from_later, axis=1)
    gradient = d_scaled[...] + until * closing
    dx_ref[...] = (gradient * steps).astype(BF16)
    direct = by_head(gradient * values, owner)
    stored = by_head(ending * closing, owner)
    kept_state = jnp.sum(
        (
            coming_ref[...].astype(F32).reshape(heads, HDIM, entries)
            * later[...].astype(F32).reshape(heads, HDIM, entries)
        ),
        axis=1,
    )
    passing = dot_split(
        kept_state, jnp.ones((8, entries), BF16), 3, ((1,), (1,)), left=False
    )[0:1, :]
    earlier = triangle(tokens, lambda t, s: s < t)
    d_decay = (
        crossing[0]
        + dot_split(reading, not_before, 3, ((1,), (0,)), left=False)
        + dot_split(stored, earlier, 3, ((1,), (0,)), left=False)
        + passing * whole
    )
    ddt_ref[...] = turned(direct - d_decay * rate_ref[...])

    for k in range(2):
        stages[2 + k][2]()
        for w in range(2):
            first = (2 * k + w) * piece_rows
            total[first : first + piece_rows, :] = stages[2 + k][3](w)

    def lines(c):
        return pl.ds(pl.multiple_of(c * cols, cols), cols)

    given = pair(2, total.at[lines(1 - core), :], proj_ref.at[:, mine(core)])
    given.start()
    proj_ref[:, mine(core)] = total[lines(core), :]
    given.wait_send()
    pair(2, total.at[lines(core), :], proj_ref.at[:, mine(1 - core)]).wait_recv()


FRONT_SCRATCH = 24
EXPERT_SCRATCH = 35


def main_kernel(n_sp, n_tp, *refs):
    (stream, weights, x, dt, rate, extra, first, b, c, gate, scale) = refs[:11]
    (w_gate, w_up, w_down, routes, grads, own) = refs[11:17]
    tail_outs = refs[17:23]
    weight_grads = refs[23:26]
    (packed, arrived, y, normed, coming, decays, mix, all_weight) = refs[26:34]
    front_scratch = refs[34 : 34 + FRONT_SCRATCH]
    expert_scratch = refs[34 + FRONT_SCRATCH : 34 + FRONT_SCRATCH + EXPERT_SCRATCH]
    tail_scratch = refs[34 + FRONT_SCRATCH + EXPERT_SCRATCH :]
    steps = expert_part(
        n_sp,
        n_tp,
        arrived,
        w_gate,
        w_up,
        w_down,
        routes,
        grads,
        own,
        mix,
        all_weight,
        *weight_grads,
        *expert_scratch,
    )
    front_part(
        n_sp,
        n_tp,
        lambda: next(steps),
        lambda: pack(n_sp, routes, weights, stream, grads, packed),
        lambda: next(steps),
        packed,
        x,
        dt,
        rate,
        extra,
        first,
        b,
        c,
        gate,
        scale,
        arrived,
        y,
        normed,
        coming,
        decays,
        *front_scratch,
    )
    for _ in steps:
        pass
    tail_part(
        n_sp,
        n_tp,
        mix,
        all_weight,
        y,
        normed,
        x,
        dt,
        rate,
        extra,
        coming,
        decays,
        b,
        c,
        gate,
        scale,
        *tail_outs,
        *tail_scratch,
    )


def main(
    stream, weights, x, dt, rate, extra, first, b, c, gate, scale, w_gate, w_up, w_down, routes, grads, own, n_sp, n_tp
):
    dma = pltpu.SemaphoreType.DMA
    tokens, channels = x.shape
    _, rows, entries = first.shape
    _, model, units = w_gate.shape
    pairs = n_sp * CAP
    width = grads.shape[1]
    half, quarter = width // 2, width // 4
    front_scratch = (
        [
            pltpu.VMEM((n_sp, rows, entries), BF16),
            pltpu.VMEM((n_sp, 1, entries), F32),
            pltpu.VMEM((n_sp, rows, entries), BF16),
            pltpu.VMEM((n_sp, rows, entries), BF16),
            pltpu.VMEM((tokens, channels), F32),
            dma,
            dma,
            dma,
        ]
        + [dma((n_sp,))] * 2
        + [dma((4,))] * 4
        + [dma((8,))] * 2
        + [dma((n_sp,))] * 6
        + [pltpu.VMEM((rows, entries), F32), dma]
    )
    expert_scratch = [
        pltpu.VMEM((model, units), BF16),
        pltpu.VMEM((model, units), BF16),
        pltpu.VMEM((units, model), BF16),
        pltpu.VMEM((model, units), BF16),
        pltpu.VMEM((model, units), BF16),
        pltpu.VMEM((units, model), BF16),
        pltpu.VMEM((pairs, model), BF16),
        pltpu.VMEM((model, pairs), BF16),
        pltpu.VMEM((pairs, model), BF16),
        pltpu.VMEM((pairs, units), BF16),
        pltpu.VMEM((pairs, units), BF16),
        pltpu.VMEM((pairs, units), BF16),
        pltpu.VMEM((2 * n_tp, pairs, half), BF16),
        pltpu.VMEM((3, pairs, half), BF16),
        pltpu.VMEM((3, pairs, half), BF16),
        pltpu.VMEM((pairs, half), BF16),
        pltpu.VMEM((pairs, half), BF16),
        pltpu.VMEM((n_sp, 4 * CAP, quarter), BF16),
        pltpu.VMEM((n_sp, 4 * CAP, quarter), BF16),
        pltpu.VMEM((tokens, width), BF16),
        dma((12,)),
        dma((20,)),
        dma((3,)),
        dma((3,)),
        dma((3,)),
        dma((3,)),
        dma((n_sp,)),
        dma((n_sp,)),
        dma((4,)),
        dma((4,)),
        dma,
        dma,
        dma((13,)),
        dma((13,)),
        pltpu.VMEM((3, pairs, units), F32),
    ]
    cols = own.shape[0] * own.shape[1]
    tail_scratch = (
        [
            pltpu.VMEM((tokens, channels // 2), BF16),
            pltpu.VMEM((tokens, width * n_tp), BF16),
            pltpu.VMEM((4, 4, 2, 2, cols // 2, channels // 2), BF16),
            pltpu.VMEM((2, 2, 3, 4, cols // 2, channels // 2), BF16),
            pltpu.VMEM((2, 2, 4, cols // 2, channels // 2), BF16),
            pltpu.VMEM((2, 2, 3, cols // 2, channels // 2), BF16),
            pltpu.VMEM((2, 2, cols // 2, channels // 2), BF16),
            pltpu.VMEM((2, 2, 4, cols // 2, channels // 2), BF16),
            pltpu.VMEM((2 * cols, channels // 2), F32),
            pltpu.VMEM((n_sp, rows, entries), BF16),
            pltpu.VMEM((n_sp, rows, entries), BF16),
            pltpu.VMEM((n_sp, rows, entries), BF16),
            pltpu.VMEM((n_sp, rows, entries), BF16),
            pltpu.VMEM((tokens, channels), F32),
            dma,
            dma((3,)),
            dma((3,)),
            dma((4, 4, 3)),
        ]
        + [dma((n_sp,))] * 4
    )
    return pl.pallas_call(
        functools.partial(main_kernel, n_sp, n_tp),
        out_shape=(
            jax.ShapeDtypeStruct((own.shape[0] * own.shape[1], channels), F32),
            jax.ShapeDtypeStruct((tokens, channels), BF16),
            jax.ShapeDtypeStruct(dt.shape, F32),
            jax.ShapeDtypeStruct(b.shape, BF16),
            jax.ShapeDtypeStruct(c.shape, BF16),
            jax.ShapeDtypeStruct((tokens, channels), BF16),
            jax.ShapeDtypeStruct(w_gate.shape, BF16),
            jax.ShapeDtypeStruct(w_up.shape, BF16),
            jax.ShapeDtypeStruct(w_down.shape, BF16),
        ),
        in_specs=[vmem_spec()] * 6
        + [any_spec()]
        + [vmem_spec()] * 4
        + [any_spec()] * 3
        + [vmem_spec()] * 2
        + [any_spec()],
        out_specs=(vmem_spec(),) * 6 + (any_spec(),) * 3,
        scratch_shapes=[
            pltpu.VMEM((n_sp, 4 * CAP, half), BF16),
            pltpu.VMEM((n_tp, n_sp, 4 * CAP, half), BF16),
            pltpu.VMEM((tokens, channels), F32),
            pltpu.VMEM((tokens, channels), BF16),
            pltpu.VMEM((n_sp, rows, entries), BF16),
            pltpu.VMEM((n_sp, 1, entries), F32),
            pltpu.VMEM((tokens, width * n_tp), BF16),
            pltpu.VMEM((4, 4, 2) + own.shape, BF16),
        ]
        + front_scratch
        + expert_scratch
        + tail_scratch,
        compiler_params=pltpu.CompilerParams(
            collective_id=0, has_side_effects=True, vmem_limit_bytes=VMEM_BYTES
        ),
        name="main",
    )(
        stream, weights, x, dt, rate, extra, first, b, c, gate, scale, w_gate, w_up, w_down, routes, grads, own
    )


def finish_kernel(count, *refs):
    sources, results, held = refs[:count], refs[count : 2 * count], refs[2 * count : 3 * count]
    loads, stores = refs[3 * count :]
    copies = []
    for i in range(count):
        lines = sources[i].shape[-2]
        pieces = 4 if lines > 512 else 1
        for p in range(pieces):
            at = pl.ds(p * (lines // pieces), lines // pieces)
            views = [
                ref.at[0, at, :] if len(ref.shape) == 3 else ref.at[at, :]
                for ref in (sources[i], held[i], results[i])
            ]
            k = len(copies)
            copies.append(
                (
                    pltpu.make_async_copy(views[0], views[1], loads.at[k]),
                    pltpu.make_async_copy(views[1], views[2], stores.at[k]),
                )
            )
    for load, _ in copies:
        load.start()
    for load, store in copies:
        load.wait()
        store.start()
    for _, store in copies:
        store.wait()


def finish(*arrays):
    count = len(arrays)
    dma = pltpu.SemaphoreType.DMA
    return pl.pallas_call(
        functools.partial(finish_kernel, count),
        out_shape=tuple(jax.ShapeDtypeStruct(a.shape, a.dtype) for a in arrays),
        in_specs=[any_spec()] * count,
        out_specs=(any_spec(),) * count,
        scratch_shapes=[pltpu.VMEM(a.shape, a.dtype) for a in arrays]
        + [dma((4 * count,)), dma((4 * count,))],
        compiler_params=pltpu.CompilerParams(vmem_limit_bytes=VMEM_BYTES),
        name="finish",
    )(*arrays)


def body(
    n_sp,
    n_tp,
    mixer_output_stream,
    layer_output_gradient,
    routes,
    expert_combine_weight,
    expert_gate_weight,
    expert_up_weight,
    expert_down_weight,
    head_mixer_input,
    head_step_size,
    head_decay_rate,
    extra_log_decay,
    state_entering_span,
    state_input_vectors,
    state_readout_vectors,
    gate_preactivation,
    group_norm_scale,
    mixer_output_weight,
):
    heads = head_step_size.shape[1]
    part_rows = heads * HDIM // n_sp
    entering = state_entering_span.reshape(n_sp, part_rows, STATE)
    rate = head_decay_rate[None, :]
    scale = group_norm_scale[None, :]
    proj_grad, input_grad, step_grad, b_grad, c_grad, gate_grad_in, grad_g, grad_u, grad_d = main(
        mixer_output_stream,
        expert_combine_weight.T,
        head_mixer_input,
        head_step_size.T,
        rate,
        extra_log_decay.T,
        entering,
        state_input_vectors,
        state_readout_vectors,
        gate_preactivation,
        scale,
        expert_gate_weight,
        expert_up_weight,
        expert_down_weight,
        routes.T,
        layer_output_gradient,
        mixer_output_weight.T.reshape(2, -1, mixer_output_weight.shape[0]),
        n_sp,
        n_tp,
    )
    proj_grad, input_grad, step_grad, b_grad, c_grad, gate_grad_in, grad_g, grad_u, grad_d = finish(
        proj_grad,
        input_grad,
        step_grad,
        b_grad,
        c_grad,
        gate_grad_in,
        grad_g,
        grad_u,
        grad_d,
    )
    return (
        grad_g,
        grad_u,
        grad_d,
        proj_grad.T,
        input_grad,
        step_grad.T,
        b_grad,
        c_grad,
        gate_grad_in,
    )


def solution(mesh):
    placed = (
        P(SP, "tp"),
        P(SP, "tp"),
        P(SP, None),
        P(SP, None),
        P(SP, None, "tp"),
        P(SP, None, "tp"),
        P(SP, "tp", None),
        P(SP, "tp"),
        P(SP, "tp"),
        P("tp"),
        P(SP, "tp"),
        P("tp", None, None),
        P(SP, "tp"),
        P(SP, "tp"),
        P(SP, "tp"),
        P("tp"),
        P("tp", SP),
    )
    return jax.shard_map(
        functools.partial(body, mesh.shape["sp"], mesh.shape["tp"]),
        mesh=mesh,
        in_specs=placed,
        out_specs=(
            P(SP, None, "tp"),
            P(SP, None, "tp"),
            P(SP, "tp", None),
            P("tp", SP),
            P(SP, "tp"),
            P(SP, "tp"),
            P(SP, "tp"),
            P(SP, "tp"),
            P(SP, "tp"),
        ),
        check_vma=False,
    )
```
